128 devices in a mesh: sp: 16 (over z, x), fs: 4 (over y), tp: 2 (over core).
Axes of the slice: x: 4, y: 4, z: 4, core: 2. Of those that a mesh axis runs over, the one named last changes fastest.
Arguments:
- tokens: bfloat16 [4, 16384, 2048], P('fs', ('sp', 'tp')), may hold values from -6 to 6
- norm_gain: bfloat16 [2048], replicated, may hold values from 0.099609375 to 1.8984375
- w_query: bfloat16 [2048, 1024], P(None, 'tp'), may hold values from -0.125 to 0.125
- w_key: bfloat16 [2048, 1024], P(None, 'tp'), may hold values from -0.125 to 0.125
- w_value: bfloat16 [2048, 1024], P(None, 'tp'), may hold values from -0.125 to 0.125
- w_outgate: bfloat16 [2048, 1024], P(None, 'tp'), may hold values from -0.125 to 0.125
- w_gatein: bfloat16 [2048, 1024], P(None, 'tp'), may hold values from -0.125 to 0.125
- w_gateout: bfloat16 [2048, 1024], P(None, 'tp'), may hold values from -0.125 to 0.125
- w_convin: bfloat16 [2048, 1024], P(None, 'tp'), may hold values from -0.125 to 0.125
- w_igate: bfloat16 [2048, 8], replicated, may hold values from -0.125 to 0.125
- w_fgate: bfloat16 [2048, 8], replicated, may hold values from -0.125 to 0.125
- input_bias: float32 [8], replicated, may hold values from -1 to 101
- forget_bias: float32 [8], replicated
- forget_extra: float32 [4, 16384, 8], P('fs', 'sp', 'tp'), may hold values from -0.7 to 0
- init_memory: float32 [4, 8, 128, 128], P('fs', 'tp'), may hold values from -112 to 112
- head_gain: bfloat16 [1024], replicated, may hold values from 0.099609375 to 1.8984375
- conv_taps: bfloat16 [3, 1024], replicated, may hold values from -3.5 to 3.5
- out_memory: bfloat16 [1024, 2048], P('tp'), may hold values from -0.125 to 0.125
- out_conv: bfloat16 [1024, 2048], P('tp'), may hold values from -0.125 to 0.125
Outputs:
- layer_out: bfloat16 [4, 16384, 2048], P('fs', ('sp', 'tp'))
The draws below stay inside these ranges and needn't reach their ends.
All inputs are finite; a program needn't handle non-finite values.
Results may differ from the reference program's by a relative error of at most 0.017.
Values may be sent and summed in bfloat16 or wider, within the bound.
No kernel may reach another device: no remote copies, remote signals or barrier semaphores. Data moves between devices by JAX's collectives and lax.ppermute only.
A program may use at most 128 MiB of HBM per device.

```python
import math
import jax
import jax.numpy as jnp
from jax import lax

D = 2048
MEMORY_HEADS = 8
DH = 128
HALF = 1024
BLOCK = 128
TAPS = 3
TOK_DEV = 1024
SEQUENCE_COUNT = 4
SEQUENCE_LENGTH = 16384
N_TP = 2


def draw_input_bias(key, part):
    base_key = jax.random.fold_in(jax.random.fold_in(key, 11), 0)
    steady_forget = jax.random.uniform(base_key, (MEMORY_HEADS,), jnp.float32, -1.0, 1.0)
    return steady_forget


def draw_forget_bias(key, part):
    slow_key, fast_key, pick_key = jax.random.split(jax.random.fold_in(key, 23), 3)
    slow_bias = math.log(SEQUENCE_LENGTH) + jax.random.uniform(slow_key, (MEMORY_HEADS,), jnp.float32, 1.5, 3.0)
    fast_bias = jax.random.uniform(fast_key, (MEMORY_HEADS,), jnp.float32, 3.4, 4.6)
    chosen = jax.random.permutation(pick_key, MEMORY_HEADS) < MEMORY_HEADS // 2
    return jnp.where(chosen, fast_bias, slow_bias)


def draw_forget_extra(key, part):
    rate_key, place_random_key, drop_random_key = jax.random.split(jax.random.fold_in(key, 37), 3)
    span_count = SEQUENCE_LENGTH // TOK_DEV
    span_rates = jnp.exp(jax.random.uniform(rate_key, (SEQUENCE_COUNT, span_count, 1, MEMORY_HEADS), jnp.float32, math.log(0.1), math.log(0.8))) / SEQUENCE_LENGTH
    steady_forget = -jnp.broadcast_to(span_rates, (SEQUENCE_COUNT, span_count, TOK_DEV, MEMORY_HEADS)).reshape(SEQUENCE_COUNT, SEQUENCE_LENGTH, MEMORY_HEADS)
    sudden_drop_places = jax.random.randint(place_random_key, (SEQUENCE_COUNT, 2), 0, SEQUENCE_LENGTH)
    sudden_drop_mask = jnp.any(jnp.arange(SEQUENCE_LENGTH)[None, :, None] == sudden_drop_places[:, None, :], axis=-1)
    sudden_drop_values = jax.random.uniform(drop_random_key, (SEQUENCE_COUNT, SEQUENCE_LENGTH, MEMORY_HEADS), jnp.float32, math.log(0.5), math.log(0.8))
    return steady_forget + jnp.where(sudden_drop_mask[:, :, None], sudden_drop_values, 0.0)


def shard_levels(key, extent, cuts, smallest, top_value):
    level = 1.0
    for dim, parts in cuts:
        steps = jax.random.uniform(jax.random.fold_in(jax.random.fold_in(key, 6), dim), (parts,), jnp.float32, smallest / len(cuts), top_value / len(cuts))
        level = level * jnp.repeat(jnp.exp(steps), extent[dim] // parts).reshape((-1,) + (1,) * (len(extent) - 1 - dim))
    return level


def gaussian(own_key, extent, spread, reach, shards=(), held_as=jnp.bfloat16):
    result = spread * jax.random.normal(own_key, extent, jnp.float32)
    if shards:
        result = result * shard_levels(own_key, extent, shards, -0.22, 0.18)
    return jnp.clip(result, -reach, reach).astype(held_as)


def setup_inputs(seed: int = 0) -> dict:
    seeds = jax.random.split(jax.random.key(seed), 20)
    return {
        "tokens": gaussian(seeds[0], (SEQUENCE_COUNT, SEQUENCE_LENGTH, D), 1.0, 6.0, ((0, 4), (1, 32))),
        "norm_gain": jnp.clip(1.0 + 0.18 * jax.random.normal(seeds[1], (D,), jnp.float32), 0.099609375, 1.8984375).astype(jnp.bfloat16),
        "w_query": gaussian(seeds[2], (D, HALF), D ** -0.5, 0.125, ((1, 2),)),
        "w_key": gaussian(seeds[3], (D, HALF), D ** -0.5, 0.125, ((1, 2),)),
        "w_value": gaussian(seeds[4], (D, HALF), D ** -0.5, 0.125, ((1, 2),)),
        "w_outgate": gaussian(seeds[5], (D, HALF), D ** -0.5, 0.125, ((1, 2),)),
        "w_gatein": gaussian(seeds[6], (D, HALF), D ** -0.5, 0.125, ((1, 2),)),
        "w_gateout": gaussian(seeds[7], (D, HALF), D ** -0.5, 0.125, ((1, 2),)),
        "w_convin": gaussian(seeds[8], (D, HALF), D ** -0.5, 0.125, ((1, 2),)),
        "w_igate": gaussian(seeds[9], (D, MEMORY_HEADS), D ** -0.5, 0.125),
        "w_fgate": gaussian(seeds[10], (D, MEMORY_HEADS), D ** -0.5, 0.125),
        "input_bias": draw_input_bias(jax.random.fold_in(seeds[19], 71), 0),
        "forget_bias": draw_forget_bias(jax.random.fold_in(seeds[19], 71), 0),
        "forget_extra": draw_forget_extra(jax.random.fold_in(seeds[19], 71), 0),
        "init_memory": gaussian(seeds[14], (SEQUENCE_COUNT, MEMORY_HEADS, DH, DH), (0.15 * SEQUENCE_LENGTH ** 0.5), 112.0, ((0, 4), (1, 2)), jnp.float32),
        "head_gain": jnp.clip(1.0 + 0.18 * jax.random.normal(seeds[15], (HALF,), jnp.float32), 0.099609375, 1.8984375).astype(jnp.bfloat16),
        "conv_taps": gaussian(seeds[16], (TAPS, HALF), TAPS ** -0.5, 3.5),
        "out_memory": gaussian(seeds[17], (HALF, D), (2 * HALF) ** -0.5, 0.125, ((0, 2),)),
        "out_conv": gaussian(seeds[18], (HALF, D), (2 * HALF) ** -0.5, 0.125, ((0, 2),)),
    }


EPSILON = 1e-06

def memory_cell(queries, key_rows, value_rows, input_pre, log_forget, start_memory):
    nblocks = SEQUENCE_LENGTH // BLOCK
    key_factor = DH ** (-0.5)
    highest = lax.Precision.HIGHEST

    def blocked(matrix):
        return jnp.swapaxes(matrix.reshape(nblocks, BLOCK, MEMORY_HEADS, DH), 1, 2).astype(jnp.float32)

    def gate_blocks(matrix):
        return jnp.swapaxes(matrix.reshape(nblocks, BLOCK, MEMORY_HEADS), 1, 2)
    causal = jnp.tril(jnp.ones((BLOCK, BLOCK), dtype=bool))

    def advance(memory_pair, inputs):
        memory, log_scale = memory_pair
        query_blk, key_blk, value_blk, gate_in_blk, forget_blk = inputs
        cumulative = jnp.cumsum(forget_blk, axis=-1)
        block_total = cumulative[:, -1]
        exponent = block_total[:, None] - cumulative + gate_in_blk
        block_top = lax.optimization_barrier(jnp.max(exponent, axis=-1))
        weighted_keys = (jnp.exp(exponent - block_top[:, None])[:, :, None] * key_blk * key_factor).astype(jnp.bfloat16)
        weighted_keys = lax.optimization_barrier(weighted_keys).astype(jnp.float32)
        block_terms = jnp.einsum('hsd,hse->hde', weighted_keys, value_blk, precision=highest)
        pair_log = cumulative[:, :, None] - cumulative[:, None, :] + gate_in_blk[:, None, :]
        pair_log = jnp.where(causal, pair_log, -jnp.inf)
        carried_log = cumulative + log_scale[:, None]
        row_top = jnp.maximum(carried_log, lax.optimization_barrier(jnp.max(pair_log, axis=-1)))
        scores = jnp.einsum('htd,hsd->hts', query_blk, key_blk, precision=highest) * key_factor
        weighted = (jnp.exp(pair_log - row_top[:, :, None]) * scores).astype(jnp.bfloat16)
        weighted = lax.optimization_barrier(weighted).astype(jnp.float32)
        carried = jnp.einsum('htd,hde->hte', query_blk, memory, precision=highest)
        readout = jnp.exp(carried_log - row_top)[:, :, None] * carried
        readout = readout + jnp.einsum('hts,hse->hte', weighted, value_blk, precision=highest)
        new_scale = jnp.maximum(block_total + log_scale, block_top)
        new_memory = jnp.exp(block_total + log_scale - new_scale)[:, None, None] * memory
        new_memory = new_memory + jnp.exp(block_top - new_scale)[:, None, None] * block_terms
        return ((new_memory, new_scale), readout)
    start_pair = (start_memory, jnp.zeros((MEMORY_HEADS,), jnp.float32))
    inputs = (blocked(queries), blocked(key_rows), blocked(value_rows), gate_blocks(input_pre), gate_blocks(log_forget))
    final_pair, readouts = lax.scan(advance, start_pair, inputs)
    return jnp.swapaxes(readouts, 1, 2).reshape(SEQUENCE_LENGTH, HALF)

def reference(tokens, norm_gain, w_query, w_key, w_value, w_outgate, w_gatein, w_gateout, w_convin, w_igate, w_fgate, input_bias, forget_bias, forget_extra, init_memory, head_gain, conv_taps, out_memory, out_conv):
    group_width = HALF // N_TP
    outputs = []
    for seq_index in range(SEQUENCE_COUNT):
        seq_rows = tokens[seq_index].astype(jnp.float32)
        normed = seq_rows * lax.rsqrt(lax.optimization_barrier(jnp.mean(seq_rows * seq_rows, axis=-1, keepdims=True)) + EPSILON)
        normed = (normed * norm_gain.astype(jnp.float32)).astype(jnp.bfloat16)

        def project(weight):
            return jnp.dot(normed, weight, preferred_element_type=jnp.float32).astype(jnp.bfloat16)
        queries = project(w_query)
        key_rows = project(w_key)
        value_rows = project(w_value)
        out_gate = project(w_outgate)
        gate_in = project(w_gatein)
        gate_out = project(w_gateout)
        conv_input = project(w_convin)
        input_pre = jnp.dot(normed, w_igate, preferred_element_type=jnp.float32) + input_bias
        forget_pre = jnp.dot(normed, w_fgate, preferred_element_type=jnp.float32) + forget_bias
        log_forget = jax.nn.log_sigmoid(forget_pre) + forget_extra[seq_index]
        readout = memory_cell(queries, key_rows, value_rows, input_pre, log_forget, init_memory[seq_index])
        per_head = readout.reshape(SEQUENCE_LENGTH, MEMORY_HEADS, DH)
        normalized = per_head * lax.rsqrt(lax.optimization_barrier(jnp.mean(per_head * per_head, axis=-1, keepdims=True)) + EPSILON)
        memory_out = normalized.reshape(SEQUENCE_LENGTH, HALF) * head_gain.astype(jnp.float32) * jax.nn.sigmoid(out_gate.astype(jnp.float32))
        memory_out = memory_out.astype(jnp.bfloat16)
        conv_product = (gate_in.astype(jnp.float32) * conv_input.astype(jnp.float32)).astype(jnp.bfloat16)
        conv_product = lax.optimization_barrier(conv_product).astype(jnp.float32)
        padded = jnp.pad(conv_product, ((TAPS - 1, 0), (0, 0)))
        mixed_conv = jnp.zeros((SEQUENCE_LENGTH, HALF), jnp.float32)
        for tap_index in range(TAPS):
            mixed_conv = mixed_conv + padded[tap_index:tap_index + SEQUENCE_LENGTH] * conv_taps[tap_index].astype(jnp.float32)
        conv_out = (gate_out.astype(jnp.float32) * mixed_conv).astype(jnp.bfloat16)
        summed = jnp.zeros((SEQUENCE_LENGTH, D), jnp.float32)
        for part_index in range(N_TP):
            low_col = part_index * group_width
            high_col = low_col + group_width
            partial_value = jnp.dot(memory_out[:, low_col:high_col], out_memory[low_col:high_col], preferred_element_type=jnp.float32)
            partial_value = partial_value + jnp.dot(conv_out[:, low_col:high_col], out_conv[low_col:high_col], preferred_element_type=jnp.float32)
            summed = summed + lax.optimization_barrier(partial_value.astype(jnp.bfloat16)).astype(jnp.float32)
        outputs.append(summed.astype(jnp.bfloat16))
    return jnp.stack(outputs)
```

```python
import math

import jax
import jax.numpy as jnp
from jax import lax
from jax.experimental import pallas as pl
from jax.experimental.pallas import tpu as pltpu
from jax.sharding import Mesh
from jax.sharding import PartitionSpec as P

BF = jnp.bfloat16
F32 = jnp.float32
BLOCK = 128
DH = 128
HEADS = 4
ROWS = 512
NB = 4
WIDTH = 512
D = 2048
EPSILON = 1e-06
LOWEST_LOG = -1e30
KEY_FACTOR = DH ** (-0.5)
LOG_KEY_FACTOR = math.log(KEY_FACTOR)
PAY = 544
SP = ("sp_0", "sp_1")
V = pl.BlockSpec(memory_space=pltpu.VMEM)
ANY = pl.BlockSpec(memory_space=pl.ANY)
SM = pl.BlockSpec(memory_space=pltpu.SMEM)
MIB = 2**20


def sds(shape, dtype=BF):
    return jax.ShapeDtypeStruct(shape, dtype)


def call(body, name, in_specs, outs, scratch=(), flops=0, vmem=16, nbytes=4 * MIB):
    return pl.pallas_call(
        body,
        name=name,
        in_specs=in_specs,
        out_specs=[V] * len(outs),
        out_shape=outs,
        scratch_shapes=list(scratch),
        compiler_params=pltpu.CompilerParams(vmem_limit_bytes=vmem * MIB),
        cost_estimate=pl.CostEstimate(flops=flops, bytes_accessed=nbytes, transcendentals=0),
    )


def dot(a, b):
    return jnp.dot(a, b, preferred_element_type=F32)


def dot_nt(a, b):
    return lax.dot_general(a, b, (((1,), (1,)), ((), ())), preferred_element_type=F32)


def norm_rows(x_ref, n_ref, gain, start, count):
    @pl.loop(start // 16, (start + count) // 16)
    def _(i):
        rows = pl.ds(pl.multiple_of(i * 16, 16), 16)
        x = x_ref[rows, :].astype(F32)
        scale = lax.rsqrt(jnp.mean(x * x, axis=-1, keepdims=True) + EPSILON)
        n_ref[rows, :] = (x * scale * gain).astype(BF)


def project(n_ref, w, out_ref):
    for j in range(WIDTH // 256):
        cols = slice(j * 256, (j + 1) * 256)
        out_ref[:, cols] = dot(n_ref[...], w[:, cols]).astype(BF)


def gate_rows(wi_ref, wf_ref, n_ref, g_ref):
    wg = jnp.concatenate([wi_ref[...].astype(F32), wf_ref[...].astype(F32)], axis=0).astype(BF)
    g_ref[...] = dot_nt(wg, n_ref[...])


def k1_body(t_hbm, gain_ref, wi_ref, wf_ref, wk_hbm, wv_hbm, wq_hbm,
            n_ref, k_ref, v_ref, q_ref, g_ref, t_buf, w_buf, t_sem, w_sem):
    for i in range(4):
        rows = pl.ds(i * 128, 128)
        pltpu.make_async_copy(t_hbm.at[rows, :], t_buf.at[rows, :], t_sem.at[i]).start()
    weights = (wk_hbm, wv_hbm, wq_hbm)
    for i, w in enumerate(weights):
        pltpu.make_async_copy(w, w_buf.at[i], w_sem.at[i]).start()
    gain = gain_ref[...].astype(F32)
    for i in range(4):
        rows = pl.ds(i * 128, 128)
        pltpu.make_async_copy(t_hbm.at[rows, :], t_buf.at[rows, :], t_sem.at[i]).wait()
        norm_rows(t_buf, n_ref, gain, i * 128, 128)
    gate_rows(wi_ref, wf_ref, n_ref, g_ref)
    for i, out in enumerate((k_ref, v_ref, q_ref)):
        pltpu.make_async_copy(weights[i], w_buf.at[i], w_sem.at[i]).wait()
        project(n_ref, w_buf.at[i], out)


def log_sigmoid(v):
    x = jnp.exp(-jnp.abs(v))
    series = x * (1.0 - x * (0.5 - x * (1.0 / 3.0 - x * 0.25)))
    return jnp.minimum(v, 0.0) - jnp.where(x < 0.01, series, jnp.log(1.0 + x))


def lane_scan(x, op, fill):
    lane = lax.broadcasted_iota(jnp.int32, x.shape, 1)
    for sh in (1, 2, 4, 8, 16, 32, 64):
        x = op(x, jnp.where(lane >= sh, pltpu.roll(x, sh, 1), fill))
    return x


def split3(x):
    a = x.astype(BF).astype(F32)
    r = x - a
    b = r.astype(BF).astype(F32)
    return a, b, r - b


def write_scalars(pay_ref, ts):
    a, b, c = split3(ts)
    pay_ref[512:PAY, :] = jnp.concatenate([a, b, c, jnp.zeros_like(a)], axis=0).astype(BF)


def read_scalars(pay_ref):
    s = pay_ref[512:PAY, :].astype(F32)
    ts = s[0:8] + s[8:16] + s[16:24]
    return ts[0:4], ts[4:8]


def k2_body(t_ref, gain_ref, wi_ref, wf_ref, wk_ref, wv_ref, g_own_ref, k_own_ref, v_own_ref,
            fx_ref, ib_ref, fb_ref,
            n_ref, k_ref, v_ref, u_ref, cm_ref, tot_ref, bt_ref, term_ref, pay_ref,
            g_ref, i_s, f_s, ws_s, wb_s, ts_s):
    tp = lax.axis_index("tp")
    norm_rows(t_ref, n_ref, gain_ref[...].astype(F32), 0, ROWS)
    gate_rows(wi_ref, wf_ref, n_ref, g_ref)
    project(n_ref, wk_ref, k_ref)
    project(n_ref, wv_ref, v_ref)
    row = lax.broadcasted_iota(jnp.int32, (HEADS, ROWS), 0)
    first_core = jnp.full((HEADS, ROWS), tp, jnp.int32) == 0

    def column(ref):
        out = jnp.full((HEADS, ROWS), ref[tp * HEADS], F32)
        for h in range(1, HEADS):
            out = jnp.where(row == h, ref[tp * HEADS + h], out)
        return out

    in_bias, forget_bias = column(ib_ref), column(fb_ref)
    for half in range(2):
        if half == 0:
            g = [jnp.where(first_core, g_own_ref[4 * a : 4 * a + 4, :], g_ref[4 * a : 4 * a + 4, :]) for a in range(4)]
        else:
            g = [jnp.where(first_core, g_ref[4 * a : 4 * a + 4, :], g_own_ref[4 * a : 4 * a + 4, :]) for a in range(4)]
        in_pre = jnp.where(first_core, g[0], g[1]) + in_bias
        forget_pre = jnp.where(first_core, g[2], g[3]) + forget_bias
        lf = log_sigmoid(forget_pre) + fx_ref[:, half * ROWS : (half + 1) * ROWS]
        for j in range(NB):
            b = half * NB + j
            i_s[b * 4 : b * 4 + 4, :] = in_pre[:, j * BLOCK : (j + 1) * BLOCK]
            f_s[b * 4 : b * 4 + 4, :] = lf[:, j * BLOCK : (j + 1) * BLOCK]
    cum = lane_scan(f_s[...], jnp.add, 0.0)
    u = i_s[...] - cum
    cmax = lane_scan(u, jnp.maximum, -jnp.inf)
    tot = jnp.broadcast_to(cum[:, BLOCK - 1 :], cum.shape)
    top = tot + jnp.broadcast_to(cmax[:, BLOCK - 1 :], cum.shape)
    u_ref[...] = u + LOG_KEY_FACTOR
    cm_ref[...] = cmax
    tot_ref[...] = tot
    bt_ref[...] = top
    ws_s[...] = jnp.exp(tot + u - top) * KEY_FACTOR
    suffix = jnp.zeros((HEADS, BLOCK), F32)
    scale = jnp.full((HEADS, BLOCK), LOWEST_LOG, F32)
    for b in reversed(range(2 * NB)):
        e = suffix + bt_ref[b * 4 : b * 4 + 4, :]
        wb_s[b * 4 : b * 4 + 4, :] = e
        scale = jnp.maximum(scale, e)
        suffix = suffix + tot_ref[b * 4 : b * 4 + 4, :]
    for b in range(2 * NB):
        wb_s[b * 4 : b * 4 + 4, :] = jnp.exp(wb_s[b * 4 : b * 4 + 4, :] - scale)
    ts_s[0:4, :] = suffix
    ts_s[4:8, :] = scale
    write_scalars(pay_ref, ts_s[...])
    for h in range(HEADS):
        cols = slice(h * DH, (h + 1) * DH)
        total = jnp.zeros((DH, DH), F32)
        for slot, (kr, vr) in enumerate(((k_own_ref, v_own_ref), (k_ref, v_ref))):
            half = tp if slot == 0 else 1 - tp
            for j in range(NB):
                rows = slice(j * BLOCK, (j + 1) * BLOCK)
                r = half * 16 + (j * 4 + h)
                kt = kr[rows, cols].T.astype(F32) * ws_s[pl.ds(r, 1), :]
                term = dot(kt.astype(BF), vr[rows, cols])
                term_ref[r] = term
                total = total + wb_s[pl.ds(r, 1), :] * term
        pay_ref[h * DH : (h + 1) * DH, :] = total.astype(BF)


def k3a_body(n_own_ref, n_oth_ref, wi_ref, wc_ref, wq_ref, wo_ref,
             cp_own_ref, cp_oth_ref, q_ref, og_own_ref, og_oth_ref, rim_ref):
    tp = lax.axis_index("tp")
    for n_ref, cp_ref in ((n_own_ref, cp_own_ref), (n_oth_ref, cp_oth_ref)):
        for j in range(2):
            cols = slice(j * 256, (j + 1) * 256)
            a = dot(n_ref[...], wi_ref[:, cols]).astype(BF).astype(F32)
            c = dot(n_ref[...], wc_ref[:, cols]).astype(BF).astype(F32)
            cp_ref[:, cols] = (a * c).astype(BF)
    own_last = jnp.full((16, WIDTH), tp, jnp.int32) == 1
    rim_ref[...] = jnp.where(own_last, cp_own_ref[ROWS - 16 :, :].astype(F32), cp_oth_ref[ROWS - 16 :, :].astype(F32)).astype(BF)
    project(n_oth_ref, wq_ref, q_ref)
    project(n_own_ref, wo_ref, og_own_ref)
    project(n_oth_ref, wo_ref, og_oth_ref)


def c1_body(own_ref, r1_ref, r2_ref, r3_ref, pm_ref, ps_ref, pay_ref, ts_s):
    x = lax.axis_index("sp_1")
    refs = (own_ref, r1_ref, r2_ref, r3_ref)
    place = [x] + [lax.rem(x + 4 - d, 4) for d in (1, 2, 3)]
    scal = [read_scalars(r) for r in refs]
    low = jnp.full((HEADS, BLOCK), LOWEST_LOG, F32)
    xv = jnp.full((HEADS, BLOCK), x, jnp.int32)
    suffix = jnp.zeros((HEADS, BLOCK), F32)
    levels = []
    for d in (1, 2, 3):
        levels.append(jnp.where(xv >= d, scal[d][1] + suffix, low))
        suffix = suffix + jnp.where(xv >= d, scal[d][0], 0.0)
    top = jnp.maximum(jnp.maximum(levels[0], levels[1]), levels[2])
    pw = [jnp.where(xv >= d, jnp.exp(levels[d - 1] - top), 0.0) for d in (1, 2, 3)]
    ps_ref[0:4, :] = suffix
    ps_ref[4:8, :] = top
    levels = []
    for a in range(4):
        level = scal[a][1]
        for b in range(4):
            if a != b:
                later = jnp.full((HEADS, BLOCK), place[b] - place[a], jnp.int32) > 0
                level = level + jnp.where(later, scal[b][0], 0.0)
        levels.append(level)
    rtop = jnp.maximum(jnp.maximum(levels[0], levels[1]), jnp.maximum(levels[2], levels[3]))
    rw = [jnp.exp(level - rtop) for level in levels]
    ts_s[0:4, :] = scal[0][0] + scal[1][0] + scal[2][0] + scal[3][0]
    ts_s[4:8, :] = rtop
    write_scalars(pay_ref, ts_s[...])
    for h in range(HEADS):
        rows = slice(h * DH, (h + 1) * DH)
        m = [r[rows, :].astype(F32) for r in refs]
        one = slice(h, h + 1)
        pm_ref[rows, :] = pw[0][one] * m[1] + pw[1][one] * m[2] + pw[2][one] * m[3]
        pay_ref[rows, :] = (rw[0][one] * m[0] + rw[1][one] * m[1] + rw[2][one] * m[2] + rw[3][one] * m[3]).astype(BF)


def slot_rows(ref, half):
    return ref[pl.ds(pl.multiple_of(half * 16, 16), 16), :]


def columns_of(rows16, pad_s):
    pad_s[0:16, :] = rows16
    return pad_s[...].T


def intra_half(q_ref, k_ref, v_ref, u_ref, cm_ref, half, out_ref, pad_s):
    cmt = columns_of(slot_rows(cm_ref, half), pad_s)
    causal = lax.broadcasted_iota(jnp.int32, (BLOCK, BLOCK), 1) <= lax.broadcasted_iota(jnp.int32, (BLOCK, BLOCK), 0)
    for j in range(NB):
        rows = slice(j * BLOCK, (j + 1) * BLOCK)
        for h in range(HEADS):
            cols = slice(h * DH, (h + 1) * DH)
            c = j * 4 + h
            scores = dot_nt(q_ref[rows, cols], k_ref[rows, cols])
            log = u_ref[pl.ds(half * 16 + c, 1), :] - cmt[:, c : c + 1]
            weight = jnp.exp(jnp.where(causal, log, -jnp.inf)) * scores
            out_ref[rows, cols] = dot(weight.astype(BF), v_ref[rows, cols])


def k3b_body(n_own_ref, n_oth_ref, wg_ref, q_own_ref, q_oth_ref, k_own_ref, k_oth_ref,
             v_own_ref, v_oth_ref, u_ref, cm_ref,
             go_own_ref, go_oth_ref, in_own_ref, in_oth_ref, pad_s):
    tp = lax.axis_index("tp")
    pad_s[...] = jnp.zeros_like(pad_s)
    project(n_own_ref, wg_ref, go_own_ref)
    intra_half(q_own_ref, k_own_ref, v_own_ref, u_ref, cm_ref, tp, in_own_ref, pad_s)
    project(n_oth_ref, wg_ref, go_oth_ref)
    intra_half(q_oth_ref, k_oth_ref, v_oth_ref, u_ref, cm_ref, 1 - tp, in_oth_ref, pad_s)


def readout_half(q_ref, in_ref, og_ref, st_ref, sc_ref, cm_ref, gain_ref, half, out_ref, pad_s):
    tp = lax.axis_index("tp")
    cm = slot_rows(cm_ref, half)
    sc = slot_rows(sc_ref, half)
    m = jnp.maximum(cm, sc)
    e_in = columns_of(jnp.exp(cm - m), pad_s)
    e_carry = columns_of(jnp.exp(sc - m), pad_s)
    gain = gain_ref[0:1, pl.ds(pl.multiple_of(tp * WIDTH, WIDTH), WIDTH)].astype(F32)
    for j in range(NB):
        rows = slice(j * BLOCK, (j + 1) * BLOCK)
        for h in range(HEADS):
            cols = slice(h * DH, (h + 1) * DH)
            c = j * 4 + h
            carried = dot(q_ref[rows, cols], st_ref[half * 16 + c])
            read = e_carry[:, c : c + 1] * carried + e_in[:, c : c + 1] * in_ref[rows, cols]
            scale = lax.rsqrt(jnp.mean(read * read, axis=-1, keepdims=True) + EPSILON)
            gate = jax.nn.sigmoid(og_ref[rows, cols].astype(F32))
            out_ref[rows, cols] = (read * scale * gain[:, cols] * gate).astype(BF)


def conv_half(cp_ref, before_ref, rim_ref, go_ref, taps_ref, half, out_ref, buf_s):
    tp = lax.axis_index("tp")
    first = jnp.full((16, WIDTH), half, jnp.int32) == 0
    taps = taps_ref[:, pl.ds(pl.multiple_of(tp * WIDTH, WIDTH), WIDTH)].astype(F32)
    before = jnp.where(first, rim_ref[...].astype(F32), before_ref[ROWS - 16 :, :].astype(F32))
    buf_s[0:16, :] = before
    for r in range(0, ROWS, 64):
        buf_s[16 + r : 80 + r, :] = cp_ref[r : r + 64, :].astype(F32)
        mixed = buf_s[14 + r : 78 + r, :] * taps[0:1]
        mixed = mixed + buf_s[15 + r : 79 + r, :] * taps[1:2]
        mixed = mixed + buf_s[16 + r : 80 + r, :] * taps[2:3]
        out_ref[r : r + 64, WIDTH:] = (go_ref[r : r + 64, :].astype(F32) * mixed).astype(BF)


def out_project(a_ref, wm_ref, wc_ref, store):
    for j in range(D // 256):
        cols = slice(j * 256, (j + 1) * 256)
        store(cols, dot(a_ref[:, :WIDTH], wm_ref[:, cols]) + dot(a_ref[:, WIDTH:], wc_ref[:, cols]))


def k4_body(pm_ref, ps_ref, r1_ref, r2_ref, r3_ref, init_ref, tot_ref, bt_ref, term_ref,
            q_ref, in_ref, og_ref, cm_ref, gain_ref, cp_ref, cp_own_ref, rim_ref, go_ref, taps_ref,
            wm_ref, wc_ref,
            send_ref, st_ref, sc_ref, a_s, pad_s, buf_s, cs_s):
    tp = lax.axis_index("tp")
    z = lax.axis_index("sp_0")
    half = 1 - tp
    pad_s[...] = jnp.zeros_like(pad_s)
    refs = (r1_ref, r2_ref, r3_ref)
    zv = jnp.full((HEADS, BLOCK), z, jnp.int32)
    low = jnp.full((HEADS, BLOCK), LOWEST_LOG, F32)
    suffix = ps_ref[0:4, :]
    levels = [ps_ref[4:8, :]]
    for d in (1, 2, 3):
        t, s = read_scalars(refs[d - 1])
        levels.append(jnp.where(zv >= d, s + suffix, low))
        suffix = suffix + jnp.where(zv >= d, t, 0.0)
    levels.append(suffix)
    top = levels[0]
    for level in levels[1:]:
        top = jnp.maximum(top, level)
    w = [jnp.exp(level - top) for level in levels]
    for b in range(2 * NB):
        cs_s[b * 4 : b * 4 + 4, :] = top
        tot = tot_ref[b * 4 : b * 4 + 4, :] + top
        bt = bt_ref[b * 4 : b * 4 + 4, :]
        top = jnp.maximum(tot, bt)
        cs_s[32 + b * 4 : 36 + b * 4, :] = jnp.exp(tot - top)
        cs_s[64 + b * 4 : 68 + b * 4, :] = jnp.exp(bt - top)
    sc_ref[...] = cs_s[0:32, :]
    for h in range(HEADS):
        rows = slice(h * DH, (h + 1) * DH)
        one = slice(h, h + 1)
        mem = w[0][one] * pm_ref[rows, :] + w[4][one] * init_ref[h]
        for d in (1, 2, 3):
            mem = mem + w[d][one] * refs[d - 1][rows, :].astype(F32)
        for b in range(2 * NB):
            r = b * 4 + h
            st_ref[r] = mem.astype(BF)
            if b < 2 * NB - 1:
                mem = cs_s[32 + r : 33 + r, :] * mem + cs_s[64 + r : 65 + r, :] * term_ref[r]
    readout_half(q_ref, in_ref, og_ref, st_ref, sc_ref, cm_ref, gain_ref, half, a_s, pad_s)
    conv_half(cp_ref, cp_own_ref, rim_ref, go_ref, taps_ref, half, a_s, buf_s)

    def store(cols, value):
        send_ref[:, cols] = value.astype(BF)

    out_project(a_s, wm_ref, wc_ref, store)


def k5a_body(q_ref, in_ref, og_ref, st_ref, sc_ref, cm_ref, gain_ref, cp_ref, cp_oth_ref, rim_ref, go_ref, taps_ref,
             a_ref, pad_s, buf_s):
    tp = lax.axis_index("tp")
    pad_s[...] = jnp.zeros_like(pad_s)
    readout_half(q_ref, in_ref, og_ref, st_ref, sc_ref, cm_ref, gain_ref, tp, a_ref, pad_s)
    conv_half(cp_ref, cp_oth_ref, rim_ref, go_ref, taps_ref, tp, a_ref, buf_s)


def k5b_body(a_ref, recv_ref, wm_ref, wc_ref, out_ref):
    def store(cols, value):
        out_ref[:, cols] = (value.astype(BF).astype(F32) + recv_ref[:, cols].astype(F32)).astype(BF)

    out_project(a_ref, wm_ref, wc_ref, store)


def rotated(value, axis, distance):
    size = lax.axis_size(axis)
    return lax.ppermute(value, axis, [(i, (i + distance) % size) for i in range(size)])


def local(
    tokens, norm_gain, w_query, w_key, w_value, w_outgate, w_gatein, w_gateout, w_convin,
    w_igate, w_fgate, input_bias, forget_bias, forget_extra, init_memory, head_gain, conv_taps,
    out_memory, out_conv,
):
    own = tokens[0]
    other = rotated(own, "tp", 1)
    gain = norm_gain.reshape(1, D)
    hgain = head_gain.reshape(1, 2 * WIDTH)
    wi, wf = w_igate.T, w_fgate.T
    fx = forget_extra[0].T
    half_act = sds((ROWS, WIDTH))
    gflop = 2 * ROWS * D * WIDTH
    n_own, k_own, v_own, q_own, g_own = call(
        k1_body, "k1", [ANY, V, V, V, ANY, ANY, ANY],
        [sds((ROWS, D)), half_act, half_act, half_act, sds((16, ROWS), F32)],
        [pltpu.VMEM((ROWS, D), BF), pltpu.VMEM((3, D, WIDTH), BF), pltpu.SemaphoreType.DMA((4,)), pltpu.SemaphoreType.DMA((3,))],
        flops=3 * gflop, vmem=20,
    )(own, gain, wi, wf, w_key, w_value, w_query)
    rows32 = sds((32, BLOCK), F32)
    n_oth, k_oth, v_oth, u, cm, tot, bt, terms, pay = call(
        k2_body, "k2", [V] * 10 + [SM, SM],
        [sds((ROWS, D)), half_act, half_act, rows32, rows32, rows32, rows32, sds((32, DH, DH), F32), sds((PAY, DH))],
        [pltpu.VMEM((16, ROWS), F32)] + [pltpu.VMEM((32, BLOCK), F32)] * 4 + [pltpu.VMEM((8, BLOCK), F32)],
        flops=2 * gflop,
    )(other, gain, wi, wf, w_key, w_value, g_own, k_own, v_own, fx, input_bias, forget_bias)
    first = [rotated(pay, "sp_1", d) for d in (1, 2, 3)]
    cp_own, cp_oth, q_oth, og_own, og_oth, rim = call(
        k3a_body, "k3a", [V] * 6, [half_act] * 5 + [sds((16, WIDTH))], flops=7 * gflop,
    )(n_own, n_oth, w_gatein, w_convin, w_query, w_outgate)
    chain = [(i, i + 1) for i in range(15)]
    rim = lax.ppermute(rim, SP, chain)
    pm, ps, pay2 = call(
        c1_body, "c1", [V] * 4, [sds((512, DH), F32), sds((8, BLOCK), F32), sds((PAY, DH))],
        [pltpu.VMEM((8, BLOCK), F32)], flops=2**20, vmem=8,
    )(pay, *first)
    second = [rotated(pay2, "sp_0", d) for d in (1, 2, 3)]
    go_own, go_oth, in_own, in_oth = call(
        k3b_body, "k3b", [V] * 11, [half_act, half_act, sds((ROWS, WIDTH), F32), sds((ROWS, WIDTH), F32)],
        [pltpu.VMEM((BLOCK, BLOCK), F32)], flops=4 * gflop,
    )(n_own, n_oth, w_gateout, q_own, q_oth, k_own, k_oth, v_own, v_oth, u, cm)
    send, states, scales = call(
        k4_body, "k4", [V] * 21, [sds((ROWS, D)), sds((32, DH, DH)), rows32],
        [pltpu.VMEM((ROWS, 2 * WIDTH), BF), pltpu.VMEM((BLOCK, BLOCK), F32), pltpu.VMEM((ROWS + 16, WIDTH), F32), pltpu.VMEM((96, BLOCK), F32)],
        flops=3 * gflop,
    )(pm, ps, *second, init_memory[0], tot, bt, terms, q_oth, in_oth, og_oth, cm, hgain, cp_oth, cp_own, rim, go_oth,
      conv_taps, out_memory, out_conv)
    recv = rotated(send, "tp", 1)
    (act,) = call(
        k5a_body, "k5a", [V] * 12, [sds((ROWS, 2 * WIDTH))],
        [pltpu.VMEM((BLOCK, BLOCK), F32), pltpu.VMEM((ROWS + 16, WIDTH), F32)], flops=gflop,
    )(q_own, in_own, og_own, states, scales, cm, hgain, cp_own, cp_oth, rim, go_own, conv_taps)
    (out,) = call(k5b_body, "k5b", [V] * 4, [sds((ROWS, D))], flops=2 * gflop)(act, recv, out_memory, out_conv)
    return out[None]


def solution(mesh):
    finer = Mesh(
        mesh.devices.reshape(4, 4, mesh.shape["fs"], mesh.shape["tp"]), ("sp_0", "sp_1", "fs", "tp")
    )
    sp_tp = ("sp_0", "sp_1", "tp")
    by_col = P(None, "tp")
    return jax.shard_map(
        local,
        mesh=finer,
        in_specs=(
            P("fs", sp_tp, None), P(), by_col, by_col, by_col, by_col, by_col, by_col, by_col,
            P(), P(), P(), P(), P("fs", SP, "tp"), P("fs", "tp", None, None), P(), P(),
            P("tp", None), P("tp", None),
        ),
        out_specs=P("fs", sp_tp, None),
        check_vma=False,
    )
```

```python
import math

import jax
import jax.numpy as jnp
from jax import lax
from jax.experimental import pallas as pl
from jax.experimental.pallas import tpu as pltpu
from jax.sharding import Mesh
from jax.sharding import PartitionSpec as P

BF = jnp.bfloat16
F32 = jnp.float32
BLOCK = 128
DH = 128
HEADS = 4
ROWS = 512
NB = 4
WIDTH = 512
D = 2048
EPSILON = 1e-06
LOWEST_LOG = -1e30
KEY_FACTOR = DH ** (-0.5)
LOG_KEY_FACTOR = math.log(KEY_FACTOR)
PAY = 544
SP = ("sp_0", "sp_1")
V = pl.BlockSpec(memory_space=pltpu.VMEM)
HBM = pl.BlockSpec(memory_space=pltpu.HBM)
SM = pl.BlockSpec(memory_space=pltpu.SMEM)
MIB = 2**20


def sds(shape, dtype=BF):
    return jax.ShapeDtypeStruct(shape, dtype)


def call(body, name, in_specs, outs, scratch=(), flops=0, vmem=16, nbytes=4 * MIB):
    return pl.pallas_call(
        body,
        name=name,
        in_specs=in_specs,
        out_specs=[V] * len(outs),
        out_shape=outs,
        scratch_shapes=list(scratch),
        compiler_params=pltpu.CompilerParams(vmem_limit_bytes=vmem * MIB),
        cost_estimate=pl.CostEstimate(flops=flops, bytes_accessed=nbytes, transcendentals=0),
    )


def dot(a, b):
    return jnp.dot(a, b, preferred_element_type=F32)


def dot_nt(a, b):
    return lax.dot_general(a, b, (((1,), (1,)), ((), ())), preferred_element_type=F32)


def norm_rows(x_ref, n_ref, gain, start, count):
    groups = 8

    @pl.loop(start // (16 * groups), (start + count) // (16 * groups))
    def _(i):
        scales = []
        for g in range(groups):
            rows = pl.ds(pl.multiple_of(i * (16 * groups) + g * 16, 16), 16)
            x = x_ref[rows, :].astype(F32)
            scales.append(lax.rsqrt(jnp.mean(x * x, axis=-1, keepdims=True) + EPSILON))
        for g in range(groups):
            rows = pl.ds(pl.multiple_of(i * (16 * groups) + g * 16, 16), 16)
            n_ref[rows, :] = (x_ref[rows, :].astype(F32) * scales[g] * gain).astype(BF)


def project(n_ref, w, out_ref):
    for j in range(WIDTH // 256):
        cols = slice(j * 256, (j + 1) * 256)
        out_ref[:, cols] = dot(n_ref[...], w[:, cols]).astype(BF)


def gate_rows(wi_ref, wf_ref, n_ref, g_ref):
    wg = jnp.concatenate([wi_ref[...].astype(F32), wf_ref[...].astype(F32)], axis=0).astype(BF)
    g_ref[...] = dot_nt(wg, n_ref[...])


def k1_body(t_hbm, gain_ref, wi_ref, wf_ref, wk_hbm, wv_hbm,
            n_ref, k_ref, v_ref, g_ref, t_buf, w_buf, t_sem, w_sem):
    for i in range(4):
        rows = pl.ds(i * 128, 128)
        pltpu.make_async_copy(t_hbm.at[rows, :], t_buf.at[rows, :], t_sem.at[i]).start()
    weights = (wk_hbm, wv_hbm)
    for i, w in enumerate(weights):
        pltpu.make_async_copy(w, w_buf.at[i], w_sem.at[i]).start()
    gain = gain_ref[...].astype(F32).reshape(1, D)
    for i in range(4):
        rows = pl.ds(i * 128, 128)
        pltpu.make_async_copy(t_hbm.at[rows, :], t_buf.at[rows, :], t_sem.at[i]).wait()
        norm_rows(t_buf, n_ref, gain, i * 128, 128)
    gate_rows(wi_ref, wf_ref, n_ref, g_ref)
    for i, out in enumerate((k_ref, v_ref)):
        pltpu.make_async_copy(weights[i], w_buf.at[i], w_sem.at[i]).wait()
        project(n_ref, w_buf.at[i], out)


def log_sigmoid(v):
    x = jnp.exp(-jnp.abs(v))
    series = x * (1.0 - x * (0.5 - x * (1.0 / 3.0 - x * 0.25)))
    return jnp.minimum(v, 0.0) - jnp.where(x < 0.01, series, jnp.log(1.0 + x))


def lane_scan(x, op, fill):
    lane = lax.broadcasted_iota(jnp.int32, x.shape, 1)
    for sh in (1, 2, 4, 8, 16, 32, 64):
        x = op(x, jnp.where(lane >= sh, pltpu.roll(x, sh, 1), fill))
    return x


def split3(x):
    a = x.astype(BF).astype(F32)
    r = x - a
    b = r.astype(BF).astype(F32)
    return a, b, r - b


def write_scalars(pay_ref, ts, rim):
    a, b, c = split3(ts)
    pay_ref[512:PAY, :] = jnp.concatenate([a, b, c, rim], axis=0).astype(BF)


def read_scalars(pay_ref):
    s = pay_ref[512:PAY, :].astype(F32)
    ts = s[0:8] + s[8:16] + s[16:24]
    return ts[0:4], ts[4:8]


def k2_body(t_ref, gain_ref, wi_ref, wf_ref, wk_ref, wv_ref, g_own_ref, k_own_ref, v_own_ref,
            fx_ref, ib_ref, fb_ref, n_own_ref, win_ref, wcv_ref,
            n_ref, k_ref, v_ref, kt_ref, u_ref, cm_ref, tot_ref, bt_ref, term_ref, pay_ref,
            g_ref, i_s, f_s, ws_s, wb_s, ts_s):
    tp = lax.axis_index("tp")
    norm_rows(t_ref, n_ref, gain_ref[...].astype(F32).reshape(1, D), 0, ROWS)
    own_last = jnp.full((16, D), tp, jnp.int32) == 1
    last = jnp.where(own_last, n_own_ref[ROWS - 16 :, :].astype(F32), n_ref[ROWS - 16 :, :].astype(F32)).astype(BF)
    rim = dot(last, win_ref[...]).astype(BF).astype(F32) * dot(last, wcv_ref[...]).astype(BF).astype(F32)
    rim = jnp.concatenate([rim[14 + r : 15 + r, c * 128 : (c + 1) * 128] for r in range(2) for c in range(4)], axis=0)
    gate_rows(wi_ref, wf_ref, n_ref, g_ref)
    project(n_ref, wk_ref, k_ref)
    project(n_ref, wv_ref, v_ref)
    row = lax.broadcasted_iota(jnp.int32, (HEADS, ROWS), 0)
    first_core = jnp.full((HEADS, ROWS), tp, jnp.int32) == 0

    def column(ref):
        out = jnp.full((HEADS, ROWS), ref[tp * HEADS], F32)
        for h in range(1, HEADS):
            out = jnp.where(row == h, ref[tp * HEADS + h], out)
        return out

    in_bias, forget_bias = column(ib_ref), column(fb_ref)
    for half in range(2):
        if half == 0:
            g = [jnp.where(first_core, g_own_ref[4 * a : 4 * a + 4, :], g_ref[4 * a : 4 * a + 4, :]) for a in range(4)]
        else:
            g = [jnp.where(first_core, g_ref[4 * a : 4 * a + 4, :], g_own_ref[4 * a : 4 * a + 4, :]) for a in range(4)]
        in_pre = jnp.where(first_core, g[0], g[1]) + in_bias
        forget_pre = jnp.where(first_core, g[2], g[3]) + forget_bias
        lf = log_sigmoid(forget_pre) + fx_ref[:, half * ROWS : (half + 1) * ROWS]
        for j in range(NB):
            b = half * NB + j
            i_s[b * 4 : b * 4 + 4, :] = in_pre[:, j * BLOCK : (j + 1) * BLOCK]
            f_s[b * 4 : b * 4 + 4, :] = lf[:, j * BLOCK : (j + 1) * BLOCK]
    cum = lane_scan(f_s[...], jnp.add, 0.0)
    u = i_s[...] - cum
    cmax = lane_scan(u, jnp.maximum, -jnp.inf)
    tot = jnp.broadcast_to(cum[:, BLOCK - 1 :], cum.shape)
    top = tot + jnp.broadcast_to(cmax[:, BLOCK - 1 :], cum.shape)
    u_ref[...] = u + LOG_KEY_FACTOR
    cm_ref[...] = cmax
    tot_ref[...] = tot
    bt_ref[...] = top
    ws_s[...] = jnp.exp(tot + u - top) * KEY_FACTOR
    suffix = jnp.zeros((HEADS, BLOCK), F32)
    scale = jnp.full((HEADS, BLOCK), LOWEST_LOG, F32)
    for b in reversed(range(2 * NB)):
        e = suffix + bt_ref[b * 4 : b * 4 + 4, :]
        wb_s[b * 4 : b * 4 + 4, :] = e
        scale = jnp.maximum(scale, e)
        suffix = suffix + tot_ref[b * 4 : b * 4 + 4, :]
    for b in range(2 * NB):
        wb_s[b * 4 : b * 4 + 4, :] = jnp.exp(wb_s[b * 4 : b * 4 + 4, :] - scale)
    ts_s[0:4, :] = suffix
    ts_s[4:8, :] = scale
    write_scalars(pay_ref, ts_s[...], rim)
    for h in range(HEADS):
        cols = slice(h * DH, (h + 1) * DH)
        total = jnp.zeros((DH, DH), F32)
        for slot, (kr, vr) in enumerate(((k_own_ref, v_own_ref), (k_ref, v_ref))):
            half = tp if slot == 0 else 1 - tp
            for j in range(NB):
                rows = slice(j * BLOCK, (j + 1) * BLOCK)
                r = half * 16 + (j * 4 + h)
                kt = kr[rows, cols].T
                kt_ref[r] = kt
                term = dot((kt.astype(F32) * ws_s[pl.ds(r, 1), :]).astype(BF), vr[rows, cols])
                term_ref[r] = term
                total = total + wb_s[pl.ds(r, 1), :] * term
        pay_ref[h * DH : (h + 1) * DH, :] = total.astype(BF)


def k3a_body(n_own_ref, n_oth_ref, wi_ref, wc_ref, wq_ref, cp_own_ref, cp_oth_ref, q_own_ref, q_oth_ref):
    for n_ref, cp_ref in ((n_own_ref, cp_own_ref), (n_oth_ref, cp_oth_ref)):
        for j in range(2):
            cols = slice(j * 256, (j + 1) * 256)
            a = dot(n_ref[...], wi_ref[:, cols]).astype(BF).astype(F32)
            c = dot(n_ref[...], wc_ref[:, cols]).astype(BF).astype(F32)
            cp_ref[:, cols] = (a * c).astype(BF)
    project(n_own_ref, wq_ref, q_own_ref)
    project(n_oth_ref, wq_ref, q_oth_ref)


def c1_body(own_ref, r1_ref, r2_ref, r3_ref, pm_ref, ps_ref, pay_ref, ts_s):
    x = lax.axis_index("sp_1")
    refs = (own_ref, r1_ref, r2_ref, r3_ref)
    place = [x] + [lax.rem(x + 4 - d, 4) for d in (1, 2, 3)]
    scal = [read_scalars(r) for r in refs]
    low = jnp.full((HEADS, BLOCK), LOWEST_LOG, F32)
    xv = jnp.full((HEADS, BLOCK), x, jnp.int32)
    suffix = jnp.zeros((HEADS, BLOCK), F32)
    levels = []
    for d in (1, 2, 3):
        levels.append(jnp.where(xv >= d, scal[d][1] + suffix, low))
        suffix = suffix + jnp.where(xv >= d, scal[d][0], 0.0)
    top = jnp.maximum(jnp.maximum(levels[0], levels[1]), levels[2])
    pw = [jnp.where(xv >= d, jnp.exp(levels[d - 1] - top), 0.0) for d in (1, 2, 3)]
    ps_ref[0:4, :] = suffix
    ps_ref[4:8, :] = top
    levels = []
    for a in range(4):
        level = scal[a][1]
        for b in range(4):
            if a != b:
                later = jnp.full((HEADS, BLOCK), place[b] - place[a], jnp.int32) > 0
                level = level + jnp.where(later, scal[b][0], 0.0)
        levels.append(level)
    rtop = jnp.maximum(jnp.maximum(levels[0], levels[1]), jnp.maximum(levels[2], levels[3]))
    rw = [jnp.exp(level - rtop) for level in levels]
    ts_s[0:4, :] = scal[0][0] + scal[1][0] + scal[2][0] + scal[3][0]
    ts_s[4:8, :] = rtop
    write_scalars(pay_ref, ts_s[...], r1_ref[536:PAY, :].astype(F32))
    for h in range(HEADS):
        rows = slice(h * DH, (h + 1) * DH)
        m = [r[rows, :].astype(F32) for r in refs]
        one = slice(h, h + 1)
        pm_ref[rows, :] = pw[0][one] * m[1] + pw[1][one] * m[2] + pw[2][one] * m[3]
        pay_ref[rows, :] = (rw[0][one] * m[0] + rw[1][one] * m[1] + rw[2][one] * m[2] + rw[3][one] * m[3]).astype(BF)


def slot_rows(ref, half):
    return ref[pl.ds(pl.multiple_of(half * 16, 16), 16), :]


def columns_of(rows16, pad_s):
    pad_s[0:16, :] = rows16
    return pad_s[...].T


def scores_half(q_ref, kt_ref, half, s_s):
    for c in range(16):
        rows, cols = slice(c // 4 * BLOCK, (c // 4 + 1) * BLOCK), slice(c % 4 * DH, (c % 4 + 1) * DH)
        s_s[c * BLOCK : (c + 1) * BLOCK, :] = dot(q_ref[rows, cols], kt_ref[half * 16 + c])


def weights_half(u_ref, cm_ref, half, s_s, w_s, pad_s):
    cmt = columns_of(slot_rows(cm_ref, half), pad_s)
    causal = lax.broadcasted_iota(jnp.int32, (BLOCK, BLOCK), 1) <= lax.broadcasted_iota(jnp.int32, (BLOCK, BLOCK), 0)
    for c in range(16):
        rows = slice(c * BLOCK, (c + 1) * BLOCK)
        log = u_ref[pl.ds(half * 16 + c, 1), :] - cmt[:, c : c + 1]
        w_s[rows, :] = (jnp.exp(jnp.where(causal, log, -jnp.inf)) * s_s[rows, :]).astype(BF)


def intra_half(w_s, v_ref, out_ref):
    for c in range(16):
        rows, cols = slice(c // 4 * BLOCK, (c // 4 + 1) * BLOCK), slice(c % 4 * DH, (c % 4 + 1) * DH)
        out_ref[rows, cols] = dot(w_s[c * BLOCK : (c + 1) * BLOCK, :], v_ref[rows, cols])


def local_cols(ref, tp):
    return ref[..., pl.ds(pl.multiple_of(tp * WIDTH, WIDTH), WIDTH)].astype(F32)


def gate_half(n_ref, wo_ref, gain, out_ref):
    for j in range(WIDTH // 256):
        cols = slice(j * 256, (j + 1) * 256)
        raw = dot(n_ref[...], wo_ref[:, cols]).astype(BF).astype(F32)
        out_ref[:, cols] = jax.nn.sigmoid(raw) * gain[:, cols]


def conv_half(cp_ref, before_ref, go_ref, taps, out_ref, buf_s):
    buf_s[0:16, :] = before_ref[ROWS - 16 :, :].astype(F32)
    for r in range(0, ROWS, 64):
        buf_s[16 + r : 80 + r, :] = cp_ref[r : r + 64, :].astype(F32)
        mixed = buf_s[14 + r : 78 + r, :] * taps[0:1]
        mixed = mixed + buf_s[15 + r : 79 + r, :] * taps[1:2]
        mixed = mixed + buf_s[16 + r : 80 + r, :] * taps[2:3]
        out_ref[r : r + 64, :] = (go_ref[r : r + 64, :].astype(F32) * mixed).astype(BF)


def k3b_body(n_own_ref, n_oth_ref, wg_ref, wo_ref, q_own_ref, q_oth_ref, kt_ref,
             v_own_ref, v_oth_ref, u_ref, cm_ref, cp_own_ref, cp_oth_ref, gain_ref, taps_ref,
             go_own_ref, go_oth_ref, cv_own_ref, cv_oth_ref, sg_own_ref, sg_oth_ref, in_own_ref, in_oth_ref,
             pad_s, s_s, w_s, buf_s):
    tp = lax.axis_index("tp")
    pad_s[...] = jnp.zeros_like(pad_s)
    gain = local_cols(gain_ref, tp).reshape(1, WIDTH)
    taps = local_cols(taps_ref, tp)
    for slot, (q_ref, v_ref, n_ref, out, go_ref, sg_ref, cp_ref, before_ref, cv_ref) in enumerate((
        (q_own_ref, v_own_ref, n_own_ref, in_own_ref, go_own_ref, sg_own_ref, cp_own_ref, cp_oth_ref, cv_own_ref),
        (q_oth_ref, v_oth_ref, n_oth_ref, in_oth_ref, go_oth_ref, sg_oth_ref, cp_oth_ref, cp_own_ref, cv_oth_ref),
    )):
        half = tp if slot == 0 else 1 - tp
        scores_half(q_ref, kt_ref, half, s_s)
        project(n_ref, wg_ref, go_ref)
        weights_half(u_ref, cm_ref, half, s_s, w_s, pad_s)
        gate_half(n_ref, wo_ref, gain, sg_ref)
        intra_half(w_s, v_ref, out)
        conv_half(cp_ref, before_ref, go_ref, taps, cv_ref, buf_s)


def readout_half(q_ref, in_ref, sg_ref, st_ref, sc_ref, cm_ref, half, out_ref, pad_s, c_s):
    for c in range(16):
        rows, cols = slice(c // 4 * BLOCK, (c // 4 + 1) * BLOCK), slice(c % 4 * DH, (c % 4 + 1) * DH)
        c_s[c * BLOCK : (c + 1) * BLOCK, :] = dot(q_ref[rows, cols], st_ref[half * 16 + c])
    cm = slot_rows(cm_ref, half)
    sc = slot_rows(sc_ref, half)
    m = jnp.maximum(cm, sc)
    e_in = columns_of(jnp.exp(cm - m), pad_s)
    e_carry = columns_of(jnp.exp(sc - m), pad_s)
    for c in range(16):
        cols = slice(c % 4 * DH, (c % 4 + 1) * DH)
        for g in range(2):
            rows = slice(c // 4 * BLOCK + g * 64, c // 4 * BLOCK + g * 64 + 64)
            t = slice(g * 64, g * 64 + 64)
            read = e_carry[t, c : c + 1] * c_s[c * BLOCK + g * 64 : c * BLOCK + g * 64 + 64, :] + e_in[t, c : c + 1] * in_ref[rows, cols]
            scale = lax.rsqrt(jnp.mean(read * read, axis=-1, keepdims=True) + EPSILON)
            out_ref[rows, cols] = (read * scale * sg_ref[rows, cols]).astype(BF)


def conv_fix(cv_ref, cp_ref, go_ref, r1_ref, z1_ref, taps_ref, half, out_ref):
    tp = lax.axis_index("tp")
    x = lax.axis_index("sp_1")
    z = lax.axis_index("sp_0")
    here = jnp.full((8, BLOCK), x, jnp.int32)
    row = jnp.full((8, BLOCK), z, jnp.int32)
    rim8 = jnp.where(here > 0, r1_ref[536:PAY, :].astype(F32), jnp.where(row > 0, z1_ref[536:PAY, :].astype(F32), 0.0))
    rim = [jnp.concatenate([rim8[r * 4 + c : r * 4 + c + 1, :] for c in range(4)], axis=1) for r in range(2)]
    taps = local_cols(taps_ref, tp)
    p = jnp.concatenate([rim[0], rim[1], cp_ref[0:16, :].astype(F32)], axis=0)
    mixed = p[0:16] * taps[0:1] + p[1:17] * taps[1:2] + p[2:18] * taps[2:3]
    fixed = go_ref[0:16, :].astype(F32) * mixed
    first = jnp.full((16, WIDTH), half, jnp.int32) == 0
    out_ref[0:16, WIDTH:] = jnp.where(first, fixed, cv_ref[0:16, :].astype(F32)).astype(BF)
    out_ref[16:, WIDTH:] = cv_ref[16:, :]


def out_project(a_ref, wm_ref, wc_ref, store):
    for j in range(D // 256):
        cols = slice(j * 256, (j + 1) * 256)
        store(cols, dot(a_ref[:, :WIDTH], wm_ref[:, cols]) + dot(a_ref[:, WIDTH:], wc_ref[:, cols]))


def k4_body(pm_ref, ps_ref, r1_ref, r2_ref, r3_ref, x1_ref, init_ref, tot_ref, bt_ref, term_ref,
            q_ref, in_ref, sg_ref, cm_ref, cv_ref, cp_ref, go_ref, taps_ref, wm_ref, wc_ref,
            send_ref, st_ref, sc_ref, a_s, pad_s, c_s, cs_s):
    tp = lax.axis_index("tp")
    z = lax.axis_index("sp_0")
    half = 1 - tp
    pad_s[...] = jnp.zeros_like(pad_s)
    refs = (r1_ref, r2_ref, r3_ref)
    zv = jnp.full((HEADS, BLOCK), z, jnp.int32)
    low = jnp.full((HEADS, BLOCK), LOWEST_LOG, F32)
    suffix = ps_ref[0:4, :]
    levels = [ps_ref[4:8, :]]
    for d in (1, 2, 3):
        t, s = read_scalars(refs[d - 1])
        levels.append(jnp.where(zv >= d, s + suffix, low))
        suffix = suffix + jnp.where(zv >= d, t, 0.0)
    levels.append(suffix)
    top = levels[0]
    for level in levels[1:]:
        top = jnp.maximum(top, level)
    w = [jnp.exp(level - top) for level in levels]
    for b in range(2 * NB):
        cs_s[b * 4 : b * 4 + 4, :] = top
        tot = tot_ref[b * 4 : b * 4 + 4, :] + top
        bt = bt_ref[b * 4 : b * 4 + 4, :]
        top = jnp.maximum(tot, bt)
        cs_s[32 + b * 4 : 36 + b * 4, :] = jnp.exp(tot - top)
        cs_s[64 + b * 4 : 68 + b * 4, :] = jnp.exp(bt - top)
    sc_ref[...] = cs_s[0:32, :]
    for h in range(HEADS):
        rows = slice(h * DH, (h + 1) * DH)
        one = slice(h, h + 1)
        mem = w[0][one] * pm_ref[rows, :] + w[4][one] * init_ref[h]
        for d in (1, 2, 3):
            mem = mem + w[d][one] * refs[d - 1][rows, :].astype(F32)
        for b in range(2 * NB):
            r = b * 4 + h
            st_ref[r] = mem.astype(BF)
            if b < 2 * NB - 1:
                mem = cs_s[32 + r : 33 + r, :] * mem + cs_s[64 + r : 65 + r, :] * term_ref[r]
    conv_fix(cv_ref, cp_ref, go_ref, x1_ref, r1_ref, taps_ref, half, a_s)
    readout_half(q_ref, in_ref, sg_ref, st_ref, sc_ref, cm_ref, half, a_s, pad_s, c_s)

    def store(cols, value):
        send_ref[:, cols] = value.astype(BF)

    out_project(a_s, wm_ref, wc_ref, store)


def k5a_body(x1_ref, z1_ref, q_ref, in_ref, sg_ref, st_ref, sc_ref, cm_ref, cv_ref, cp_ref, go_ref, taps_ref, wm_ref, wc_ref,
             part_ref, a_s, pad_s, c_s):
    tp = lax.axis_index("tp")
    pad_s[...] = jnp.zeros_like(pad_s)
    conv_fix(cv_ref, cp_ref, go_ref, x1_ref, z1_ref, taps_ref, tp, a_s)
    readout_half(q_ref, in_ref, sg_ref, st_ref, sc_ref, cm_ref, tp, a_s, pad_s, c_s)

    def store(cols, value):
        part_ref[:, cols] = value.astype(BF)

    out_project(a_s, wm_ref, wc_ref, store)


def k5b_body(part_ref, recv_ref, out_ref):
    rows = pl.ds(pl.multiple_of(pl.program_id(0) * 128, 128), 128)
    out_ref[...] = (part_ref[rows, :].astype(F32) + recv_ref[rows, :].astype(F32)).astype(BF)


def rotated(value, axis, distance):
    size = lax.axis_size(axis)
    return lax.ppermute(value, axis, [(i, (i + distance) % size) for i in range(size)])


def local(
    tokens, norm_gain, w_query, w_key, w_value, w_outgate, w_gatein, w_gateout, w_convin,
    w_igate, w_fgate, input_bias, forget_bias, forget_extra, init_memory, head_gain, conv_taps,
    out_memory, out_conv,
):
    own = tokens[0]
    other = rotated(own, "tp", 1)
    wi, wf = w_igate.T, w_fgate.T
    fx = forget_extra[0].T
    half_act = sds((ROWS, WIDTH))
    half_f32 = sds((ROWS, WIDTH), F32)
    gflop = 2 * ROWS * D * WIDTH
    n_own, k_own, v_own, g_own = call(
        k1_body, "k1", [HBM, V, V, V, HBM, HBM],
        [sds((ROWS, D)), half_act, half_act, sds((16, ROWS), F32)],
        [pltpu.VMEM((ROWS, D), BF), pltpu.VMEM((2, D, WIDTH), BF), pltpu.SemaphoreType.DMA((4,)), pltpu.SemaphoreType.DMA((2,))],
        flops=3 * gflop,
    )(own, norm_gain, wi, wf, w_key, w_value)
    rows32 = sds((32, BLOCK), F32)
    n_oth, k_oth, v_oth, kt, u, cm, tot, bt, terms, pay = call(
        k2_body, "k2", [V] * 10 + [SM, SM] + [V] * 3,
        [sds((ROWS, D)), half_act, half_act, sds((32, DH, DH)), rows32, rows32, rows32, rows32, sds((32, DH, DH), F32), sds((PAY, DH))],
        [pltpu.VMEM((16, ROWS), F32)] + [pltpu.VMEM((32, BLOCK), F32)] * 4 + [pltpu.VMEM((8, BLOCK), F32)],
        flops=3 * gflop,
    )(other, norm_gain, wi, wf, w_key, w_value, g_own, k_own, v_own, fx, input_bias, forget_bias, n_own, w_gatein, w_convin)
    first = [rotated(pay, "sp_1", d) for d in (1, 2, 3)]
    cp_own, cp_oth, q_own, q_oth = call(
        k3a_body, "k3a", [V] * 5, [half_act] * 4, flops=7 * gflop,
    )(n_own, n_oth, w_gatein, w_convin, w_query)
    pm, ps, pay2 = call(
        c1_body, "c1", [V] * 4, [sds((512, DH), F32), sds((8, BLOCK), F32), sds((PAY, DH))],
        [pltpu.VMEM((8, BLOCK), F32)], flops=2**20, vmem=8,
    )(pay, *first)
    second = [rotated(pay2, "sp_0", d) for d in (1, 2, 3)]
    square = pltpu.VMEM((BLOCK, BLOCK), F32)
    tall = pltpu.VMEM((16 * BLOCK, BLOCK), F32)
    go_own, go_oth, cv_own, cv_oth, sg_own, sg_oth, in_own, in_oth = call(
        k3b_body, "k3b", [V] * 15, [half_act] * 4 + [half_f32] * 4,
        [square, tall, pltpu.VMEM((16 * BLOCK, BLOCK), BF), pltpu.VMEM((ROWS + 16, WIDTH), F32)], flops=7 * gflop,
    )(n_own, n_oth, w_gateout, w_outgate, q_own, q_oth, kt, v_own, v_oth, u, cm, cp_own, cp_oth, head_gain, conv_taps)
    wide = pltpu.VMEM((ROWS, 2 * WIDTH), BF)
    send, states, scales = call(
        k4_body, "k4", [V] * 20, [sds((ROWS, D)), sds((32, DH, DH)), rows32],
        [wide, square, tall, pltpu.VMEM((96, BLOCK), F32)], flops=3 * gflop,
    )(pm, ps, *second, first[0], init_memory[0], tot, bt, terms, q_oth, in_oth, sg_oth, cm, cv_oth, cp_oth, go_oth,
      conv_taps, out_memory, out_conv)
    recv = rotated(send, "tp", 1)
    (part,) = call(
        k5a_body, "k5a", [V] * 14, [sds((ROWS, D))], [wide, square, tall], flops=3 * gflop,
    )(first[0], second[0], q_own, in_own, sg_own, states, scales, cm, cv_own, cp_own, go_own, conv_taps, out_memory, out_conv)
    out = pl.pallas_call(
        k5b_body, name="k5b", grid=(4,), in_specs=[V, V], out_specs=pl.BlockSpec((128, D), lambda i: (i, 0)),
        out_shape=sds((ROWS, D)), compiler_params=pltpu.CompilerParams(vmem_limit_bytes=16 * MIB),
    )(part, recv)
    return out[None]


def solution(mesh):
    finer = Mesh(
        mesh.devices.reshape(4, 4, mesh.shape["fs"], mesh.shape["tp"]), ("sp_0", "sp_1", "fs", "tp")
    )
    sp_tp = ("sp_0", "sp_1", "tp")
    by_col = P(None, "tp")
    return jax.shard_map(
        local,
        mesh=finer,
        in_specs=(
            P("fs", sp_tp, None), P(), by_col, by_col, by_col, by_col, by_col, by_col, by_col,
            P(), P(), P(), P(), P("fs", SP, "tp"), P("fs", "tp", None, None), P(), P(),
            P("tp", None), P("tp", None),
        ),
        out_specs=P("fs", sp_tp, None),
        check_vma=False,
    )
```

```python
import math

import jax
import jax.numpy as jnp
from jax import lax
from jax.experimental import pallas as pl
from jax.experimental.pallas import tpu as pltpu
from jax.sharding import Mesh
from jax.sharding import PartitionSpec as P

BF = jnp.bfloat16
F32 = jnp.float32
BLOCK = 128
DH = 128
HEADS = 4
ROWS = 512
NB = 4
WIDTH = 512
D = 2048
EPSILON = 1e-06
LOWEST_LOG = -1e30
KEY_FACTOR = DH ** (-0.5)
LOG_KEY_FACTOR = math.log(KEY_FACTOR)
PAY = 544
SP = ("sp_0", "sp_1")
V = pl.BlockSpec(memory_space=pltpu.VMEM)
HBM = pl.BlockSpec(memory_space=pltpu.HBM)
SM = pl.BlockSpec(memory_space=pltpu.SMEM)
MIB = 2**20


def sds(shape, dtype=BF):
    return jax.ShapeDtypeStruct(shape, dtype)


def call(body, name, in_specs, outs, scratch=(), flops=0, vmem=16, nbytes=4 * MIB):
    return pl.pallas_call(
        body,
        name=name,
        in_specs=in_specs,
        out_specs=[V] * len(outs),
        out_shape=outs,
        scratch_shapes=list(scratch),
        compiler_params=pltpu.CompilerParams(vmem_limit_bytes=vmem * MIB),
        cost_estimate=pl.CostEstimate(flops=flops, bytes_accessed=nbytes, transcendentals=0),
    )


def dot(a, b):
    return jnp.dot(a, b, preferred_element_type=F32)


def dot_nt(a, b):
    return lax.dot_general(a, b, (((1,), (1,)), ((), ())), preferred_element_type=F32)


def norm_rows(x_ref, n_ref, gain, start, groups):
    scales = []
    for g in range(groups):
        rows = slice(start + g * 16, start + g * 16 + 16)
        x = x_ref[rows, :].astype(F32)
        scales.append(lax.rsqrt(jnp.mean(x * x, axis=-1, keepdims=True) + EPSILON))
    for g in range(groups):
        rows = slice(start + g * 16, start + g * 16 + 16)
        n_ref[rows, :] = (x_ref[rows, :].astype(F32) * scales[g] * gain).astype(BF)


FIRST, SECOND, WHOLE = slice(0, 256), slice(256, 512), slice(0, 512)


def project(n_ref, w, out_ref, rows=WHOLE, between=()):
    for j in range(WIDTH // 256):
        cols = slice(j * 256, (j + 1) * 256)
        out_ref[rows, cols] = dot(n_ref[rows, :], w[:, cols]).astype(BF)
        for step in between[j::2]:
            step()


def gate_rows(wi_ref, wf_ref, n_ref, g_ref):
    wg = jnp.concatenate([wi_ref[...].astype(F32), wf_ref[...].astype(F32)], axis=0).astype(BF)
    g_ref[...] = dot_nt(wg, n_ref[...])


def norm_steps(x_ref, n_ref, gain, start, count):
    return [lambda g=g: norm_rows(x_ref, n_ref, gain, start + g * 64, 4) for g in range(count // 64)]


def k1_body(t_hbm, gain_hbm, wi_hbm, wf_hbm, wk_hbm, wv_hbm, wq_hbm, win_hbm, wcv_hbm,
            n_ref, k_ref, v_ref, q_ref, g_ref, gain_ref, wi_ref, wf_ref, wk_ref, wv_ref, wq_ref, win_ref, wcv_ref,
            t_buf, sem):
    half = [pl.ds(0, 256), pl.ds(256, 256)]
    pairs = [
        (gain_hbm, gain_ref), (t_hbm.at[half[0], :], t_buf.at[half[0], :]), (t_hbm.at[half[1], :], t_buf.at[half[1], :]),
        (wk_hbm, wk_ref), (wi_hbm, wi_ref), (wf_hbm, wf_ref), (wv_hbm, wv_ref), (wq_hbm, wq_ref), (win_hbm, win_ref), (wcv_hbm, wcv_ref),
    ]
    copies = [pltpu.make_async_copy(src, dst, sem.at[i]) for i, (src, dst) in enumerate(pairs)]
    for copy in copies:
        copy.start()
    copies[0].wait()
    copies[1].wait()
    gain = gain_ref[...].astype(F32).reshape(1, D)
    norm_rows(t_buf, n_ref, gain, 0, 16)
    copies[2].wait()
    copies[3].wait()
    project(n_ref, wk_ref, k_ref, FIRST, norm_steps(t_buf, n_ref, gain, 256, 256))
    project(n_ref, wk_ref, k_ref, SECOND)
    for copy in copies[4:7]:
        copy.wait()
    gate_rows(wi_ref, wf_ref, n_ref, g_ref)
    project(n_ref, wv_ref, v_ref)
    copies[7].wait()
    project(n_ref, wq_ref, q_ref)
    for copy in copies[8:]:
        copy.wait()


def log_sigmoid(v):
    x = jnp.exp(-jnp.abs(v))
    series = x * (1.0 - x * (0.5 - x * (1.0 / 3.0 - x * 0.25)))
    return jnp.minimum(v, 0.0) - jnp.where(x < 0.01, series, jnp.log(1.0 + x))


def lane_scan(x, op, fill):
    lane = lax.broadcasted_iota(jnp.int32, x.shape, 1)
    for sh in (1, 2, 4, 8, 16, 32, 64):
        x = op(x, jnp.where(lane >= sh, pltpu.roll(x, sh, 1), fill))
    return x


def split3(x):
    a = x.astype(BF).astype(F32)
    r = x - a
    b = r.astype(BF).astype(F32)
    return a, b, r - b


def write_scalars(pay_ref, ts, rim):
    a, b, c = split3(ts)
    pay_ref[512:PAY, :] = jnp.concatenate([a, b, c, rim], axis=0).astype(BF)


def read_scalars(pay_ref):
    s = pay_ref[512:PAY, :].astype(F32)
    ts = s[0:8] + s[8:16] + s[16:24]
    return ts[0:4], ts[4:8]


def k2_body(t_ref, gain_ref, wi_ref, wf_ref, wk_ref, wv_ref, g_own_ref, k_own_ref, v_own_ref,
            fx_ref, ib_ref, fb_ref, n_own_ref, win_ref, wcv_ref,
            n_ref, k_ref, v_ref, kt_ref, u_ref, cm_ref, tot_ref, bt_ref, term_ref, pay_ref,
            g_ref, i_s, f_s, ws_s, wb_s, ts_s):
    tp = lax.axis_index("tp")
    gain = gain_ref[...].astype(F32).reshape(1, D)
    norm_rows(t_ref, n_ref, gain, 0, 16)
    project(n_ref, wk_ref, k_ref, FIRST, norm_steps(t_ref, n_ref, gain, 256, 256))
    project(n_ref, wk_ref, k_ref, SECOND)
    own_last = jnp.full((16, D), tp, jnp.int32) == 1
    last = jnp.where(own_last, n_own_ref[ROWS - 16 :, :].astype(F32), n_ref[ROWS - 16 :, :].astype(F32)).astype(BF)
    rim = dot(last, win_ref[...]).astype(BF).astype(F32) * dot(last, wcv_ref[...]).astype(BF).astype(F32)
    rim = jnp.concatenate([rim[14 + r : 15 + r, c * 128 : (c + 1) * 128] for r in range(2) for c in range(4)], axis=0)
    gate_rows(wi_ref, wf_ref, n_ref, g_ref)
    project(n_ref, wv_ref, v_ref)
    row = lax.broadcasted_iota(jnp.int32, (HEADS, ROWS), 0)
    first_core = jnp.full((HEADS, ROWS), tp, jnp.int32) == 0

    def column(ref):
        out = jnp.full((HEADS, ROWS), ref[tp * HEADS], F32)
        for h in range(1, HEADS):
            out = jnp.where(row == h, ref[tp * HEADS + h], out)
        return out

    in_bias, forget_bias = column(ib_ref), column(fb_ref)
    for half in range(2):
        if half == 0:
            g = [jnp.where(first_core, g_own_ref[4 * a : 4 * a + 4, :], g_ref[4 * a : 4 * a + 4, :]) for a in range(4)]
        else:
            g = [jnp.where(first_core, g_ref[4 * a : 4 * a + 4, :], g_own_ref[4 * a : 4 * a + 4, :]) for a in range(4)]
        in_pre = jnp.where(first_core, g[0], g[1]) + in_bias
        forget_pre = jnp.where(first_core, g[2], g[3]) + forget_bias
        lf = log_sigmoid(forget_pre) + fx_ref[:, half * ROWS : (half + 1) * ROWS]
        for j in range(NB):
            b = half * NB + j
            i_s[b * 4 : b * 4 + 4, :] = in_pre[:, j * BLOCK : (j + 1) * BLOCK]
            f_s[b * 4 : b * 4 + 4, :] = lf[:, j * BLOCK : (j + 1) * BLOCK]
    cum = lane_scan(f_s[...], jnp.add, 0.0)
    u = i_s[...] - cum
    cmax = lane_scan(u, jnp.maximum, -jnp.inf)
    tot = jnp.broadcast_to(cum[:, BLOCK - 1 :], cum.shape)
    top = tot + jnp.broadcast_to(cmax[:, BLOCK - 1 :], cum.shape)
    u_ref[...] = u + LOG_KEY_FACTOR
    cm_ref[...] = cmax
    tot_ref[...] = tot
    bt_ref[...] = top
    ws_s[...] = jnp.exp(tot + u - top) * KEY_FACTOR
    suffix = jnp.zeros((HEADS, BLOCK), F32)
    scale = jnp.full((HEADS, BLOCK), LOWEST_LOG, F32)
    for b in reversed(range(2 * NB)):
        e = suffix + bt_ref[b * 4 : b * 4 + 4, :]
        wb_s[b * 4 : b * 4 + 4, :] = e
        scale = jnp.maximum(scale, e)
        suffix = suffix + tot_ref[b * 4 : b * 4 + 4, :]
    for b in range(2 * NB):
        wb_s[b * 4 : b * 4 + 4, :] = jnp.exp(wb_s[b * 4 : b * 4 + 4, :] - scale)
    ts_s[0:4, :] = suffix
    ts_s[4:8, :] = scale
    write_scalars(pay_ref, ts_s[...], rim)
    for h in range(HEADS):
        cols = slice(h * DH, (h + 1) * DH)
        total = jnp.zeros((DH, DH), F32)
        for slot, (kr, vr) in enumerate(((k_own_ref, v_own_ref), (k_ref, v_ref))):
            half = tp if slot == 0 else 1 - tp
            for j in range(NB):
                rows = slice(j * BLOCK, (j + 1) * BLOCK)
                r = half * 16 + (j * 4 + h)
                kt = kr[rows, cols].T
                kt_ref[r] = kt
                term = dot((kt.astype(F32) * ws_s[pl.ds(r, 1), :]).astype(BF), vr[rows, cols])
                term_ref[r] = term
                total = total + wb_s[pl.ds(r, 1), :] * term
        pay_ref[h * DH : (h + 1) * DH, :] = total.astype(BF)


def k3a_body(n_own_ref, n_oth_ref, wi_ref, wc_ref, wq_ref, cp_own_ref, cp_oth_ref, q_oth_ref):
    for n_ref, cp_ref in ((n_own_ref, cp_own_ref), (n_oth_ref, cp_oth_ref)):
        for j in range(2):
            cols = slice(j * 256, (j + 1) * 256)
            a = dot(n_ref[...], wi_ref[:, cols]).astype(BF).astype(F32)
            c = dot(n_ref[...], wc_ref[:, cols]).astype(BF).astype(F32)
            cp_ref[:, cols] = (a * c).astype(BF)
    project(n_oth_ref, wq_ref, q_oth_ref)


def c1_body(own_ref, r1_ref, r2_ref, r3_ref, pm_ref, ps_ref, pay_ref, ts_s):
    x = lax.axis_index("sp_1")
    refs = (own_ref, r1_ref, r2_ref, r3_ref)
    place = [x] + [lax.rem(x + 4 - d, 4) for d in (1, 2, 3)]
    scal = [read_scalars(r) for r in refs]
    low = jnp.full((HEADS, BLOCK), LOWEST_LOG, F32)
    xv = jnp.full((HEADS, BLOCK), x, jnp.int32)
    suffix = jnp.zeros((HEADS, BLOCK), F32)
    levels = []
    for d in (1, 2, 3):
        levels.append(jnp.where(xv >= d, scal[d][1] + suffix, low))
        suffix = suffix + jnp.where(xv >= d, scal[d][0], 0.0)
    top = jnp.maximum(jnp.maximum(levels[0], levels[1]), levels[2])
    pw = [jnp.where(xv >= d, jnp.exp(levels[d - 1] - top), 0.0) for d in (1, 2, 3)]
    ps_ref[0:4, :] = suffix
    ps_ref[4:8, :] = top
    levels = []
    for a in range(4):
        level = scal[a][1]
        for b in range(4):
            if a != b:
                later = jnp.full((HEADS, BLOCK), place[b] - place[a], jnp.int32) > 0
                level = level + jnp.where(later, scal[b][0], 0.0)
        levels.append(level)
    rtop = jnp.maximum(jnp.maximum(levels[0], levels[1]), jnp.maximum(levels[2], levels[3]))
    rw = [jnp.exp(level - rtop) for level in levels]
    ts_s[0:4, :] = scal[0][0] + scal[1][0] + scal[2][0] + scal[3][0]
    ts_s[4:8, :] = rtop
    write_scalars(pay_ref, ts_s[...], r1_ref[536:PAY, :].astype(F32))
    for h in range(HEADS):
        rows = slice(h * DH, (h + 1) * DH)
        m = [r[rows, :].astype(F32) for r in refs]
        one = slice(h, h + 1)
        pm_ref[rows, :] = pw[0][one] * m[1] + pw[1][one] * m[2] + pw[2][one] * m[3]
        pay_ref[rows, :] = (rw[0][one] * m[0] + rw[1][one] * m[1] + rw[2][one] * m[2] + rw[3][one] * m[3]).astype(BF)


def slot_rows(ref, half):
    return ref[pl.ds(pl.multiple_of(half * 16, 16), 16), :]


def columns_of(rows16, pad_s):
    pad_s[0:16, :] = rows16
    return pad_s[...].T


def scores_half(q_ref, kt_ref, half, s_s):
    for c in range(16):
        rows, cols = slice(c // 4 * BLOCK, (c // 4 + 1) * BLOCK), slice(c % 4 * DH, (c % 4 + 1) * DH)
        s_s[c * BLOCK : (c + 1) * BLOCK, :] = dot(q_ref[rows, cols], kt_ref[half * 16 + c])


def weights_half(u_ref, cm_ref, half, s_s, w_s, pad_s):
    cmt = columns_of(slot_rows(cm_ref, half), pad_s)
    causal = lax.broadcasted_iota(jnp.int32, (BLOCK, BLOCK), 1) <= lax.broadcasted_iota(jnp.int32, (BLOCK, BLOCK), 0)
    for c in range(16):
        rows = slice(c * BLOCK, (c + 1) * BLOCK)
        log = u_ref[pl.ds(half * 16 + c, 1), :] - cmt[:, c : c + 1]
        w_s[rows, :] = (jnp.exp(jnp.where(causal, log, -jnp.inf)) * s_s[rows, :]).astype(BF)


def intra_half(w_s, v_ref, out_ref):
    for c in range(16):
        rows, cols = slice(c // 4 * BLOCK, (c // 4 + 1) * BLOCK), slice(c % 4 * DH, (c % 4 + 1) * DH)
        out_ref[rows, cols] = dot(w_s[c * BLOCK : (c + 1) * BLOCK, :], v_ref[rows, cols])


def local_cols(ref, tp):
    return ref[..., pl.ds(pl.multiple_of(tp * WIDTH, WIDTH), WIDTH)].astype(F32)


def gate_half(n_ref, wo_ref, gain, out_ref):
    for j in range(WIDTH // 256):
        cols = slice(j * 256, (j + 1) * 256)
        raw = dot(n_ref[...], wo_ref[:, cols]).astype(BF).astype(F32)
        out_ref[:, cols] = jax.nn.sigmoid(raw) * gain[:, cols]


def conv_half(cp_ref, before_ref, go_ref, taps, out_ref, buf_s):
    buf_s[0:16, :] = before_ref[ROWS - 16 :, :].astype(F32)
    for r in range(0, ROWS, 64):
        buf_s[16 + r : 80 + r, :] = cp_ref[r : r + 64, :].astype(F32)
        mixed = buf_s[14 + r : 78 + r, :] * taps[0:1]
        mixed = mixed + buf_s[15 + r : 79 + r, :] * taps[1:2]
        mixed = mixed + buf_s[16 + r : 80 + r, :] * taps[2:3]
        out_ref[r : r + 64, :] = (go_ref[r : r + 64, :].astype(F32) * mixed).astype(BF)


def k3b_body(n_own_ref, n_oth_ref, wg_ref, wo_ref, q_own_ref, q_oth_ref, kt_ref,
             v_own_ref, v_oth_ref, u_ref, cm_ref, cp_own_ref, cp_oth_ref, gain_ref, taps_ref,
             go_own_ref, go_oth_ref, cv_own_ref, cv_oth_ref, sg_own_ref, sg_oth_ref, in_own_ref, in_oth_ref,
             pad_s, s_s, w_s, buf_s):
    tp = lax.axis_index("tp")
    pad_s[...] = jnp.zeros_like(pad_s)
    gain = local_cols(gain_ref, tp).reshape(1, WIDTH)
    taps = local_cols(taps_ref, tp)
    for slot, (q_ref, v_ref, n_ref, out, go_ref, sg_ref, cp_ref, before_ref, cv_ref) in enumerate((
        (q_own_ref, v_own_ref, n_own_ref, in_own_ref, go_own_ref, sg_own_ref, cp_own_ref, cp_oth_ref, cv_own_ref),
        (q_oth_ref, v_oth_ref, n_oth_ref, in_oth_ref, go_oth_ref, sg_oth_ref, cp_oth_ref, cp_own_ref, cv_oth_ref),
    )):
        half = tp if slot == 0 else 1 - tp
        scores_half(q_ref, kt_ref, half, s_s)
        project(n_ref, wg_ref, go_ref)
        weights_half(u_ref, cm_ref, half, s_s, w_s, pad_s)
        gate_half(n_ref, wo_ref, gain, sg_ref)
        intra_half(w_s, v_ref, out)
        conv_half(cp_ref, before_ref, go_ref, taps, cv_ref, buf_s)


def readout_steps(q_ref, in_ref, sg_ref, st_ref, sc_ref, cm_ref, half, out_ref, pad_s, c_s):
    for c in range(16):
        rows, cols = slice(c // 4 * BLOCK, (c // 4 + 1) * BLOCK), slice(c % 4 * DH, (c % 4 + 1) * DH)
        c_s[c * BLOCK : (c + 1) * BLOCK, :] = dot(q_ref[rows, cols], st_ref[half * 16 + c])
    cm = slot_rows(cm_ref, half)
    sc = slot_rows(sc_ref, half)
    m = jnp.maximum(cm, sc)
    e_in = columns_of(jnp.exp(cm - m), pad_s)
    e_carry = columns_of(jnp.exp(sc - m), pad_s)

    def step(c):
        cols = slice(c % 4 * DH, (c % 4 + 1) * DH)
        for g in range(2):
            rows = slice(c // 4 * BLOCK + g * 64, c // 4 * BLOCK + g * 64 + 64)
            t = slice(g * 64, g * 64 + 64)
            read = e_carry[t, c : c + 1] * c_s[c * BLOCK + g * 64 : c * BLOCK + g * 64 + 64, :] + e_in[t, c : c + 1] * in_ref[rows, cols]
            scale = lax.rsqrt(jnp.mean(read * read, axis=-1, keepdims=True) + EPSILON)
            out_ref[rows, cols] = (read * scale * sg_ref[rows, cols]).astype(BF)

    return [lambda c=c: step(c) for c in range(16)]


def conv_fix(cv_ref, cp_ref, go_ref, r1_ref, z1_ref, taps_ref, half, out_ref):
    tp = lax.axis_index("tp")
    x = lax.axis_index("sp_1")
    z = lax.axis_index("sp_0")
    here = jnp.full((8, BLOCK), x, jnp.int32)
    row = jnp.full((8, BLOCK), z, jnp.int32)
    rim8 = jnp.where(here > 0, r1_ref[536:PAY, :].astype(F32), jnp.where(row > 0, z1_ref[536:PAY, :].astype(F32), 0.0))
    rim = [jnp.concatenate([rim8[r * 4 + c : r * 4 + c + 1, :] for c in range(4)], axis=1) for r in range(2)]
    taps = local_cols(taps_ref, tp)
    p = jnp.concatenate([rim[0], rim[1], cp_ref[0:16, :].astype(F32)], axis=0)
    mixed = p[0:16] * taps[0:1] + p[1:17] * taps[1:2] + p[2:18] * taps[2:3]
    fixed = go_ref[0:16, :].astype(F32) * mixed
    first = jnp.full((16, WIDTH), half, jnp.int32) == 0
    out_ref[0:16, WIDTH:] = jnp.where(first, fixed, cv_ref[0:16, :].astype(F32)).astype(BF)
    out_ref[16:, WIDTH:] = cv_ref[16:, :]


def out_project(a_ref, wm_ref, wc_ref, out_ref, rows, between=()):
    for j in range(D // 256):
        cols = slice(j * 256, (j + 1) * 256)
        out_ref[rows, cols] = (dot(a_ref[rows, :WIDTH], wm_ref[:, cols]) + dot(a_ref[rows, WIDTH:], wc_ref[:, cols])).astype(BF)
        for step in between[j::8]:
            step()


def finish_half(steps, a_ref, wm_ref, wc_ref, out_ref):
    for step in steps[:8]:
        step()
    out_project(a_ref, wm_ref, wc_ref, out_ref, FIRST, steps[8:])
    out_project(a_ref, wm_ref, wc_ref, out_ref, SECOND)


def k4_body(pm_ref, ps_ref, r1_ref, r2_ref, r3_ref, x1_ref, init_ref, tot_ref, bt_ref, term_ref,
            q_ref, in_ref, sg_ref, cm_ref, cv_ref, cp_ref, go_ref, taps_ref, wm_ref, wc_ref,
            send_ref, st_ref, sc_ref, a_s, pad_s, c_s, cs_s):
    tp = lax.axis_index("tp")
    z = lax.axis_index("sp_0")
    half = 1 - tp
    pad_s[...] = jnp.zeros_like(pad_s)
    refs = (r1_ref, r2_ref, r3_ref)
    zv = jnp.full((HEADS, BLOCK), z, jnp.int32)
    low = jnp.full((HEADS, BLOCK), LOWEST_LOG, F32)
    suffix = ps_ref[0:4, :]
    levels = [ps_ref[4:8, :]]
    for d in (1, 2, 3):
        t, s = read_scalars(refs[d - 1])
        levels.append(jnp.where(zv >= d, s + suffix, low))
        suffix = suffix + jnp.where(zv >= d, t, 0.0)
    levels.append(suffix)
    top = levels[0]
    for level in levels[1:]:
        top = jnp.maximum(top, level)
    w = [jnp.exp(level - top) for level in levels]
    for b in range(2 * NB):
        cs_s[b * 4 : b * 4 + 4, :] = top
        tot = tot_ref[b * 4 : b * 4 + 4, :] + top
        bt = bt_ref[b * 4 : b * 4 + 4, :]
        top = jnp.maximum(tot, bt)
        cs_s[32 + b * 4 : 36 + b * 4, :] = jnp.exp(tot - top)
        cs_s[64 + b * 4 : 68 + b * 4, :] = jnp.exp(bt - top)
    sc_ref[...] = cs_s[0:32, :]
    for h in range(HEADS):
        rows = slice(h * DH, (h + 1) * DH)
        one = slice(h, h + 1)
        mem = w[0][one] * pm_ref[rows, :] + w[4][one] * init_ref[h]
        for d in (1, 2, 3):
            mem = mem + w[d][one] * refs[d - 1][rows, :].astype(F32)
        for b in range(2 * NB):
            r = b * 4 + h
            st_ref[r] = mem.astype(BF)
            if b < 2 * NB - 1:
                mem = cs_s[32 + r : 33 + r, :] * mem + cs_s[64 + r : 65 + r, :] * term_ref[r]
    conv_fix(cv_ref, cp_ref, go_ref, x1_ref, r1_ref, taps_ref, half, a_s)
    steps = readout_steps(q_ref, in_ref, sg_ref, st_ref, sc_ref, cm_ref, half, a_s, pad_s, c_s)
    finish_half(steps, a_s, wm_ref, wc_ref, send_ref)


def k5a_body(x1_ref, z1_ref, q_ref, in_ref, sg_ref, st_ref, sc_ref, cm_ref, cv_ref, cp_ref, go_ref, taps_ref, wm_ref, wc_ref,
             part_ref, a_s, pad_s, c_s):
    tp = lax.axis_index("tp")
    pad_s[...] = jnp.zeros_like(pad_s)
    conv_fix(cv_ref, cp_ref, go_ref, x1_ref, z1_ref, taps_ref, tp, a_s)
    steps = readout_steps(q_ref, in_ref, sg_ref, st_ref, sc_ref, cm_ref, tp, a_s, pad_s, c_s)
    finish_half(steps, a_s, wm_ref, wc_ref, part_ref)


def k5b_body(part_ref, recv_ref, out_hbm, buf, sem):
    copies = []
    for i in range(8):
        rows = pl.ds(i * 64, 64)
        buf[rows, :] = (part_ref[rows, :].astype(F32) + recv_ref[rows, :].astype(F32)).astype(BF)
        copies.append(pltpu.make_async_copy(buf.at[rows, :], out_hbm.at[rows, :], sem.at[i]))
        copies[-1].start()
    for copy in copies:
        copy.wait()


def in_hbm(value):
    return pltpu.with_memory_space_constraint(value, pltpu.HBM)


def rotated(value, axis, distance):
    size = lax.axis_size(axis)
    return lax.ppermute(value, axis, [(i, (i + distance) % size) for i in range(size)])


def local(
    tokens, norm_gain, w_query, w_key, w_value, w_outgate, w_gatein, w_gateout, w_convin,
    w_igate, w_fgate, input_bias, forget_bias, forget_extra, init_memory, head_gain, conv_taps,
    out_memory, out_conv,
):
    own = tokens[0]
    other = rotated(own, "tp", 1)
    fx = forget_extra[0].T
    half_act = sds((ROWS, WIDTH))
    half_f32 = sds((ROWS, WIDTH), F32)
    gflop = 2 * ROWS * D * WIDTH
    weight = sds((D, WIDTH))
    n_own, k_own, v_own, q_own, g_own, gain, wi, wf, wk, wv, wq, win, wcv = call(
        k1_body, "k1", [HBM] * 9,
        [sds((ROWS, D)), half_act, half_act, half_act, sds((16, ROWS), F32), sds((D,)), sds((8, D)), sds((8, D))] + [weight] * 5,
        [pltpu.VMEM((ROWS, D), BF), pltpu.SemaphoreType.DMA((10,))],
        flops=3 * gflop,
    )(*[in_hbm(a) for a in (own, norm_gain, w_igate.T, w_fgate.T, w_key, w_value, w_query, w_gatein, w_convin)])
    rows32 = sds((32, BLOCK), F32)
    n_oth, k_oth, v_oth, kt, u, cm, tot, bt, terms, pay = call(
        k2_body, "k2", [V] * 10 + [SM, SM] + [V] * 3,
        [sds((ROWS, D)), half_act, half_act, sds((32, DH, DH)), rows32, rows32, rows32, rows32, sds((32, DH, DH), F32), sds((PAY, DH))],
        [pltpu.VMEM((16, ROWS), F32)] + [pltpu.VMEM((32, BLOCK), F32)] * 4 + [pltpu.VMEM((8, BLOCK), F32)],
        flops=3 * gflop,
    )(other, gain, wi, wf, wk, wv, g_own, k_own, v_own, fx, input_bias, forget_bias, n_own, win, wcv)
    first = [rotated(pay, "sp_1", d) for d in (1, 2, 3)]
    cp_own, cp_oth, q_oth = call(
        k3a_body, "k3a", [V] * 5, [half_act] * 3, flops=7 * gflop,
    )(n_own, n_oth, win, wcv, wq)
    pm, ps, pay2 = call(
        c1_body, "c1", [V] * 4, [sds((512, DH), F32), sds((8, BLOCK), F32), sds((PAY, DH))],
        [pltpu.VMEM((8, BLOCK), F32)], flops=2**20, vmem=8,
    )(pay, *first)
    second = [lax.ppermute(pay2, "sp_0", [(i, i + d) for i in range(4 - d)]) for d in (1, 2, 3)]
    square = pltpu.VMEM((BLOCK, BLOCK), F32)
    tall = pltpu.VMEM((16 * BLOCK, BLOCK), F32)
    go_own, go_oth, cv_own, cv_oth, sg_own, sg_oth, in_own, in_oth = call(
        k3b_body, "k3b", [V] * 15, [half_act] * 4 + [half_f32] * 4,
        [square, tall, pltpu.VMEM((16 * BLOCK, BLOCK), BF), pltpu.VMEM((ROWS + 16, WIDTH), F32)], flops=7 * gflop,
    )(n_own, n_oth, w_gateout, w_outgate, q_own, q_oth, kt, v_own, v_oth, u, cm, cp_own, cp_oth, head_gain, conv_taps)
    wide = pltpu.VMEM((ROWS, 2 * WIDTH), BF)
    send, states, scales = call(
        k4_body, "k4", [V] * 20, [sds((ROWS, D)), sds((32, DH, DH)), rows32],
        [wide, square, tall, pltpu.VMEM((96, BLOCK), F32)], flops=3 * gflop,
    )(pm, ps, *second, first[0], init_memory[0], tot, bt, terms, q_oth, in_oth, sg_oth, cm, cv_oth, cp_oth, go_oth,
      conv_taps, out_memory, out_conv)
    recv = rotated(send, "tp", 1)
    (part,) = call(
        k5a_body, "k5a", [V] * 14, [sds((ROWS, D))], [wide, square, tall], flops=3 * gflop,
    )(first[0], second[0], q_own, in_own, sg_own, states, scales, cm, cv_own, cp_own, go_own, conv_taps, out_memory, out_conv)
    out = pl.pallas_call(
        k5b_body, name="k5b", in_specs=[V, V], out_specs=HBM, out_shape=sds((ROWS, D)),
        scratch_shapes=[pltpu.VMEM((ROWS, D), BF), pltpu.SemaphoreType.DMA((8,))],
        compiler_params=pltpu.CompilerParams(vmem_limit_bytes=8 * MIB),
    )(part, recv)
    return out[None]


def solution(mesh):
    finer = Mesh(
        mesh.devices.reshape(4, 4, mesh.shape["fs"], mesh.shape["tp"]), ("sp_0", "sp_1", "fs", "tp")
    )
    sp_tp = ("sp_0", "sp_1", "tp")
    by_col = P(None, "tp")
    return jax.shard_map(
        local,
        mesh=finer,
        in_specs=(
            P("fs", sp_tp, None), P(), by_col, by_col, by_col, by_col, by_col, by_col, by_col,
            P(), P(), P(), P(), P("fs", SP, "tp"), P("fs", "tp", None, None), P(), P(),
            P("tp", None), P("tp", None),
        ),
        out_specs=P("fs", sp_tp, None),
        check_vma=False,
    )
```

```python
import math

import jax
import jax.numpy as jnp
from jax import lax
from jax.experimental import pallas as pl
from jax.experimental.pallas import tpu as pltpu
from jax.sharding import Mesh
from jax.sharding import PartitionSpec as P

BF = jnp.bfloat16
F32 = jnp.float32
BLOCK = 128
DH = 128
HEADS = 4
ROWS = 512
NB = 4
WIDTH = 512
D = 2048
EPSILON = 1e-06
LOWEST_LOG = -1e30
KEY_FACTOR = DH ** (-0.5)
LOG_KEY_FACTOR = math.log(KEY_FACTOR)
PAY = 544
SP = ("sp_0", "sp_1")
V = pl.BlockSpec(memory_space=pltpu.VMEM)
HBM = pl.BlockSpec(memory_space=pltpu.HBM)
SM = pl.BlockSpec(memory_space=pltpu.SMEM)
MIB = 2**20


def sds(shape, dtype=BF):
    return jax.ShapeDtypeStruct(shape, dtype)


def call(body, name, in_specs, outs, scratch=(), flops=0, vmem=16, nbytes=4 * MIB):
    return pl.pallas_call(
        body,
        name=name,
        in_specs=in_specs,
        out_specs=[V] * len(outs),
        out_shape=outs,
        scratch_shapes=list(scratch),
        compiler_params=pltpu.CompilerParams(vmem_limit_bytes=vmem * MIB),
        cost_estimate=pl.CostEstimate(flops=flops, bytes_accessed=nbytes, transcendentals=0),
    )


def dot(a, b):
    return jnp.dot(a, b, preferred_element_type=F32)


def dot_nt(a, b):
    return lax.dot_general(a, b, (((1,), (1,)), ((), ())), preferred_element_type=F32)


def norm_rows(x_ref, n_ref, gain, start, groups):
    scales = []
    for g in range(groups):
        rows = slice(start + g * 16, start + g * 16 + 16)
        x = x_ref[rows, :].astype(F32)
        scales.append(lax.rsqrt(jnp.mean(x * x, axis=-1, keepdims=True) + EPSILON))
    for g in range(groups):
        rows = slice(start + g * 16, start + g * 16 + 16)
        n_ref[rows, :] = (x_ref[rows, :].astype(F32) * scales[g] * gain).astype(BF)


FIRST, SECOND, WHOLE = slice(0, 256), slice(256, 512), slice(0, 512)


def project(n_ref, w, out_ref, rows=WHOLE, between=()):
    for j in range(WIDTH // 256):
        cols = slice(j * 256, (j + 1) * 256)
        out_ref[rows, cols] = dot(n_ref[rows, :], w[:, cols]).astype(BF)
        for step in between[j::2]:
            step()


def gate_rows(wi_ref, wf_ref, n_ref, g_ref):
    wg = jnp.concatenate([wi_ref[...].astype(F32), wf_ref[...].astype(F32)], axis=0).astype(BF)
    g_ref[...] = dot_nt(wg, n_ref[...])


def norm_steps(x_ref, n_ref, gain, start, count):
    return [lambda g=g: norm_rows(x_ref, n_ref, gain, start + g * 64, 4) for g in range(count // 64)]


def k1_body(t_hbm, gain_hbm, wi_hbm, wf_hbm, wk_hbm, wv_hbm, wq_hbm, win_hbm, wcv_hbm,
            n_ref, k_ref, v_ref, gain_ref, wi_ref, wf_ref, wk_ref, wv_ref, wq_ref, win_ref, wcv_ref,
            t_buf, sem):
    half = [pl.ds(0, 256), pl.ds(256, 256)]
    pairs = [
        (gain_hbm, gain_ref), (t_hbm.at[half[0], :], t_buf.at[half[0], :]), (t_hbm.at[half[1], :], t_buf.at[half[1], :]),
        (wk_hbm, wk_ref), (wv_hbm, wv_ref), (wi_hbm, wi_ref), (wf_hbm, wf_ref), (win_hbm, win_ref), (wcv_hbm, wcv_ref), (wq_hbm, wq_ref),
    ]
    copies = [pltpu.make_async_copy(src, dst, sem.at[i]) for i, (src, dst) in enumerate(pairs)]
    for copy in copies[:3]:
        copy.start()
    copies[0].wait()
    copies[1].wait()
    copies[3].start()
    copies[4].start()
    gain = gain_ref[...].astype(F32).reshape(1, D)
    norm_rows(t_buf, n_ref, gain, 0, 16)
    copies[2].wait()
    copies[3].wait()
    for copy in copies[5:]:
        copy.start()
    project(n_ref, wk_ref, k_ref, FIRST, norm_steps(t_buf, n_ref, gain, 256, 256))
    project(n_ref, wk_ref, k_ref, SECOND)
    copies[4].wait()
    project(n_ref, wv_ref, v_ref)
    for copy in copies[5:]:
        copy.wait()


def log_sigmoid(v):
    x = jnp.exp(-jnp.abs(v))
    series = x * (1.0 - x * (0.5 - x * (1.0 / 3.0 - x * 0.25)))
    return jnp.minimum(v, 0.0) - jnp.where(x < 0.01, series, jnp.log(1.0 + x))


def lane_scan(x, op, fill):
    lane = lax.broadcasted_iota(jnp.int32, x.shape, 1)
    for sh in (1, 2, 4, 8, 16, 32, 64):
        x = op(x, jnp.where(lane >= sh, pltpu.roll(x, sh, 1), fill))
    return x


def split3(x):
    a = x.astype(BF).astype(F32)
    r = x - a
    b = r.astype(BF).astype(F32)
    return a, b, r - b


def write_scalars(pay_ref, ts, rim):
    a, b, c = split3(ts)
    pay_ref[512:PAY, :] = jnp.concatenate([a, b, c, rim], axis=0).astype(BF)


def read_scalars(pay_ref):
    s = pay_ref[512:PAY, :].astype(F32)
    ts = s[0:8] + s[8:16] + s[16:24]
    return ts[0:4], ts[4:8]


def k2_body(t_ref, gain_ref, wi_ref, wf_ref, wk_ref, wv_ref, k_own_ref, v_own_ref,
            fx_ref, ib_ref, fb_ref, n_own_ref, win_ref, wcv_ref,
            n_ref, v_ref, kt_ref, u_ref, cm_ref, tot_ref, bt_ref, term_ref, pay_ref,
            k_ref, g_own_ref, g_ref, i_s, f_s, ws_s, wb_s, ts_s):
    tp = lax.axis_index("tp")
    gain = gain_ref[...].astype(F32).reshape(1, D)
    gate_rows(wi_ref, wf_ref, n_own_ref, g_own_ref)
    norm_rows(t_ref, n_ref, gain, 0, 16)
    project(n_ref, wk_ref, k_ref, FIRST, norm_steps(t_ref, n_ref, gain, 256, 256))
    project(n_ref, wk_ref, k_ref, SECOND)
    own_last = jnp.full((16, D), tp, jnp.int32) == 1
    last = jnp.where(own_last, n_own_ref[ROWS - 16 :, :].astype(F32), n_ref[ROWS - 16 :, :].astype(F32)).astype(BF)
    rim = dot(last, win_ref[...]).astype(BF).astype(F32) * dot(last, wcv_ref[...]).astype(BF).astype(F32)
    rim = jnp.concatenate([rim[14 + r : 15 + r, c * 128 : (c + 1) * 128] for r in range(2) for c in range(4)], axis=0)
    gate_rows(wi_ref, wf_ref, n_ref, g_ref)
    project(n_ref, wv_ref, v_ref)
    row = lax.broadcasted_iota(jnp.int32, (HEADS, ROWS), 0)
    first_core = jnp.full((HEADS, ROWS), tp, jnp.int32) == 0

    def column(ref):
        out = jnp.full((HEADS, ROWS), ref[tp * HEADS], F32)
        for h in range(1, HEADS):
            out = jnp.where(row == h, ref[tp * HEADS + h], out)
        return out

    in_bias, forget_bias = column(ib_ref), column(fb_ref)
    for half in range(2):
        if half == 0:
            g = [jnp.where(first_core, g_own_ref[4 * a : 4 * a + 4, :], g_ref[4 * a : 4 * a + 4, :]) for a in range(4)]
        else:
            g = [jnp.where(first_core, g_ref[4 * a : 4 * a + 4, :], g_own_ref[4 * a : 4 * a + 4, :]) for a in range(4)]
        in_pre = jnp.where(first_core, g[0], g[1]) + in_bias
        forget_pre = jnp.where(first_core, g[2], g[3]) + forget_bias
        lf = log_sigmoid(forget_pre) + fx_ref[:, half * ROWS : (half + 1) * ROWS]
        for j in range(NB):
            b = half * NB + j
            i_s[b * 4 : b * 4 + 4, :] = in_pre[:, j * BLOCK : (j + 1) * BLOCK]
            f_s[b * 4 : b * 4 + 4, :] = lf[:, j * BLOCK : (j + 1) * BLOCK]
    cum = lane_scan(f_s[...], jnp.add, 0.0)
    u = i_s[...] - cum
    cmax = lane_scan(u, jnp.maximum, -jnp.inf)
    tot = jnp.broadcast_to(cum[:, BLOCK - 1 :], cum.shape)
    top = tot + jnp.broadcast_to(cmax[:, BLOCK - 1 :], cum.shape)
    u_ref[...] = u + LOG_KEY_FACTOR
    cm_ref[...] = cmax
    tot_ref[...] = tot
    bt_ref[...] = top
    ws_s[...] = jnp.exp(tot + u - top) * KEY_FACTOR
    suffix = jnp.zeros((HEADS, BLOCK), F32)
    scale = jnp.full((HEADS, BLOCK), LOWEST_LOG, F32)
    for b in reversed(range(2 * NB)):
        e = suffix + bt_ref[b * 4 : b * 4 + 4, :]
        wb_s[b * 4 : b * 4 + 4, :] = e
        scale = jnp.maximum(scale, e)
        suffix = suffix + tot_ref[b * 4 : b * 4 + 4, :]
    for b in range(2 * NB):
        wb_s[b * 4 : b * 4 + 4, :] = jnp.exp(wb_s[b * 4 : b * 4 + 4, :] - scale)
    ts_s[0:4, :] = suffix
    ts_s[4:8, :] = scale
    write_scalars(pay_ref, ts_s[...], rim)
    for h in range(HEADS):
        cols = slice(h * DH, (h + 1) * DH)
        total = jnp.zeros((DH, DH), F32)
        for slot, (kr, vr) in enumerate(((k_own_ref, v_own_ref), (k_ref, v_ref))):
            half = tp if slot == 0 else 1 - tp
            for j in range(NB):
                rows = slice(j * BLOCK, (j + 1) * BLOCK)
                r = half * 16 + (j * 4 + h)
                kt = kr[rows, cols].T
                kt_ref[r] = kt
                term = dot((kt.astype(F32) * ws_s[pl.ds(r, 1), :]).astype(BF), vr[rows, cols])
                term_ref[r] = term
                total = total + wb_s[pl.ds(r, 1), :] * term
        pay_ref[h * DH : (h + 1) * DH, :] = total.astype(BF)


def k3a_body(n_own_ref, n_oth_ref, wi_ref, wc_ref, wq_ref, cp_own_ref, cp_oth_ref, q_own_ref, q_oth_ref):
    for n_ref, cp_ref in ((n_own_ref, cp_own_ref), (n_oth_ref, cp_oth_ref)):
        for j in range(2):
            cols = slice(j * 256, (j + 1) * 256)
            a = dot(n_ref[...], wi_ref[:, cols]).astype(BF).astype(F32)
            c = dot(n_ref[...], wc_ref[:, cols]).astype(BF).astype(F32)
            cp_ref[:, cols] = (a * c).astype(BF)
    project(n_own_ref, wq_ref, q_own_ref)
    project(n_oth_ref, wq_ref, q_oth_ref)


def c1_body(own_ref, r1_ref, r2_ref, r3_ref, pm_ref, ps_ref, pay_ref, ts_s):
    x = lax.axis_index("sp_1")
    refs = (own_ref, r1_ref, r2_ref, r3_ref)
    place = [x] + [lax.rem(x + 4 - d, 4) for d in (1, 2, 3)]
    scal = [read_scalars(r) for r in refs]
    low = jnp.full((HEADS, BLOCK), LOWEST_LOG, F32)
    xv = jnp.full((HEADS, BLOCK), x, jnp.int32)
    suffix = jnp.zeros((HEADS, BLOCK), F32)
    levels = []
    for d in (1, 2, 3):
        levels.append(jnp.where(xv >= d, scal[d][1] + suffix, low))
        suffix = suffix + jnp.where(xv >= d, scal[d][0], 0.0)
    top = jnp.maximum(jnp.maximum(levels[0], levels[1]), levels[2])
    pw = [jnp.where(xv >= d, jnp.exp(levels[d - 1] - top), 0.0) for d in (1, 2, 3)]
    ps_ref[0:4, :] = suffix
    ps_ref[4:8, :] = top
    levels = []
    for a in range(4):
        level = scal[a][1]
        for b in range(4):
            if a != b:
                later = jnp.full((HEADS, BLOCK), place[b] - place[a], jnp.int32) > 0
                level = level + jnp.where(later, scal[b][0], 0.0)
        levels.append(level)
    rtop = jnp.maximum(jnp.maximum(levels[0], levels[1]), jnp.maximum(levels[2], levels[3]))
    rw = [jnp.exp(level - rtop) for level in levels]
    ts_s[0:4, :] = scal[0][0] + scal[1][0] + scal[2][0] + scal[3][0]
    ts_s[4:8, :] = rtop
    write_scalars(pay_ref, ts_s[...], r1_ref[536:PAY, :].astype(F32))
    for h in range(HEADS):
        rows = slice(h * DH, (h + 1) * DH)
        m = [r[rows, :].astype(F32) for r in refs]
        one = slice(h, h + 1)
        pm_ref[rows, :] = pw[0][one] * m[1] + pw[1][one] * m[2] + pw[2][one] * m[3]
        pay_ref[rows, :] = (rw[0][one] * m[0] + rw[1][one] * m[1] + rw[2][one] * m[2] + rw[3][one] * m[3]).astype(BF)


def slot_rows(ref, half):
    return ref[pl.ds(pl.multiple_of(half * 16, 16), 16), :]


def columns_of(rows16, pad_s):
    pad_s[0:16, :] = rows16
    return pad_s[...].T


def scores_half(q_ref, kt_ref, half, s_s):
    for c in range(16):
        rows, cols = slice(c // 4 * BLOCK, (c // 4 + 1) * BLOCK), slice(c % 4 * DH, (c % 4 + 1) * DH)
        s_s[c * BLOCK : (c + 1) * BLOCK, :] = dot(q_ref[rows, cols], kt_ref[half * 16 + c])


def weights_half(u_ref, cm_ref, half, s_s, w_s, pad_s):
    cmt = columns_of(slot_rows(cm_ref, half), pad_s)
    causal = lax.broadcasted_iota(jnp.int32, (BLOCK, BLOCK), 1) <= lax.broadcasted_iota(jnp.int32, (BLOCK, BLOCK), 0)
    for c in range(16):
        rows = slice(c * BLOCK, (c + 1) * BLOCK)
        log = u_ref[pl.ds(half * 16 + c, 1), :] - cmt[:, c : c + 1]
        w_s[rows, :] = (jnp.exp(jnp.where(causal, log, -jnp.inf)) * s_s[rows, :]).astype(BF)


def intra_half(w_s, v_ref, out_ref):
    for c in range(16):
        rows, cols = slice(c // 4 * BLOCK, (c // 4 + 1) * BLOCK), slice(c % 4 * DH, (c % 4 + 1) * DH)
        out_ref[rows, cols] = dot(w_s[c * BLOCK : (c + 1) * BLOCK, :], v_ref[rows, cols])


def local_cols(ref, tp):
    return ref[..., pl.ds(pl.multiple_of(tp * WIDTH, WIDTH), WIDTH)].astype(F32)


def gate_half(n_ref, wo_ref, gain, out_ref):
    for j in range(WIDTH // 256):
        cols = slice(j * 256, (j + 1) * 256)
        raw = dot(n_ref[...], wo_ref[:, cols]).astype(BF).astype(F32)
        out_ref[:, cols] = jax.nn.sigmoid(raw) * gain[:, cols]


def conv_half(cp_ref, before_ref, go_ref, taps, out_ref, buf_s):
    buf_s[0:16, :] = before_ref[ROWS - 16 :, :].astype(F32)
    for r in range(0, ROWS, 64):
        buf_s[16 + r : 80 + r, :] = cp_ref[r : r + 64, :].astype(F32)
        mixed = buf_s[14 + r : 78 + r, :] * taps[0:1]
        mixed = mixed + buf_s[15 + r : 79 + r, :] * taps[1:2]
        mixed = mixed + buf_s[16 + r : 80 + r, :] * taps[2:3]
        out_ref[r : r + 64, :] = (go_ref[r : r + 64, :].astype(F32) * mixed).astype(BF)


def k3b_body(n_own_ref, n_oth_ref, wg_ref, wo_ref, q_own_ref, q_oth_ref, kt_ref,
             v_own_ref, v_oth_ref, u_ref, cm_ref, cp_own_ref, cp_oth_ref, gain_ref, taps_ref,
             go_own_ref, go_oth_ref, cv_own_ref, cv_oth_ref, sg_own_ref, sg_oth_ref, in_own_ref, in_oth_ref,
             pad_s, s_s, w_s, buf_s):
    tp = lax.axis_index("tp")
    pad_s[...] = jnp.zeros_like(pad_s)
    gain = local_cols(gain_ref, tp).reshape(1, WIDTH)
    taps = local_cols(taps_ref, tp)
    for slot, (q_ref, v_ref, n_ref, out, go_ref, sg_ref, cp_ref, before_ref, cv_ref) in enumerate((
        (q_own_ref, v_own_ref, n_own_ref, in_own_ref, go_own_ref, sg_own_ref, cp_own_ref, cp_oth_ref, cv_own_ref),
        (q_oth_ref, v_oth_ref, n_oth_ref, in_oth_ref, go_oth_ref, sg_oth_ref, cp_oth_ref, cp_own_ref, cv_oth_ref),
    )):
        half = tp if slot == 0 else 1 - tp
        scores_half(q_ref, kt_ref, half, s_s)
        project(n_ref, wg_ref, go_ref)
        weights_half(u_ref, cm_ref, half, s_s, w_s, pad_s)
        gate_half(n_ref, wo_ref, gain, sg_ref)
        intra_half(w_s, v_ref, out)
        conv_half(cp_ref, before_ref, go_ref, taps, cv_ref, buf_s)


def readout_steps(q_ref, in_ref, sg_ref, st_ref, sc_ref, cm_ref, half, out_ref, pad_s, c_s):
    for c in range(16):
        rows, cols = slice(c // 4 * BLOCK, (c // 4 + 1) * BLOCK), slice(c % 4 * DH, (c % 4 + 1) * DH)
        c_s[c * BLOCK : (c + 1) * BLOCK, :] = dot(q_ref[rows, cols], st_ref[half * 16 + c])
    cm = slot_rows(cm_ref, half)
    sc = slot_rows(sc_ref, half)
    m = jnp.maximum(cm, sc)
    e_in = columns_of(jnp.exp(cm - m), pad_s)
    e_carry = columns_of(jnp.exp(sc - m), pad_s)

    def step(c):
        cols = slice(c % 4 * DH, (c % 4 + 1) * DH)
        for g in range(2):
            rows = slice(c // 4 * BLOCK + g * 64, c // 4 * BLOCK + g * 64 + 64)
            t = slice(g * 64, g * 64 + 64)
            read = e_carry[t, c : c + 1] * c_s[c * BLOCK + g * 64 : c * BLOCK + g * 64 + 64, :] + e_in[t, c : c + 1] * in_ref[rows, cols]
            scale = lax.rsqrt(jnp.mean(read * read, axis=-1, keepdims=True) + EPSILON)
            out_ref[rows, cols] = (read * scale * sg_ref[rows, cols]).astype(BF)

    return [lambda c=c: step(c) for c in range(16)]


def conv_fix(cv_ref, cp_ref, go_ref, r1_ref, z1_ref, taps_ref, half, out_ref):
    tp = lax.axis_index("tp")
    x = lax.axis_index("sp_1")
    z = lax.axis_index("sp_0")
    here = jnp.full((8, BLOCK), x, jnp.int32)
    row = jnp.full((8, BLOCK), z, jnp.int32)
    rim8 = jnp.where(here > 0, r1_ref[536:PAY, :].astype(F32), jnp.where(row > 0, z1_ref[536:PAY, :].astype(F32), 0.0))
    rim = [jnp.concatenate([rim8[r * 4 + c : r * 4 + c + 1, :] for c in range(4)], axis=1) for r in range(2)]
    taps = local_cols(taps_ref, tp)
    p = jnp.concatenate([rim[0], rim[1], cp_ref[0:16, :].astype(F32)], axis=0)
    mixed = p[0:16] * taps[0:1] + p[1:17] * taps[1:2] + p[2:18] * taps[2:3]
    fixed = go_ref[0:16, :].astype(F32) * mixed
    first = jnp.full((16, WIDTH), half, jnp.int32) == 0
    out_ref[0:16, WIDTH:] = jnp.where(first, fixed, cv_ref[0:16, :].astype(F32)).astype(BF)
    out_ref[16:, WIDTH:] = cv_ref[16:, :]


def finish_half(first_steps, second_steps, a_ref, acc_s, wm_ref, wc_ref, out_ref):
    tiles = [slice(j * 256, (j + 1) * 256) for j in range(D // 256)]
    for j, cols in enumerate(tiles):
        acc_s[:, cols] = dot(a_ref[FIRST, WIDTH:], wc_ref[:, cols])
        for step in first_steps[j::8]:
            step()
    for j, cols in enumerate(tiles):
        out_ref[FIRST, cols] = (acc_s[:, cols] + dot(a_ref[FIRST, :WIDTH], wm_ref[:, cols])).astype(BF)
        for step in second_steps[j::8]:
            step()
    for cols in tiles:
        out_ref[SECOND, cols] = (dot(a_ref[SECOND, WIDTH:], wc_ref[:, cols]) + dot(a_ref[SECOND, :WIDTH], wm_ref[:, cols])).astype(BF)


def k4_body(pm_ref, ps_ref, r1_ref, r2_ref, r3_ref, x1_ref, init_ref, tot_ref, bt_ref, term_ref,
            q_ref, in_ref, sg_ref, cm_ref, cv_ref, cp_ref, go_ref, taps_ref, wm_ref, wc_ref,
            send_ref, st_ref, sc_ref, a_s, acc_s, pad_s, c_s, cs_s):
    tp = lax.axis_index("tp")
    z = lax.axis_index("sp_0")
    half = 1 - tp
    pad_s[...] = jnp.zeros_like(pad_s)
    refs = (r1_ref, r2_ref, r3_ref)
    zv = jnp.full((HEADS, BLOCK), z, jnp.int32)
    low = jnp.full((HEADS, BLOCK), LOWEST_LOG, F32)
    suffix = ps_ref[0:4, :]
    levels = [ps_ref[4:8, :]]
    for d in (1, 2, 3):
        t, s = read_scalars(refs[d - 1])
        levels.append(jnp.where(zv >= d, s + suffix, low))
        suffix = suffix + jnp.where(zv >= d, t, 0.0)
    levels.append(suffix)
    top = levels[0]
    for level in levels[1:]:
        top = jnp.maximum(top, level)
    w = [jnp.exp(level - top) for level in levels]
    for b in range(2 * NB):
        cs_s[b * 4 : b * 4 + 4, :] = top
        tot = tot_ref[b * 4 : b * 4 + 4, :] + top
        bt = bt_ref[b * 4 : b * 4 + 4, :]
        top = jnp.maximum(tot, bt)
        cs_s[32 + b * 4 : 36 + b * 4, :] = jnp.exp(tot - top)
        cs_s[64 + b * 4 : 68 + b * 4, :] = jnp.exp(bt - top)
    sc_ref[...] = cs_s[0:32, :]
    for h in range(HEADS):
        rows = slice(h * DH, (h + 1) * DH)
        one = slice(h, h + 1)
        mem = w[0][one] * pm_ref[rows, :] + w[4][one] * init_ref[h]
        for d in (1, 2, 3):
            mem = mem + w[d][one] * refs[d - 1][rows, :].astype(F32)
        for b in range(2 * NB):
            r = b * 4 + h
            st_ref[r] = mem.astype(BF)
            if b < 2 * NB - 1:
                mem = cs_s[32 + r : 33 + r, :] * mem + cs_s[64 + r : 65 + r, :] * term_ref[r]
    conv_fix(cv_ref, cp_ref, go_ref, x1_ref, r1_ref, taps_ref, half, a_s)
    steps = readout_steps(q_ref, in_ref, sg_ref, st_ref, sc_ref, cm_ref, half, a_s, pad_s, c_s)
    finish_half(steps[:8], steps[8:], a_s, acc_s, wm_ref, wc_ref, send_ref)


def k5a_body(x1_ref, z1_ref, q_ref, in_ref, sg_ref, st_ref, sc_ref, cm_ref, cv_ref, cp_ref, go_ref, taps_ref, wm_ref, wc_ref,
             part_ref, a_s, acc_s, pad_s, c_s):
    tp = lax.axis_index("tp")
    pad_s[...] = jnp.zeros_like(pad_s)
    conv_fix(cv_ref, cp_ref, go_ref, x1_ref, z1_ref, taps_ref, tp, a_s)
    steps = readout_steps(q_ref, in_ref, sg_ref, st_ref, sc_ref, cm_ref, tp, a_s, pad_s, c_s)
    finish_half(steps[:8], steps[8:], a_s, acc_s, wm_ref, wc_ref, part_ref)


def k5b_body(part_ref, recv_ref, out_hbm, buf, sem):
    copies = []
    for i in range(8):
        rows = pl.ds(i * 64, 64)
        buf[rows, :] = (part_ref[rows, :].astype(F32) + recv_ref[rows, :].astype(F32)).astype(BF)
        copies.append(pltpu.make_async_copy(buf.at[rows, :], out_hbm.at[rows, :], sem.at[i]))
        copies[-1].start()
    for copy in copies:
        copy.wait()


def in_hbm(value):
    return pltpu.with_memory_space_constraint(value, pltpu.HBM)


def rotated(value, axis, distance):
    size = lax.axis_size(axis)
    return lax.ppermute(value, axis, [(i, (i + distance) % size) for i in range(size)])


def local(
    tokens, norm_gain, w_query, w_key, w_value, w_outgate, w_gatein, w_gateout, w_convin,
    w_igate, w_fgate, input_bias, forget_bias, forget_extra, init_memory, head_gain, conv_taps,
    out_memory, out_conv,
):
    own = tokens[0]
    other = rotated(own, "tp", 1)
    fx = forget_extra[0].T
    half_act = sds((ROWS, WIDTH))
    half_f32 = sds((ROWS, WIDTH), F32)
    gflop = 2 * ROWS * D * WIDTH
    weight = sds((D, WIDTH))
    n_own, k_own, v_own, gain, wi, wf, wk, wv, wq, win, wcv = call(
        k1_body, "k1", [HBM] * 9,
        [sds((ROWS, D)), half_act, half_act, sds((D,)), sds((8, D)), sds((8, D))] + [weight] * 5,
        [pltpu.VMEM((ROWS, D), BF), pltpu.SemaphoreType.DMA((10,))],
        flops=3 * gflop,
    )(*[in_hbm(a) for a in (own, norm_gain, w_igate.T, w_fgate.T, w_key, w_value, w_query, w_gatein, w_convin)])
    rows32 = sds((32, BLOCK), F32)
    n_oth, v_oth, kt, u, cm, tot, bt, terms, pay = call(
        k2_body, "k2", [V] * 9 + [SM, SM] + [V] * 3,
        [sds((ROWS, D)), half_act, sds((32, DH, DH)), rows32, rows32, rows32, rows32, sds((32, DH, DH), F32), sds((PAY, DH))],
        [pltpu.VMEM((ROWS, WIDTH), BF)] + [pltpu.VMEM((16, ROWS), F32)] * 2 + [pltpu.VMEM((32, BLOCK), F32)] * 4 + [pltpu.VMEM((8, BLOCK), F32)],
        flops=3 * gflop,
    )(other, gain, wi, wf, wk, wv, k_own, v_own, fx, input_bias, forget_bias, n_own, win, wcv)
    first = [rotated(pay, "sp_1", d) for d in (1, 2, 3)]
    cp_own, cp_oth, q_own, q_oth = call(
        k3a_body, "k3a", [V] * 5, [half_act] * 4, flops=7 * gflop,
    )(n_own, n_oth, win, wcv, wq)
    pm, ps, pay2 = call(
        c1_body, "c1", [V] * 4, [sds((512, DH), F32), sds((8, BLOCK), F32), sds((PAY, DH))],
        [pltpu.VMEM((8, BLOCK), F32)], flops=2**20, vmem=8,
    )(pay, *first)
    second = [lax.ppermute(pay2, "sp_0", [(i, i + d) for i in range(4 - d)]) for d in (1, 2, 3)]
    square = pltpu.VMEM((BLOCK, BLOCK), F32)
    tall = pltpu.VMEM((16 * BLOCK, BLOCK), F32)
    go_own, go_oth, cv_own, cv_oth, sg_own, sg_oth, in_own, in_oth = call(
        k3b_body, "k3b", [V] * 15, [half_act] * 4 + [half_f32] * 4,
        [square, tall, pltpu.VMEM((16 * BLOCK, BLOCK), BF), pltpu.VMEM((ROWS + 16, WIDTH), F32)], flops=7 * gflop,
    )(n_own, n_oth, w_gateout, w_outgate, q_own, q_oth, kt, v_own, v_oth, u, cm, cp_own, cp_oth, head_gain, conv_taps)
    wide = pltpu.VMEM((ROWS, 2 * WIDTH), BF)
    acc = pltpu.VMEM((256, D), F32)
    send, states, scales = call(
        k4_body, "k4", [V] * 20, [sds((ROWS, D)), sds((32, DH, DH)), rows32],
        [wide, acc, square, tall, pltpu.VMEM((96, BLOCK), F32)], flops=3 * gflop,
    )(pm, ps, *second, first[0], init_memory[0], tot, bt, terms, q_oth, in_oth, sg_oth, cm, cv_oth, cp_oth, go_oth,
      conv_taps, out_memory, out_conv)
    recv = rotated(send, "tp", 1)
    (part,) = call(
        k5a_body, "k5a", [V] * 14, [sds((ROWS, D))], [wide, acc, square, tall], flops=3 * gflop,
    )(first[0], second[0], q_own, in_own, sg_own, states, scales, cm, cv_own, cp_own, go_own, conv_taps, out_memory, out_conv)
    out = pl.pallas_call(
        k5b_body, name="k5b", in_specs=[V, V], out_specs=HBM, out_shape=sds((ROWS, D)),
        scratch_shapes=[pltpu.VMEM((ROWS, D), BF), pltpu.SemaphoreType.DMA((8,))],
        compiler_params=pltpu.CompilerParams(vmem_limit_bytes=8 * MIB),
    )(part, recv)
    return out[None]


def solution(mesh):
    finer = Mesh(
        mesh.devices.reshape(4, 4, mesh.shape["fs"], mesh.shape["tp"]), ("sp_0", "sp_1", "fs", "tp")
    )
    sp_tp = ("sp_0", "sp_1", "tp")
    by_col = P(None, "tp")
    return jax.shard_map(
        local,
        mesh=finer,
        in_specs=(
            P("fs", sp_tp, None), P(), by_col, by_col, by_col, by_col, by_col, by_col, by_col,
            P(), P(), P(), P(), P("fs", SP, "tp"), P("fs", "tp", None, None), P(), P(),
            P("tp", None), P("tp", None),
        ),
        out_specs=P("fs", sp_tp, None),
        check_vma=False,
    )
```

```python
import math

import jax
import jax.numpy as jnp
from jax import lax
from jax.experimental import pallas as pl
from jax.experimental.pallas import tpu as pltpu
from jax.sharding import Mesh
from jax.sharding import PartitionSpec as P

BF = jnp.bfloat16
F32 = jnp.float32
BLOCK = 128
DH = 128
HEADS = 4
ROWS = 512
NB = 4
WIDTH = 512
D = 2048
EPSILON = 1e-06
LOWEST_LOG = -1e30
KEY_FACTOR = DH ** (-0.5)
LOG_KEY_FACTOR = math.log(KEY_FACTOR)
PAY = 544
SP = ("sp_0", "sp_1")
V = pl.BlockSpec(memory_space=pltpu.VMEM)
HBM = pl.BlockSpec(memory_space=pltpu.HBM)
SM = pl.BlockSpec(memory_space=pltpu.SMEM)
MIB = 2**20


def sds(shape, dtype=BF):
    return jax.ShapeDtypeStruct(shape, dtype)


def call(body, name, in_specs, outs, scratch=(), flops=0, vmem=16, nbytes=4 * MIB):
    return pl.pallas_call(
        body,
        name=name,
        in_specs=in_specs,
        out_specs=[V] * len(outs),
        out_shape=outs,
        scratch_shapes=list(scratch),
        compiler_params=pltpu.CompilerParams(vmem_limit_bytes=vmem * MIB),
        cost_estimate=pl.CostEstimate(flops=flops, bytes_accessed=nbytes, transcendentals=0),
    )


def dot(a, b):
    return jnp.dot(a, b, preferred_element_type=F32)


def dot_nt(a, b):
    return lax.dot_general(a, b, (((1,), (1,)), ((), ())), preferred_element_type=F32)


def norm_rows(x_ref, n_ref, gain_ref, start, groups):
    lanes = [slice(i * 128, (i + 1) * 128) for i in range(D // 128)]
    scales = []
    for g in range(groups):
        rows = slice(start + g * 16, start + g * 16 + 16)
        total = jnp.zeros((16, 128), F32)
        for cols in lanes:
            x = x_ref[rows, cols].astype(F32)
            total = total + x * x
        mean = jnp.sum(total, axis=-1, keepdims=True) * (1.0 / D)
        scales.append(jnp.broadcast_to(lax.rsqrt(mean + EPSILON), (16, 128)))
    for cols in lanes:
        gain = jnp.broadcast_to(gain_ref[cols].astype(F32).reshape(1, 128), (16, 128))
        for g in range(groups):
            rows = slice(start + g * 16, start + g * 16 + 16)
            n_ref[rows, cols] = (x_ref[rows, cols].astype(F32) * scales[g] * gain).astype(BF)


FIRST, SECOND, WHOLE = slice(0, 256), slice(256, 512), slice(0, 512)


def project(n_ref, w, out_ref, rows=WHOLE, between=()):
    for j in range(WIDTH // 256):
        cols = slice(j * 256, (j + 1) * 256)
        out_ref[rows, cols] = dot(n_ref[rows, :], w[:, cols]).astype(BF)
        for step in between[j::2]:
            step()


def gate_rows(wi_ref, wf_ref, n_ref, g_ref):
    wg = jnp.concatenate([wi_ref[...].astype(F32), wf_ref[...].astype(F32)], axis=0).astype(BF)
    g_ref[...] = dot_nt(wg, n_ref[...])


def norm_steps(x_ref, n_ref, gain, start, count):
    return [lambda g=g: norm_rows(x_ref, n_ref, gain, start + g * 64, 4) for g in range(count // 64)]


def k1_body(t_hbm, gain_hbm, wi_hbm, wf_hbm, wk_hbm, wv_hbm, win_hbm, wcv_hbm,
            n_ref, k_ref, v_ref, g_ref, gain_ref, wi_ref, wf_ref, wk_ref, wv_ref, win_ref, wcv_ref,
            t_buf, sem):
    half = [pl.ds(0, 256), pl.ds(256, 256)]
    pairs = [
        (gain_hbm, gain_ref), (t_hbm.at[half[0], :], t_buf.at[half[0], :]), (t_hbm.at[half[1], :], t_buf.at[half[1], :]),
        (wk_hbm, wk_ref), (wv_hbm, wv_ref), (wi_hbm, wi_ref), (wf_hbm, wf_ref), (win_hbm, win_ref), (wcv_hbm, wcv_ref),
    ]
    copies = [pltpu.make_async_copy(src, dst, sem.at[i]) for i, (src, dst) in enumerate(pairs)]
    for copy in copies[:4]:
        copy.start()
    copies[0].wait()
    copies[1].wait()
    for copy in copies[4:]:
        copy.start()
    for step in norm_steps(t_buf, n_ref, gain_ref, 0, 256):
        step()
    copies[2].wait()
    copies[3].wait()
    project(n_ref, wk_ref, k_ref, FIRST, norm_steps(t_buf, n_ref, gain_ref, 256, 256))
    project(n_ref, wk_ref, k_ref, SECOND)
    for copy in copies[4:7]:
        copy.wait()
    project(n_ref, wv_ref, v_ref)
    gate_rows(wi_ref, wf_ref, n_ref, g_ref)
    for copy in copies[7:]:
        copy.wait()


def log_sigmoid(v):
    x = jnp.exp(-jnp.abs(v))
    series = x * (1.0 - x * (0.5 - x * (1.0 / 3.0 - x * 0.25)))
    return jnp.minimum(v, 0.0) - jnp.where(x < 0.01, series, jnp.log(1.0 + x))


def lane_scan(x, op, fill):
    lane = lax.broadcasted_iota(jnp.int32, x.shape, 1)
    for sh in (1, 2, 4, 8, 16, 32, 64):
        x = op(x, jnp.where(lane >= sh, pltpu.roll(x, sh, 1), fill))
    return x


def split3(x):
    a = x.astype(BF).astype(F32)
    r = x - a
    b = r.astype(BF).astype(F32)
    return a, b, r - b


def write_scalars(pay_ref, ts, rim):
    a, b, c = split3(ts)
    pay_ref[512:PAY, :] = jnp.concatenate([a, b, c, rim], axis=0).astype(BF)


def read_scalars(pay_ref):
    s = pay_ref[512:PAY, :].astype(F32)
    ts = s[0:8] + s[8:16] + s[16:24]
    return ts[0:4], ts[4:8]


def k2_body(t_ref, gain_ref, wi_ref, wf_ref, wk_ref, wv_ref, g_own_ref, k_own_ref, v_own_ref,
            fx_ref, ib_ref, fb_ref, n_own_ref, win_ref, wcv_ref, wq_hbm,
            n_ref, v_ref, wq_ref, kt_ref, u_ref, cm_ref, tot_ref, bt_ref, term_ref, pay_ref,
            k_ref, g_ref, i_s, f_s, ws_s, wb_s, ts_s, q_sem):
    load_q = pltpu.make_async_copy(wq_hbm, wq_ref, q_sem)
    load_q.start()
    tp = lax.axis_index("tp")
    for step in norm_steps(t_ref, n_ref, gain_ref, 0, 256):
        step()
    project(n_ref, wk_ref, k_ref, FIRST, norm_steps(t_ref, n_ref, gain_ref, 256, 256))
    project(n_ref, wk_ref, k_ref, SECOND)
    gate_rows(wi_ref, wf_ref, n_ref, g_ref)
    first_core = jnp.full((HEADS, ROWS), tp, jnp.int32) == 0

    def column(ref):
        square = (8, 8)
        diagonal = lax.broadcasted_iota(jnp.int32, square, 0) == lax.broadcasted_iota(jnp.int32, square, 1)
        wide = jnp.broadcast_to(ref[...].reshape(1, 8), square)
        col = jnp.sum(jnp.where(diagonal, wide, 0.0), axis=1, keepdims=True)
        full = jnp.broadcast_to(col, (8, ROWS))
        return jnp.where(first_core, full[0:4], full[4:8])

    in_bias, forget_bias = column(ib_ref), column(fb_ref)
    for half in range(2):
        if half == 0:
            g = [jnp.where(first_core, g_own_ref[4 * a : 4 * a + 4, :], g_ref[4 * a : 4 * a + 4, :]) for a in range(4)]
        else:
            g = [jnp.where(first_core, g_ref[4 * a : 4 * a + 4, :], g_own_ref[4 * a : 4 * a + 4, :]) for a in range(4)]
        in_pre = jnp.where(first_core, g[0], g[1]) + in_bias
        forget_pre = jnp.where(first_core, g[2], g[3]) + forget_bias
        lf = log_sigmoid(forget_pre) + fx_ref[:, half * ROWS : (half + 1) * ROWS]
        for j in range(NB):
            b = half * NB + j
            i_s[b * 4 : b * 4 + 4, :] = in_pre[:, j * BLOCK : (j + 1) * BLOCK]
            f_s[b * 4 : b * 4 + 4, :] = lf[:, j * BLOCK : (j + 1) * BLOCK]
    cum = lane_scan(f_s[...], jnp.add, 0.0)
    u = i_s[...] - cum
    cmax = lane_scan(u, jnp.maximum, -jnp.inf)
    tot = jnp.broadcast_to(cum[:, BLOCK - 1 :], cum.shape)
    top = tot + jnp.broadcast_to(cmax[:, BLOCK - 1 :], cum.shape)
    u_ref[...] = u + LOG_KEY_FACTOR
    cm_ref[...] = cmax
    tot_ref[...] = tot
    bt_ref[...] = top
    ws_s[...] = jnp.exp(tot + u - top) * KEY_FACTOR
    suffix = jnp.zeros((HEADS, BLOCK), F32)
    scale = jnp.full((HEADS, BLOCK), LOWEST_LOG, F32)
    for b in reversed(range(2 * NB)):
        e = suffix + bt_ref[b * 4 : b * 4 + 4, :]
        wb_s[b * 4 : b * 4 + 4, :] = e
        scale = jnp.maximum(scale, e)
        suffix = suffix + tot_ref[b * 4 : b * 4 + 4, :]
    for b in range(2 * NB):
        wb_s[b * 4 : b * 4 + 4, :] = jnp.exp(wb_s[b * 4 : b * 4 + 4, :] - scale)
    ts_s[0:4, :] = suffix
    ts_s[4:8, :] = scale
    project(n_ref, wv_ref, v_ref)
    own_last = jnp.full((16, D), tp, jnp.int32) == 1
    last = jnp.where(own_last, n_own_ref[ROWS - 16 :, :].astype(F32), n_ref[ROWS - 16 :, :].astype(F32)).astype(BF)
    rim = dot(last, win_ref[...]).astype(BF).astype(F32) * dot(last, wcv_ref[...]).astype(BF).astype(F32)
    rim = jnp.concatenate([rim[14 + r : 15 + r, c * 128 : (c + 1) * 128] for r in range(2) for c in range(4)], axis=0)
    write_scalars(pay_ref, ts_s[...], rim)
    for h in range(HEADS):
        cols = slice(h * DH, (h + 1) * DH)
        total = jnp.zeros((DH, DH), F32)
        for slot, (kr, vr) in enumerate(((k_own_ref, v_own_ref), (k_ref, v_ref))):
            half = tp if slot == 0 else 1 - tp
            for j in range(NB):
                rows = slice(j * BLOCK, (j + 1) * BLOCK)
                r = half * 16 + (j * 4 + h)
                kt = kr[rows, cols].T
                kt_ref[r] = kt
                term = dot((kt.astype(F32) * ws_s[pl.ds(r, 1), :]).astype(BF), vr[rows, cols])
                term_ref[r] = term
                total = total + wb_s[pl.ds(r, 1), :] * term
        pay_ref[h * DH : (h + 1) * DH, :] = total.astype(BF)
    load_q.wait()


def k3a_body(n_own_ref, n_oth_ref, wi_ref, wc_ref, wq_ref, cp_own_ref, cp_oth_ref, q_own_ref, q_oth_ref):
    for n_ref, cp_ref in ((n_own_ref, cp_own_ref), (n_oth_ref, cp_oth_ref)):
        for j in range(2):
            cols = slice(j * 256, (j + 1) * 256)
            a = dot(n_ref[...], wi_ref[:, cols]).astype(BF).astype(F32)
            c = dot(n_ref[...], wc_ref[:, cols]).astype(BF).astype(F32)
            cp_ref[:, cols] = (a * c).astype(BF)
    project(n_own_ref, wq_ref, q_own_ref)
    project(n_oth_ref, wq_ref, q_oth_ref)


def c1_body(own_ref, r1_ref, r2_ref, r3_ref, pm_ref, ps_ref, pay_ref, ts_s):
    x = lax.axis_index("sp_1")
    refs = (own_ref, r1_ref, r2_ref, r3_ref)
    place = [x] + [lax.rem(x + 4 - d, 4) for d in (1, 2, 3)]
    scal = [read_scalars(r) for r in refs]
    low = jnp.full((HEADS, BLOCK), LOWEST_LOG, F32)
    xv = jnp.full((HEADS, BLOCK), x, jnp.int32)
    suffix = jnp.zeros((HEADS, BLOCK), F32)
    levels = []
    for d in (1, 2, 3):
        levels.append(jnp.where(xv >= d, scal[d][1] + suffix, low))
        suffix = suffix + jnp.where(xv >= d, scal[d][0], 0.0)
    top = jnp.maximum(jnp.maximum(levels[0], levels[1]), levels[2])
    pw = [jnp.where(xv >= d, jnp.exp(levels[d - 1] - top), 0.0) for d in (1, 2, 3)]
    ps_ref[0:4, :] = suffix
    ps_ref[4:8, :] = top
    levels = []
    for a in range(4):
        level = scal[a][1]
        for b in range(4):
            if a != b:
                later = jnp.full((HEADS, BLOCK), place[b] - place[a], jnp.int32) > 0
                level = level + jnp.where(later, scal[b][0], 0.0)
        levels.append(level)
    rtop = jnp.maximum(jnp.maximum(levels[0], levels[1]), jnp.maximum(levels[2], levels[3]))
    rw = [jnp.exp(level - rtop) for level in levels]
    ts_s[0:4, :] = scal[0][0] + scal[1][0] + scal[2][0] + scal[3][0]
    ts_s[4:8, :] = rtop
    write_scalars(pay_ref, ts_s[...], r1_ref[536:PAY, :].astype(F32))
    for h in range(HEADS):
        rows = slice(h * DH, (h + 1) * DH)
        m = [r[rows, :].astype(F32) for r in refs]
        one = slice(h, h + 1)
        pm_ref[rows, :] = pw[0][one] * m[1] + pw[1][one] * m[2] + pw[2][one] * m[3]
        pay_ref[rows, :] = (rw[0][one] * m[0] + rw[1][one] * m[1] + rw[2][one] * m[2] + rw[3][one] * m[3]).astype(BF)


def slot_rows(ref, half):
    return ref[pl.ds(pl.multiple_of(half * 16, 16), 16), :]


def columns_of(rows16, pad_s, col_s):
    pad_s[0:16, :] = rows16
    col_s[...] = pad_s[...].T


def scores_half(q_ref, kt_ref, half, s_s):
    for c in range(16):
        rows, cols = slice(c // 4 * BLOCK, (c // 4 + 1) * BLOCK), slice(c % 4 * DH, (c % 4 + 1) * DH)
        s_s[c * BLOCK : (c + 1) * BLOCK, :] = dot(q_ref[rows, cols], kt_ref[half * 16 + c])


def weights_steps(u_ref, cm_ref, half, s_s, w_s, pad_s, col_s):
    columns_of(slot_rows(cm_ref, half), pad_s, col_s)
    causal = lax.broadcasted_iota(jnp.int32, (BLOCK, BLOCK), 1) <= lax.broadcasted_iota(jnp.int32, (BLOCK, BLOCK), 0)

    def step(c):
        rows = slice(c * BLOCK, (c + 1) * BLOCK)
        log = u_ref[pl.ds(half * 16 + c, 1), :] - col_s[:, c : c + 1]
        w_s[rows, :] = (jnp.exp(jnp.where(causal, log, -jnp.inf)) * s_s[rows, :]).astype(BF)

    return [lambda c=c: step(c) for c in range(16)]


def intra_half(w_s, v_ref, out_ref):
    for c in range(16):
        rows, cols = slice(c // 4 * BLOCK, (c // 4 + 1) * BLOCK), slice(c % 4 * DH, (c % 4 + 1) * DH)
        out_ref[rows, cols] = dot(w_s[c * BLOCK : (c + 1) * BLOCK, :], v_ref[rows, cols])


def local_cols(ref, tp):
    return ref[..., pl.ds(pl.multiple_of(tp * WIDTH, WIDTH), WIDTH)].astype(F32)


def gate_half(n_ref, wo_ref, gain, out_ref, between):
    for i in range(2):
        rows = slice(i * 256, (i + 1) * 256)
        for j in range(WIDTH // 256):
            cols = slice(j * 256, (j + 1) * 256)
            raw = dot(n_ref[rows, :], wo_ref[:, cols]).astype(BF).astype(F32)
            out_ref[rows, cols] = jax.nn.sigmoid(raw) * gain[:, cols]
            for step in between[i * 2 + j :: 4]:
                step()


def conv_steps(cp_ref, before_ref, go_ref, taps, out_ref, buf_s):
    buf_s[0:16, :] = before_ref[ROWS - 16 :, :].astype(F32)

    def step(r):
        for c in range(WIDTH // 128):
            cols = slice(c * 128, (c + 1) * 128)
            new = cp_ref[r : r + 32, cols].astype(F32)
            buf_s[16 + r : 48 + r, cols] = new
            mixed = buf_s[14 + r : 46 + r, cols] * taps[0:1, cols]
            mixed = mixed + buf_s[15 + r : 47 + r, cols] * taps[1:2, cols]
            mixed = mixed + new * taps[2:3, cols]
            out_ref[r : r + 32, cols] = (go_ref[r : r + 32, cols].astype(F32) * mixed).astype(BF)

    return [lambda r=r: step(r) for r in range(0, ROWS, 32)]


def k3b_body(n_own_ref, n_oth_ref, wg_ref, wo_ref, q_own_ref, q_oth_ref, kt_ref,
             v_own_ref, v_oth_ref, u_ref, cm_ref, cp_own_ref, cp_oth_ref, gain_ref, taps_ref,
             go_own_ref, go_oth_ref, cv_own_ref, cv_oth_ref, sg_own_ref, sg_oth_ref, in_own_ref, in_oth_ref,
             pad_s, col_s, s_s, w_s, buf_s):
    tp = lax.axis_index("tp")
    pad_s[...] = jnp.zeros_like(pad_s)
    gain = local_cols(gain_ref, tp).reshape(1, WIDTH)
    taps = local_cols(taps_ref, tp)
    for slot, (q_ref, v_ref, n_ref, out, go_ref, sg_ref, cp_ref, before_ref, cv_ref) in enumerate((
        (q_own_ref, v_own_ref, n_own_ref, in_own_ref, go_own_ref, sg_own_ref, cp_own_ref, cp_oth_ref, cv_own_ref),
        (q_oth_ref, v_oth_ref, n_oth_ref, in_oth_ref, go_oth_ref, sg_oth_ref, cp_oth_ref, cp_own_ref, cv_oth_ref),
    )):
        half = tp if slot == 0 else 1 - tp
        scores_half(q_ref, kt_ref, half, s_s)
        project(n_ref, wg_ref, go_ref, WHOLE, weights_steps(u_ref, cm_ref, half, s_s, w_s, pad_s, col_s.at[slot]))
        steps = conv_steps(cp_ref, before_ref, go_ref, taps, cv_ref, buf_s)
        gate_half(n_ref, wo_ref, gain, sg_ref, [steps[j * 4 + i] for i in range(4) for j in range(4)])
        intra_half(w_s, v_ref, out)


def readout_steps(q_ref, in_ref, sg_ref, st_ref, sc_ref, cm_ref, half, out_ref, pad_s, col_s, c_s):
    for c in range(16):
        rows, cols = slice(c // 4 * BLOCK, (c // 4 + 1) * BLOCK), slice(c % 4 * DH, (c % 4 + 1) * DH)
        c_s[c * BLOCK : (c + 1) * BLOCK, :] = dot(q_ref[rows, cols], st_ref[half * 16 + c])
    cm = slot_rows(cm_ref, half)
    sc = slot_rows(sc_ref, half)
    m = jnp.maximum(cm, sc)
    columns_of(jnp.exp(cm - m), pad_s, col_s.at[0])
    columns_of(jnp.exp(sc - m), pad_s, col_s.at[1])

    def step(c):
        cols = slice(c % 4 * DH, (c % 4 + 1) * DH)
        for g in range(2):
            rows = slice(c // 4 * BLOCK + g * 64, c // 4 * BLOCK + g * 64 + 64)
            t = slice(g * 64, g * 64 + 64)
            read = col_s[1, t, c : c + 1] * c_s[c * BLOCK + g * 64 : c * BLOCK + g * 64 + 64, :] + col_s[0, t, c : c + 1] * in_ref[rows, cols]
            scale = lax.rsqrt(jnp.mean(read * read, axis=-1, keepdims=True) + EPSILON)
            out_ref[rows, cols] = (read * scale * sg_ref[rows, cols]).astype(BF)

    return [lambda c=c: step(c) for c in range(16)]


def conv_fix(cv_ref, cp_ref, go_ref, r1_ref, z1_ref, taps_ref, half, out_ref):
    tp = lax.axis_index("tp")
    x = lax.axis_index("sp_1")
    z = lax.axis_index("sp_0")
    here = jnp.full((8, BLOCK), x, jnp.int32)
    row = jnp.full((8, BLOCK), z, jnp.int32)
    rim8 = jnp.where(here > 0, r1_ref[536:PAY, :].astype(F32), jnp.where(row > 0, z1_ref[536:PAY, :].astype(F32), 0.0))
    rim = [jnp.concatenate([rim8[r * 4 + c : r * 4 + c + 1, :] for c in range(4)], axis=1) for r in range(2)]
    taps = local_cols(taps_ref, tp)
    p = jnp.concatenate([rim[0], rim[1], cp_ref[0:16, :].astype(F32)], axis=0)
    mixed = p[0:16] * taps[0:1] + p[1:17] * taps[1:2] + p[2:18] * taps[2:3]
    fixed = go_ref[0:16, :].astype(F32) * mixed
    first = jnp.full((16, WIDTH), half, jnp.int32) == 0
    out_ref[0:16, WIDTH:] = jnp.where(first, fixed, cv_ref[0:16, :].astype(F32)).astype(BF)
    out_ref[16:, WIDTH:] = cv_ref[16:, :]


def finish_half(first_steps, second_steps, a_ref, acc_s, wm_ref, wc_ref, out_ref):
    tiles = [slice(j * 256, (j + 1) * 256) for j in range(D // 256)]
    for j, cols in enumerate(tiles):
        acc_s[:, cols] = dot(a_ref[FIRST, WIDTH:], wc_ref[:, cols])
        for step in first_steps[j::8]:
            step()
    for j, cols in enumerate(tiles):
        out_ref[FIRST, cols] = (acc_s[:, cols] + dot(a_ref[FIRST, :WIDTH], wm_ref[:, cols])).astype(BF)
        for step in second_steps[j::8]:
            step()
    for cols in tiles:
        out_ref[SECOND, cols] = (dot(a_ref[SECOND, WIDTH:], wc_ref[:, cols]) + dot(a_ref[SECOND, :WIDTH], wm_ref[:, cols])).astype(BF)


def k4_body(pm_ref, ps_ref, r1_ref, r2_ref, r3_ref, x1_ref, init_ref, tot_ref, bt_ref, term_ref,
            q_ref, in_ref, sg_ref, cm_ref, cv_ref, cp_ref, go_ref, taps_ref, wm_ref, wc_ref,
            send_ref, st_ref, sc_ref, a_s, acc_s, pad_s, col_s, c_s, cs_s):
    tp = lax.axis_index("tp")
    z = lax.axis_index("sp_0")
    half = 1 - tp
    pad_s[...] = jnp.zeros_like(pad_s)
    refs = (r1_ref, r2_ref, r3_ref)
    zv = jnp.full((HEADS, BLOCK), z, jnp.int32)
    low = jnp.full((HEADS, BLOCK), LOWEST_LOG, F32)
    suffix = ps_ref[0:4, :]
    levels = [ps_ref[4:8, :]]
    for d in (1, 2, 3):
        t, s = read_scalars(refs[d - 1])
        levels.append(jnp.where(zv >= d, s + suffix, low))
        suffix = suffix + jnp.where(zv >= d, t, 0.0)
    levels.append(suffix)
    top = levels[0]
    for level in levels[1:]:
        top = jnp.maximum(top, level)
    w = [jnp.exp(level - top) for level in levels]
    for b in range(2 * NB):
        cs_s[b * 4 : b * 4 + 4, :] = top
        tot = tot_ref[b * 4 : b * 4 + 4, :] + top
        bt = bt_ref[b * 4 : b * 4 + 4, :]
        top = jnp.maximum(tot, bt)
        cs_s[32 + b * 4 : 36 + b * 4, :] = jnp.exp(tot - top)
        cs_s[64 + b * 4 : 68 + b * 4, :] = jnp.exp(bt - top)
    sc_ref[...] = cs_s[0:32, :]
    for h in range(HEADS):
        rows = slice(h * DH, (h + 1) * DH)
        one = slice(h, h + 1)
        mem = w[0][one] * pm_ref[rows, :] + w[4][one] * init_ref[h]
        for d in (1, 2, 3):
            mem = mem + w[d][one] * refs[d - 1][rows, :].astype(F32)
        for b in range(2 * NB):
            r = b * 4 + h
            st_ref[r] = mem.astype(BF)
            if b < 2 * NB - 1:
                mem = cs_s[32 + r : 33 + r, :] * mem + cs_s[64 + r : 65 + r, :] * term_ref[r]
    conv_fix(cv_ref, cp_ref, go_ref, x1_ref, r1_ref, taps_ref, half, a_s)
    steps = readout_steps(q_ref, in_ref, sg_ref, st_ref, sc_ref, cm_ref, half, a_s, pad_s, col_s, c_s)
    finish_half(steps[:8], steps[8:], a_s, acc_s, wm_ref, wc_ref, send_ref)


def k5a_body(x1_ref, z1_ref, q_ref, in_ref, sg_ref, st_ref, sc_ref, cm_ref, cv_ref, cp_ref, go_ref, taps_ref, wm_ref, wc_ref,
             part_ref, a_s, acc_s, pad_s, col_s, c_s):
    tp = lax.axis_index("tp")
    pad_s[...] = jnp.zeros_like(pad_s)
    conv_fix(cv_ref, cp_ref, go_ref, x1_ref, z1_ref, taps_ref, tp, a_s)
    steps = readout_steps(q_ref, in_ref, sg_ref, st_ref, sc_ref, cm_ref, tp, a_s, pad_s, col_s, c_s)
    finish_half(steps[:8], steps[8:], a_s, acc_s, wm_ref, wc_ref, part_ref)


def k5b_body(part_ref, recv_ref, out_hbm, buf, sem):
    copies = []
    for i in range(8):
        rows = pl.ds(i * 64, 64)
        buf[rows, :] = part_ref[rows, :] + recv_ref[rows, :]
        copies.append(pltpu.make_async_copy(buf.at[rows, :], out_hbm.at[rows, :], sem.at[i]))
        copies[-1].start()
    for copy in copies:
        copy.wait()


def in_hbm(value):
    return pltpu.with_memory_space_constraint(value, pltpu.HBM)


def rotated(value, axis, distance):
    size = lax.axis_size(axis)
    return lax.ppermute(value, axis, [(i, (i + distance) % size) for i in range(size)])


def local(
    tokens, norm_gain, w_query, w_key, w_value, w_outgate, w_gatein, w_gateout, w_convin,
    w_igate, w_fgate, input_bias, forget_bias, forget_extra, init_memory, head_gain, conv_taps,
    out_memory, out_conv,
):
    own = tokens[0]
    other = rotated(own, "tp", 1)
    fx = forget_extra[0].T
    half_act = sds((ROWS, WIDTH))
    half_f32 = sds((ROWS, WIDTH), F32)
    gflop = 2 * ROWS * D * WIDTH
    weight = sds((D, WIDTH))
    n_own, k_own, v_own, g_own, gain, wi, wf, wk, wv, win, wcv = call(
        k1_body, "k1", [HBM] * 8,
        [sds((ROWS, D)), half_act, half_act, sds((16, ROWS), F32), sds((D,)), sds((8, D)), sds((8, D))] + [weight] * 4,
        [pltpu.VMEM((ROWS, D), BF), pltpu.SemaphoreType.DMA((9,))],
        flops=3 * gflop,
    )(*[in_hbm(a) for a in (own, norm_gain, w_igate.T, w_fgate.T, w_key, w_value, w_gatein, w_convin)])
    rows32 = sds((32, BLOCK), F32)
    n_oth, v_oth, wq, kt, u, cm, tot, bt, terms, pay = call(
        k2_body, "k2", [V] * 15 + [HBM],
        [sds((ROWS, D)), half_act, weight, sds((32, DH, DH)), rows32, rows32, rows32, rows32, sds((32, DH, DH), F32), sds((PAY, DH))],
        [pltpu.VMEM((ROWS, WIDTH), BF), pltpu.VMEM((16, ROWS), F32)] + [pltpu.VMEM((32, BLOCK), F32)] * 4
        + [pltpu.VMEM((8, BLOCK), F32), pltpu.SemaphoreType.DMA],
        flops=3 * gflop,
    )(other, gain, wi, wf, wk, wv, g_own, k_own, v_own, fx, input_bias, forget_bias, n_own, win, wcv, in_hbm(w_query))
    first = [rotated(pay, "sp_1", d) for d in (1, 2, 3)]
    cp_own, cp_oth, q_own, q_oth = call(
        k3a_body, "k3a", [V] * 5, [half_act] * 4, flops=7 * gflop,
    )(n_own, n_oth, win, wcv, wq)
    pm, ps, pay2 = call(
        c1_body, "c1", [V] * 4, [sds((512, DH), F32), sds((8, BLOCK), F32), sds((PAY, DH))],
        [pltpu.VMEM((8, BLOCK), F32)], flops=2**20, vmem=8,
    )(pay, *first)
    second = [rotated(pay2, "sp_0", d) for d in (1, 2, 3)]
    square = pltpu.VMEM((BLOCK, BLOCK), F32)
    pair = pltpu.VMEM((2, BLOCK, BLOCK), F32)
    tall = pltpu.VMEM((16 * BLOCK, BLOCK), F32)
    go_own, go_oth, cv_own, cv_oth, sg_own, sg_oth, in_own, in_oth = call(
        k3b_body, "k3b", [V] * 15, [half_act] * 4 + [half_f32] * 4,
        [square, pair, tall, pltpu.VMEM((16 * BLOCK, BLOCK), BF), pltpu.VMEM((ROWS + 16, WIDTH), F32)], flops=7 * gflop,
    )(n_own, n_oth, w_gateout, w_outgate, q_own, q_oth, kt, v_own, v_oth, u, cm, cp_own, cp_oth, head_gain, conv_taps)
    wide = pltpu.VMEM((ROWS, 2 * WIDTH), BF)
    acc = pltpu.VMEM((256, D), F32)
    send, states, scales = call(
        k4_body, "k4", [V] * 20, [sds((ROWS, D)), sds((32, DH, DH)), rows32],
        [wide, acc, square, pair, tall, pltpu.VMEM((96, BLOCK), F32)], flops=3 * gflop,
    )(pm, ps, *second, first[0], init_memory[0], tot, bt, terms, q_oth, in_oth, sg_oth, cm, cv_oth, cp_oth, go_oth,
      conv_taps, out_memory, out_conv)
    recv = rotated(send, "tp", 1)
    (part,) = call(
        k5a_body, "k5a", [V] * 14, [sds((ROWS, D))], [wide, acc, square, pair, tall], flops=3 * gflop,
    )(first[0], second[0], q_own, in_own, sg_own, states, scales, cm, cv_own, cp_own, go_own, conv_taps, out_memory, out_conv)
    out = pl.pallas_call(
        k5b_body, name="k5b", in_specs=[V, V], out_specs=HBM, out_shape=sds((ROWS, D)),
        scratch_shapes=[pltpu.VMEM((ROWS, D), BF), pltpu.SemaphoreType.DMA((8,))],
        compiler_params=pltpu.CompilerParams(vmem_limit_bytes=8 * MIB),
    )(part, recv)
    return out[None]


def solution(mesh):
    finer = Mesh(
        mesh.devices.reshape(4, 4, mesh.shape["fs"], mesh.shape["tp"]), ("sp_0", "sp_1", "fs", "tp")
    )
    sp_tp = ("sp_0", "sp_1", "tp")
    by_col = P(None, "tp")
    return jax.shard_map(
        local,
        mesh=finer,
        in_specs=(
            P("fs", sp_tp, None), P(), by_col, by_col, by_col, by_col, by_col, by_col, by_col,
            P(), P(), P(), P(), P("fs", SP, "tp"), P("fs", "tp", None, None), P(), P(),
            P("tp", None), P("tp", None),
        ),
        out_specs=P("fs", sp_tp, None),
        check_vma=False,
    )
```

```python
import math

import jax
import jax.numpy as jnp
from jax import lax
from jax.experimental import pallas as pl
from jax.experimental.pallas import tpu as pltpu
from jax.sharding import Mesh
from jax.sharding import PartitionSpec as P

BF = jnp.bfloat16
F32 = jnp.float32
BLOCK = 128
DH = 128
HEADS = 4
ROWS = 512
NB = 4
WIDTH = 512
D = 2048
EPSILON = 1e-06
LOWEST_LOG = -1e30
KEY_FACTOR = DH ** (-0.5)
LOG_KEY_FACTOR = math.log(KEY_FACTOR)
PAY = 144
SP = ("sp_0", "sp_1")
V = pl.BlockSpec(memory_space=pltpu.VMEM)
HBM = pl.BlockSpec(memory_space=pltpu.HBM)
SM = pl.BlockSpec(memory_space=pltpu.SMEM)
MIB = 2**20


def sds(shape, dtype=BF):
    return jax.ShapeDtypeStruct(shape, dtype)


def call(body, name, in_specs, outs, scratch=(), flops=0, vmem=16, nbytes=4 * MIB):
    return pl.pallas_call(
        body,
        name=name,
        in_specs=in_specs,
        out_specs=[V] * len(outs),
        out_shape=outs,
        scratch_shapes=list(scratch),
        compiler_params=pltpu.CompilerParams(vmem_limit_bytes=vmem * MIB),
        cost_estimate=pl.CostEstimate(flops=flops, bytes_accessed=nbytes, transcendentals=0),
    )


def dot(a, b):
    return jnp.dot(a, b, preferred_element_type=F32)


def dot_nt(a, b):
    return lax.dot_general(a, b, (((1,), (1,)), ((), ())), preferred_element_type=F32)


def norm_rows(x_ref, n_ref, gain_ref, start, groups):
    lanes = [slice(i * 128, (i + 1) * 128) for i in range(D // 128)]
    scales = []
    for g in range(groups):
        rows = slice(start + g * 16, start + g * 16 + 16)
        total = jnp.zeros((16, 128), F32)
        for cols in lanes:
            x = x_ref[rows, cols].astype(F32)
            total = total + x * x
        mean = jnp.sum(total, axis=-1, keepdims=True) * (1.0 / D)
        scales.append(jnp.broadcast_to(lax.rsqrt(mean + EPSILON), (16, 128)))
    for cols in lanes:
        gain = jnp.broadcast_to(gain_ref[cols].astype(F32).reshape(1, 128), (16, 128))
        for g in range(groups):
            rows = slice(start + g * 16, start + g * 16 + 16)
            n_ref[rows, cols] = (x_ref[rows, cols].astype(F32) * scales[g] * gain).astype(BF)


FIRST, SECOND, WHOLE = slice(0, 256), slice(256, 512), slice(0, 512)


def project(n_ref, w, out_ref, rows=WHOLE, between=()):
    for j in range(WIDTH // 256):
        cols = slice(j * 256, (j + 1) * 256)
        out_ref[rows, cols] = dot(n_ref[rows, :], w[:, cols]).astype(BF)
        for step in between[j::2]:
            step()


def gate_rows(wi_ref, wf_ref, n_ref, g_ref):
    wg = jnp.concatenate([wi_ref[...].astype(F32), wf_ref[...].astype(F32)], axis=0).astype(BF)
    g_ref[...] = dot_nt(wg, n_ref[...])


def norm_steps(x_ref, n_ref, gain, start, count):
    return [lambda g=g: norm_rows(x_ref, n_ref, gain, start + g * 64, 4) for g in range(count // 64)]


def k1_body(t_hbm, gain_hbm, wi_hbm, wf_hbm, wk_hbm, wv_hbm,
            n_ref, k_ref, v_ref, g_ref, gain_ref, wi_ref, wf_ref, wk_ref, wv_ref,
            t_buf, sem):
    half = [pl.ds(0, 256), pl.ds(256, 256)]
    pairs = [
        (gain_hbm, gain_ref), (t_hbm.at[half[0], :], t_buf.at[half[0], :]), (t_hbm.at[half[1], :], t_buf.at[half[1], :]),
        (wk_hbm, wk_ref), (wv_hbm, wv_ref), (wi_hbm, wi_ref), (wf_hbm, wf_ref),
    ]
    copies = [pltpu.make_async_copy(src, dst, sem.at[i]) for i, (src, dst) in enumerate(pairs)]
    for copy in copies[:4]:
        copy.start()
    copies[0].wait()
    copies[1].wait()
    for copy in copies[4:]:
        copy.start()
    for step in norm_steps(t_buf, n_ref, gain_ref, 0, 256):
        step()
    copies[2].wait()
    copies[3].wait()
    project(n_ref, wk_ref, k_ref, FIRST, norm_steps(t_buf, n_ref, gain_ref, 256, 256))
    project(n_ref, wk_ref, k_ref, SECOND)
    for copy in copies[4:]:
        copy.wait()
    project(n_ref, wv_ref, v_ref)
    gate_rows(wi_ref, wf_ref, n_ref, g_ref)


def log_sigmoid(v):
    x = jnp.exp(-jnp.abs(v))
    series = x * (1.0 - x * (0.5 - x * (1.0 / 3.0 - x * 0.25)))
    return jnp.minimum(v, 0.0) - jnp.where(x < 0.01, series, jnp.log(1.0 + x))


def lane_scan(x, op, fill):
    lane = lax.broadcasted_iota(jnp.int32, x.shape, 1)
    for sh in (1, 2, 4, 8, 16, 32, 64):
        x = op(x, jnp.where(lane >= sh, pltpu.roll(x, sh, 1), fill))
    return x


def split3(x):
    a = x.astype(BF).astype(F32)
    r = x - a
    b = r.astype(BF).astype(F32)
    return a, b, r - b


def write_scalars(pay_ref, total, scale, rim):
    rows = [*split3(total), *split3(scale), jnp.zeros((2, DH), F32), rim]
    pay_ref[DH:PAY, :] = jnp.concatenate(rows, axis=0).astype(BF)


def read_scalars(pay_ref):
    s = pay_ref[DH:PAY, :].astype(F32)
    return s[0:1] + s[1:2] + s[2:3], s[3:4] + s[4:5] + s[5:6]


def read_rim(pay_ref):
    return pay_ref[DH:PAY, :].astype(F32)[8:16]


def k2_body(t_ref, gain_ref, wi_ref, wf_ref, wk_ref, wv_ref, g_own_ref, k_own_ref, v_own_ref,
            fx_ref, ib_ref, fb_ref, n_own_ref, win_hbm, wcv_hbm, wq_hbm,
            n_ref, v_ref, win_ref, wcv_ref, wq_ref, kt_ref, u_ref, cm_ref, tot_ref, bt_ref, term_ref, p0_ref, p1_ref, p2_ref, p3_ref,
            k_ref, g_ref, i_s, f_s, ws_s, wb_s, ts_s, m_s, w_sem):
    pairs = ((win_hbm, win_ref), (wcv_hbm, wcv_ref), (wq_hbm, wq_ref))
    loads = [pltpu.make_async_copy(src, dst, w_sem.at[i]) for i, (src, dst) in enumerate(pairs)]
    for load in loads:
        load.start()
    tp = lax.axis_index("tp")
    for step in norm_steps(t_ref, n_ref, gain_ref, 0, 256):
        step()
    project(n_ref, wk_ref, k_ref, FIRST, norm_steps(t_ref, n_ref, gain_ref, 256, 256))
    project(n_ref, wk_ref, k_ref, SECOND)
    gate_rows(wi_ref, wf_ref, n_ref, g_ref)
    first_core = jnp.full((HEADS, ROWS), tp, jnp.int32) == 0

    def column(ref):
        square = (8, 8)
        diagonal = lax.broadcasted_iota(jnp.int32, square, 0) == lax.broadcasted_iota(jnp.int32, square, 1)
        wide = jnp.broadcast_to(ref[...].reshape(1, 8), square)
        col = jnp.sum(jnp.where(diagonal, wide, 0.0), axis=1, keepdims=True)
        full = jnp.broadcast_to(col, (8, ROWS))
        return jnp.where(first_core, full[0:4], full[4:8])

    in_bias, forget_bias = column(ib_ref), column(fb_ref)
    for half in range(2):
        if half == 0:
            g = [jnp.where(first_core, g_own_ref[4 * a : 4 * a + 4, :], g_ref[4 * a : 4 * a + 4, :]) for a in range(4)]
        else:
            g = [jnp.where(first_core, g_ref[4 * a : 4 * a + 4, :], g_own_ref[4 * a : 4 * a + 4, :]) for a in range(4)]
        in_pre = jnp.where(first_core, g[0], g[1]) + in_bias
        forget_pre = jnp.where(first_core, g[2], g[3]) + forget_bias
        lf = log_sigmoid(forget_pre) + fx_ref[:, half * ROWS : (half + 1) * ROWS]
        for j in range(NB):
            b = half * NB + j
            i_s[b * 4 : b * 4 + 4, :] = in_pre[:, j * BLOCK : (j + 1) * BLOCK]
            f_s[b * 4 : b * 4 + 4, :] = lf[:, j * BLOCK : (j + 1) * BLOCK]
    cum = lane_scan(f_s[...], jnp.add, 0.0)
    u = i_s[...] - cum
    cmax = lane_scan(u, jnp.maximum, -jnp.inf)
    tot = jnp.broadcast_to(cum[:, BLOCK - 1 :], cum.shape)
    top = tot + jnp.broadcast_to(cmax[:, BLOCK - 1 :], cum.shape)
    u_ref[...] = u + LOG_KEY_FACTOR
    cm_ref[...] = cmax
    tot_ref[...] = tot
    bt_ref[...] = top
    ws_s[...] = jnp.exp(tot + u - top) * KEY_FACTOR
    suffix = jnp.zeros((HEADS, BLOCK), F32)
    scale = jnp.full((HEADS, BLOCK), LOWEST_LOG, F32)
    for b in reversed(range(2 * NB)):
        e = suffix + bt_ref[b * 4 : b * 4 + 4, :]
        wb_s[b * 4 : b * 4 + 4, :] = e
        scale = jnp.maximum(scale, e)
        suffix = suffix + tot_ref[b * 4 : b * 4 + 4, :]
    for b in range(2 * NB):
        wb_s[b * 4 : b * 4 + 4, :] = jnp.exp(wb_s[b * 4 : b * 4 + 4, :] - scale)
    ts_s[0:4, :] = suffix
    ts_s[4:8, :] = scale
    project(n_ref, wv_ref, v_ref)
    for load in loads:
        load.wait()
    own_last = jnp.full((16, D), tp, jnp.int32) == 1
    last = jnp.where(own_last, n_own_ref[ROWS - 16 :, :].astype(F32), n_ref[ROWS - 16 :, :].astype(F32)).astype(BF)
    rim = dot(last, win_ref[...]).astype(BF).astype(F32) * dot(last, wcv_ref[...]).astype(BF).astype(F32)
    rim = jnp.concatenate([rim[14 + r : 15 + r, c * 128 : (c + 1) * 128] for r in range(2) for c in range(4)], axis=0)
    for h in range(HEADS):
        cols = slice(h * DH, (h + 1) * DH)
        total = jnp.zeros((DH, DH), F32)
        for slot, (kr, vr) in enumerate(((k_own_ref, v_own_ref), (k_ref, v_ref))):
            half = tp if slot == 0 else 1 - tp
            for j in range(NB):
                rows = slice(j * BLOCK, (j + 1) * BLOCK)
                r = half * 16 + (j * 4 + h)
                kt = kr[rows, cols].T
                kt_ref[r] = kt
                term = dot((kt.astype(F32) * ws_s[pl.ds(r, 1), :]).astype(BF), vr[rows, cols])
                term_ref[r] = term
                total = total + wb_s[pl.ds(r, 1), :] * term
        m_s[h] = total.astype(BF)
    x = lax.axis_index("sp_1")
    for d, pay_ref in enumerate((p0_ref, p1_ref, p2_ref, p3_ref)):
        h = lax.rem(x + d, 4)
        pay_ref[0:DH, :] = m_s[h]
        write_scalars(pay_ref, ts_s[pl.ds(h, 1), :], ts_s[pl.ds(h + 4, 1), :], rim)


def k3a_body(n_own_ref, n_oth_ref, wi_ref, wc_ref, cp_own_ref, cp_oth_ref):
    for n_ref, cp_ref in ((n_own_ref, cp_own_ref), (n_oth_ref, cp_oth_ref)):
        for j in range(2):
            cols = slice(j * 256, (j + 1) * 256)
            a = dot(n_ref[...], wi_ref[:, cols]).astype(BF).astype(F32)
            c = dot(n_ref[...], wc_ref[:, cols]).astype(BF).astype(F32)
            cp_ref[:, cols] = (a * c).astype(BF)


def k3q_body(n_own_ref, n_oth_ref, wq_ref, wg_ref, q_own_ref, q_oth_ref, go_own_ref, go_oth_ref):
    for w_ref, own_ref, oth_ref in ((wq_ref, q_own_ref, q_oth_ref), (wg_ref, go_own_ref, go_oth_ref)):
        project(n_own_ref, w_ref, own_ref)
        project(n_oth_ref, w_ref, oth_ref)


def flag(value, reference):
    return jnp.full((1, DH), value, jnp.int32) > reference


def c1_body(own_ref, r1_ref, r2_ref, r3_ref, pm_ref, ps_ref, pay_ref):
    x = lax.axis_index("sp_1")
    refs = (own_ref, r1_ref, r2_ref, r3_ref)
    place = [lax.rem(x + 4 - d, 4) for d in range(4)]
    scal = [read_scalars(r) for r in refs]
    low = jnp.full((1, DH), LOWEST_LOG, F32)
    segments = [r[0:DH, :].astype(F32) for r in refs]

    def merged(inside):
        levels, total = [], jnp.zeros((1, DH), F32)
        for a in range(4):
            level = scal[a][1]
            for b in range(4):
                if a != b:
                    later = flag(place[b] - place[a], 0)
                    level = level + jnp.where(later if inside is None else later & inside[b], scal[b][0], 0.0)
            levels.append(level if inside is None else jnp.where(inside[a], level, low))
            total = total + (scal[a][0] if inside is None else jnp.where(inside[a], scal[a][0], 0.0))
        top = jnp.maximum(jnp.maximum(levels[0], levels[1]), jnp.maximum(levels[2], levels[3]))
        memory = None
        for a in range(4):
            w = jnp.exp(levels[a] - top)
            w = w if inside is None else jnp.where(inside[a], w, 0.0)
            memory = w * segments[a] if memory is None else memory + w * segments[a]
        return total, top, memory

    for e in range(4):
        target = lax.rem(x + e, 4)
        total, top, memory = merged([flag(target - place[a], 0) for a in range(4)])
        pm_ref[e] = memory
        ps_ref[e : e + 1, :] = total
        ps_ref[4 + e : 5 + e, :] = top
    total, top, memory = merged(None)
    pay_ref[0:DH, :] = memory.astype(BF)
    write_scalars(pay_ref, total, top, read_rim(r1_ref))


def c2_body(pm_ref, ps_ref, r1_ref, r2_ref, r3_ref, init_ref, s0_ref, s1_ref, s2_ref, s3_ref):
    z = lax.axis_index("sp_0")
    refs = (r1_ref, r2_ref, r3_ref)
    low = jnp.full((1, DH), LOWEST_LOG, F32)
    suffix = jnp.zeros((1, DH), F32)
    levels = []
    for d in (1, 2, 3):
        t, s = read_scalars(refs[d - 1])
        levels.append(jnp.where(flag(z, d - 1), s + suffix, low))
        suffix = suffix + jnp.where(flag(z, d - 1), t, 0.0)
    top = jnp.maximum(jnp.maximum(levels[0], levels[1]), jnp.maximum(levels[2], suffix))
    memory = jnp.exp(suffix - top) * init_ref[lax.axis_index("sp_1")]
    for d in (1, 2, 3):
        memory = memory + jnp.exp(levels[d - 1] - top) * refs[d - 1][0:DH, :].astype(F32)
    for e, out_ref in enumerate((s0_ref, s1_ref, s2_ref, s3_ref)):
        base = top + ps_ref[e : e + 1, :]
        seg = ps_ref[4 + e : 5 + e, :]
        scale = jnp.maximum(base, seg)
        out_ref[0:DH, :] = (jnp.exp(base - scale) * memory + jnp.exp(seg - scale) * pm_ref[e]).astype(BF)
        write_scalars(out_ref, base, scale, jnp.zeros((8, DH), F32))


def slot_rows(ref, half):
    return ref[pl.ds(pl.multiple_of(half * 16, 16), 16), :]


def columns_of(rows16, pad_s, col_s):
    pad_s[0:16, :] = rows16
    col_s[...] = pad_s[...].T


def scores_half(q_ref, kt_ref, half, s_s):
    for c in range(16):
        rows, cols = slice(c // 4 * BLOCK, (c // 4 + 1) * BLOCK), slice(c % 4 * DH, (c % 4 + 1) * DH)
        s_s[c * BLOCK : (c + 1) * BLOCK, :] = dot(q_ref[rows, cols], kt_ref[half * 16 + c])


def weights_steps(u_ref, cm_ref, half, s_s, w_s, pad_s, col_s):
    columns_of(slot_rows(cm_ref, half), pad_s, col_s)
    causal = lax.broadcasted_iota(jnp.int32, (BLOCK, BLOCK), 1) <= lax.broadcasted_iota(jnp.int32, (BLOCK, BLOCK), 0)

    def step(c):
        rows = slice(c * BLOCK, (c + 1) * BLOCK)
        log = u_ref[pl.ds(half * 16 + c, 1), :] - col_s[:, c : c + 1]
        w_s[rows, :] = (jnp.exp(jnp.where(causal, log, -jnp.inf)) * s_s[rows, :]).astype(BF)

    return [lambda c=c: step(c) for c in range(16)]


def intra_half(w_s, v_ref, out_ref):
    for c in range(16):
        rows, cols = slice(c // 4 * BLOCK, (c // 4 + 1) * BLOCK), slice(c % 4 * DH, (c % 4 + 1) * DH)
        out_ref[rows, cols] = dot(w_s[c * BLOCK : (c + 1) * BLOCK, :], v_ref[rows, cols])


def local_cols(ref, tp):
    return ref[..., pl.ds(pl.multiple_of(tp * WIDTH, WIDTH), WIDTH)].astype(F32)


def gate_half(n_ref, wo_ref, gain, out_ref, between):
    for i in range(2):
        rows = slice(i * 256, (i + 1) * 256)
        for j in range(WIDTH // 256):
            cols = slice(j * 256, (j + 1) * 256)
            raw = dot(n_ref[rows, :], wo_ref[:, cols]).astype(BF).astype(F32)
            out_ref[rows, cols] = jax.nn.sigmoid(raw) * gain[:, cols]
            for step in between[(i * 2 + j) * 8 : (i * 2 + j) * 8 + 8]:
                step()


def conv_steps(cp_ref, before_ref, go_ref, taps, out_ref, buf_s):
    buf_s[0:16, :] = before_ref[ROWS - 16 :, :].astype(F32)

    def step(r):
        for c in range(WIDTH // 128):
            cols = slice(c * 128, (c + 1) * 128)
            new = cp_ref[r : r + 32, cols].astype(F32)
            buf_s[16 + r : 48 + r, cols] = new
            mixed = buf_s[14 + r : 46 + r, cols] * taps[0:1, cols]
            mixed = mixed + buf_s[15 + r : 47 + r, cols] * taps[1:2, cols]
            mixed = mixed + new * taps[2:3, cols]
            out_ref[r : r + 32, cols] = (go_ref[r : r + 32, cols].astype(F32) * mixed).astype(BF)

    return [lambda r=r: step(r) for r in range(0, ROWS, 32)]


def k3b_body(n_own_ref, n_oth_ref, wo_ref, go_own_ref, go_oth_ref, q_own_ref, q_oth_ref, kt_ref,
             v_own_ref, v_oth_ref, u_ref, cm_ref, cp_own_ref, cp_oth_ref, gain_ref, taps_ref,
             cv_own_ref, cv_oth_ref, sg_own_ref, sg_oth_ref, in_own_ref, in_oth_ref,
             pad_s, col_s, s_s, w_s, buf_s):
    tp = lax.axis_index("tp")
    pad_s[...] = jnp.zeros_like(pad_s)
    gain = local_cols(gain_ref, tp).reshape(1, WIDTH)
    taps = local_cols(taps_ref, tp)
    for slot, (q_ref, v_ref, n_ref, out, go_ref, sg_ref, cp_ref, before_ref, cv_ref) in enumerate((
        (q_own_ref, v_own_ref, n_own_ref, in_own_ref, go_own_ref, sg_own_ref, cp_own_ref, cp_oth_ref, cv_own_ref),
        (q_oth_ref, v_oth_ref, n_oth_ref, in_oth_ref, go_oth_ref, sg_oth_ref, cp_oth_ref, cp_own_ref, cv_oth_ref),
    )):
        half = tp if slot == 0 else 1 - tp
        scores_half(q_ref, kt_ref, half, s_s)
        weights = weights_steps(u_ref, cm_ref, half, s_s, w_s, pad_s, col_s.at[slot])
        steps = conv_steps(cp_ref, before_ref, go_ref, taps, cv_ref, buf_s)
        gate_half(n_ref, wo_ref, gain, sg_ref, [step for pair in zip(weights, steps) for step in pair])
        intra_half(w_s, v_ref, out)


def readout_steps(q_ref, in_ref, sg_ref, st_ref, sc_ref, cm_ref, half, out_ref, pad_s, col_s, c_s):
    for c in range(16):
        rows, cols = slice(c // 4 * BLOCK, (c // 4 + 1) * BLOCK), slice(c % 4 * DH, (c % 4 + 1) * DH)
        c_s[c * BLOCK : (c + 1) * BLOCK, :] = dot(q_ref[rows, cols], st_ref[half * 16 + c])
    cm = slot_rows(cm_ref, half)
    sc = slot_rows(sc_ref, half)
    m = jnp.maximum(cm, sc)
    columns_of(jnp.exp(cm - m), pad_s, col_s.at[0])
    columns_of(jnp.exp(sc - m), pad_s, col_s.at[1])

    def step(c):
        cols = slice(c % 4 * DH, (c % 4 + 1) * DH)
        for g in range(2):
            rows = slice(c // 4 * BLOCK + g * 64, c // 4 * BLOCK + g * 64 + 64)
            t = slice(g * 64, g * 64 + 64)
            read = col_s[1, t, c : c + 1] * c_s[c * BLOCK + g * 64 : c * BLOCK + g * 64 + 64, :] + col_s[0, t, c : c + 1] * in_ref[rows, cols]
            scale = lax.rsqrt(jnp.mean(read * read, axis=-1, keepdims=True) + EPSILON)
            out_ref[rows, cols] = (read * scale * sg_ref[rows, cols]).astype(BF)

    return [lambda c=c: step(c) for c in range(16)]


def conv_fix(cv_ref, cp_ref, go_ref, r1_ref, z1_ref, taps_ref, half, out_ref):
    tp = lax.axis_index("tp")
    x = lax.axis_index("sp_1")
    z = lax.axis_index("sp_0")
    here = jnp.full((8, BLOCK), x, jnp.int32)
    row = jnp.full((8, BLOCK), z, jnp.int32)
    rim8 = jnp.where(here > 0, read_rim(r1_ref), jnp.where(row > 0, read_rim(z1_ref), 0.0))
    rim = [jnp.concatenate([rim8[r * 4 + c : r * 4 + c + 1, :] for c in range(4)], axis=1) for r in range(2)]
    taps = local_cols(taps_ref, tp)
    p = jnp.concatenate([rim[0], rim[1], cp_ref[0:16, :].astype(F32)], axis=0)
    mixed = p[0:16] * taps[0:1] + p[1:17] * taps[1:2] + p[2:18] * taps[2:3]
    fixed = go_ref[0:16, :].astype(F32) * mixed
    first = jnp.full((16, WIDTH), half, jnp.int32) == 0
    out_ref[0:16, WIDTH:] = jnp.where(first, fixed, cv_ref[0:16, :].astype(F32)).astype(BF)
    out_ref[16:, WIDTH:] = cv_ref[16:, :]


def finish_half(first_steps, second_steps, a_ref, acc_s, wm_ref, wc_ref, out_ref):
    tiles = [slice(j * 256, (j + 1) * 256) for j in range(D // 256)]
    for j, cols in enumerate(tiles):
        acc_s[:, cols] = dot(a_ref[FIRST, WIDTH:], wc_ref[:, cols])
        for step in first_steps[j::8]:
            step()
    for j, cols in enumerate(tiles):
        out_ref[FIRST, cols] = (acc_s[:, cols] + dot(a_ref[FIRST, :WIDTH], wm_ref[:, cols])).astype(BF)
        for step in second_steps[j::8]:
            step()
    for cols in tiles:
        out_ref[SECOND, cols] = (dot(a_ref[SECOND, WIDTH:], wc_ref[:, cols]) + dot(a_ref[SECOND, :WIDTH], wm_ref[:, cols])).astype(BF)


def k4_body(s0_ref, s1_ref, s2_ref, s3_ref, x1_ref, z1_ref, tot_ref, bt_ref, term_ref,
            q_ref, in_ref, sg_ref, cm_ref, cv_ref, cp_ref, go_ref, taps_ref, wm_ref, wc_ref,
            send_ref, st_ref, sc_ref, a_s, acc_s, pad_s, col_s, c_s, cs_s, top_s):
    tp = lax.axis_index("tp")
    x = lax.axis_index("sp_1")
    half = 1 - tp
    pad_s[...] = jnp.zeros_like(pad_s)
    refs = (s0_ref, s1_ref, s2_ref, s3_ref)
    heads = [lax.rem(x + 4 - d, 4) for d in range(4)]
    for d in range(4):
        top_s[pl.ds(heads[d], 1), :] = read_scalars(refs[d])[1]
    top = top_s[0:4, :]
    for b in range(2 * NB):
        cs_s[b * 4 : b * 4 + 4, :] = top
        tot = tot_ref[b * 4 : b * 4 + 4, :] + top
        bt = bt_ref[b * 4 : b * 4 + 4, :]
        top = jnp.maximum(tot, bt)
        cs_s[32 + b * 4 : 36 + b * 4, :] = jnp.exp(tot - top)
        cs_s[64 + b * 4 : 68 + b * 4, :] = jnp.exp(bt - top)
    sc_ref[...] = cs_s[0:32, :]
    for d in range(4):
        mem = refs[d][0:DH, :].astype(F32)
        for b in range(2 * NB):
            r = b * 4 + heads[d]
            st_ref[r] = mem.astype(BF)
            if b < 2 * NB - 1:
                mem = cs_s[pl.ds(32 + r, 1), :] * mem + cs_s[pl.ds(64 + r, 1), :] * term_ref[r]
    conv_fix(cv_ref, cp_ref, go_ref, x1_ref, z1_ref, taps_ref, half, a_s)
    steps = readout_steps(q_ref, in_ref, sg_ref, st_ref, sc_ref, cm_ref, half, a_s, pad_s, col_s, c_s)
    finish_half(steps[:8], steps[8:], a_s, acc_s, wm_ref, wc_ref, send_ref)


def k5a_body(x1_ref, z1_ref, q_ref, in_ref, sg_ref, st_ref, sc_ref, cm_ref, cv_ref, cp_ref, go_ref, taps_ref, wm_ref, wc_ref,
             part_ref, a_s, acc_s, pad_s, col_s, c_s):
    tp = lax.axis_index("tp")
    pad_s[...] = jnp.zeros_like(pad_s)
    conv_fix(cv_ref, cp_ref, go_ref, x1_ref, z1_ref, taps_ref, tp, a_s)
    steps = readout_steps(q_ref, in_ref, sg_ref, st_ref, sc_ref, cm_ref, tp, a_s, pad_s, col_s, c_s)
    finish_half(steps[:8], steps[8:], a_s, acc_s, wm_ref, wc_ref, part_ref)


def k5b_body(part_ref, recv_ref, out_hbm, buf, sem):
    copies = []
    for i in range(8):
        rows = pl.ds(i * 64, 64)
        buf[rows, :] = part_ref[rows, :] + recv_ref[rows, :]
        copies.append(pltpu.make_async_copy(buf.at[rows, :], out_hbm.at[rows, :], sem.at[i]))
        copies[-1].start()
    for copy in copies:
        copy.wait()


def in_hbm(value):
    return pltpu.with_memory_space_constraint(value, pltpu.HBM)


def rotated(value, axis, distance):
    size = lax.axis_size(axis)
    return lax.ppermute(value, axis, [(i, (i + distance) % size) for i in range(size)])


def local(
    tokens, norm_gain, w_query, w_key, w_value, w_outgate, w_gatein, w_gateout, w_convin,
    w_igate, w_fgate, input_bias, forget_bias, forget_extra, init_memory, head_gain, conv_taps,
    out_memory, out_conv,
):
    own = tokens[0]
    other = rotated(own, "tp", 1)
    fx = forget_extra[0].T
    half_act = sds((ROWS, WIDTH))
    half_f32 = sds((ROWS, WIDTH), F32)
    gflop = 2 * ROWS * D * WIDTH
    weight = sds((D, WIDTH))
    n_own, k_own, v_own, g_own, gain, wi, wf, wk, wv = call(
        k1_body, "k1", [HBM] * 6,
        [sds((ROWS, D)), half_act, half_act, sds((16, ROWS), F32), sds((D,)), sds((8, D)), sds((8, D))] + [weight] * 2,
        [pltpu.VMEM((ROWS, D), BF), pltpu.SemaphoreType.DMA((7,))],
        flops=3 * gflop,
    )(*[in_hbm(a) for a in (own, norm_gain, w_igate.T, w_fgate.T, w_key, w_value)])
    rows32 = sds((32, BLOCK), F32)
    payload = sds((PAY, DH))
    n_oth, v_oth, win, wcv, wq, kt, u, cm, tot, bt, terms, *pays = call(
        k2_body, "k2", [V] * 13 + [HBM] * 3,
        [sds((ROWS, D)), half_act, weight, weight, weight, sds((32, DH, DH)), rows32, rows32, rows32, rows32,
         sds((32, DH, DH), F32)] + [payload] * 4,
        [pltpu.VMEM((ROWS, WIDTH), BF), pltpu.VMEM((16, ROWS), F32)] + [pltpu.VMEM((32, BLOCK), F32)] * 4
        + [pltpu.VMEM((8, BLOCK), F32), pltpu.VMEM((HEADS, DH, DH), BF), pltpu.SemaphoreType.DMA((3,))],
        flops=3 * gflop,
    )(other, gain, wi, wf, wk, wv, g_own, k_own, v_own, fx, input_bias, forget_bias, n_own,
      in_hbm(w_gatein), in_hbm(w_convin), in_hbm(w_query))
    first = [rotated(pays[d], "sp_1", d) for d in (1, 2, 3)]
    cp_own, cp_oth = call(k3a_body, "k3a", [V] * 4, [half_act] * 2, flops=7 * gflop)(n_own, n_oth, win, wcv)
    pm, ps, pay2 = call(
        c1_body, "c1", [V] * 4, [sds((4, DH, DH), F32), sds((8, DH), F32), payload], flops=2**20, vmem=8,
    )(pays[0], *first)
    second = [rotated(pay2, "sp_0", d) for d in (1, 2, 3)]
    q_own, q_oth, go_own, go_oth = call(
        k3q_body, "k3q", [V] * 4, [half_act] * 4, flops=7 * gflop,
    )(n_own, n_oth, wq, w_gateout)
    starts = call(
        c2_body, "c2", [V] * 6, [payload] * 4, flops=2**20, vmem=8,
    )(pm, ps, *second, init_memory[0])
    third = [rotated(starts[d], "sp_1", d) for d in (1, 2, 3)]
    square = pltpu.VMEM((BLOCK, BLOCK), F32)
    pair = pltpu.VMEM((2, BLOCK, BLOCK), F32)
    tall = pltpu.VMEM((16 * BLOCK, BLOCK), F32)
    cv_own, cv_oth, sg_own, sg_oth, in_own, in_oth = call(
        k3b_body, "k3b", [V] * 16, [half_act] * 2 + [half_f32] * 4,
        [square, pair, tall, pltpu.VMEM((16 * BLOCK, BLOCK), BF), pltpu.VMEM((ROWS + 16, WIDTH), F32)], flops=7 * gflop,
    )(n_own, n_oth, w_outgate, go_own, go_oth, q_own, q_oth, kt, v_own, v_oth, u, cm, cp_own, cp_oth, head_gain, conv_taps)
    wide = pltpu.VMEM((ROWS, 2 * WIDTH), BF)
    acc = pltpu.VMEM((256, D), F32)
    send, states, scales = call(
        k4_body, "k4", [V] * 19, [sds((ROWS, D)), sds((32, DH, DH)), rows32],
        [wide, acc, square, pair, tall, pltpu.VMEM((96, BLOCK), F32), pltpu.VMEM((8, BLOCK), F32)], flops=3 * gflop,
    )(starts[0], *third, first[0], second[0], tot, bt, terms, q_oth, in_oth, sg_oth, cm, cv_oth, cp_oth, go_oth,
      conv_taps, out_memory, out_conv)
    recv = rotated(send, "tp", 1)
    (part,) = call(
        k5a_body, "k5a", [V] * 14, [sds((ROWS, D))], [wide, acc, square, pair, tall], flops=3 * gflop,
    )(first[0], second[0], q_own, in_own, sg_own, states, scales, cm, cv_own, cp_own, go_own, conv_taps, out_memory, out_conv)
    out = pl.pallas_call(
        k5b_body, name="k5b", in_specs=[V, V], out_specs=HBM, out_shape=sds((ROWS, D)),
        scratch_shapes=[pltpu.VMEM((ROWS, D), BF), pltpu.SemaphoreType.DMA((8,))],
        compiler_params=pltpu.CompilerParams(vmem_limit_bytes=8 * MIB),
    )(part, recv)
    return out[None]


def solution(mesh):
    finer = Mesh(
        mesh.devices.reshape(4, 4, mesh.shape["fs"], mesh.shape["tp"]), ("sp_0", "sp_1", "fs", "tp")
    )
    sp_tp = ("sp_0", "sp_1", "tp")
    by_col = P(None, "tp")
    return jax.shard_map(
        local,
        mesh=finer,
        in_specs=(
            P("fs", sp_tp, None), P(), by_col, by_col, by_col, by_col, by_col, by_col, by_col,
            P(), P(), P(), P(), P("fs", SP, "tp"), P("fs", "tp", None, None), P(), P(),
            P("tp", None), P("tp", None),
        ),
        out_specs=P("fs", sp_tp, None),
        check_vma=False,
    )
```

```python
import functools
import math

import jax
import jax.numpy as jnp
from jax import lax
from jax.experimental import pallas as pl
from jax.experimental.pallas import tpu as pltpu
from jax.sharding import Mesh
from jax.sharding import PartitionSpec as P

BF = jnp.bfloat16
F32 = jnp.float32
BLOCK = 128
DH = 128
HEADS = 4
ROWS = 512
NB = 4
WIDTH = 512
D = 2048
EPSILON = 1e-06
LOWEST_LOG = -1e30
KEY_FACTOR = DH ** (-0.5)
LOG_KEY_FACTOR = math.log(KEY_FACTOR)
PAY = 544
SP = ("sp_0", "sp_1")
V = pl.BlockSpec(memory_space=pltpu.VMEM)
HBM = pl.BlockSpec(memory_space=pltpu.HBM)
SM = pl.BlockSpec(memory_space=pltpu.SMEM)
MIB = 2**20


def sds(shape, dtype=BF):
    return jax.ShapeDtypeStruct(shape, dtype)


def call(body, name, in_specs, outs, scratch=(), flops=0, vmem=16, nbytes=4 * MIB):
    return pl.pallas_call(
        body,
        name=name,
        in_specs=in_specs,
        out_specs=[V] * len(outs),
        out_shape=outs,
        scratch_shapes=list(scratch),
        compiler_params=pltpu.CompilerParams(vmem_limit_bytes=vmem * MIB),
        cost_estimate=pl.CostEstimate(flops=flops, bytes_accessed=nbytes, transcendentals=0),
    )


def dot(a, b):
    return jnp.dot(a, b, preferred_element_type=F32)


def dot_nt(a, b):
    return lax.dot_general(a, b, (((1,), (1,)), ((), ())), preferred_element_type=F32)


def norm_rows(x_ref, n_ref, gain_ref, start, groups):
    lanes = [slice(i * 128, (i + 1) * 128) for i in range(D // 128)]
    scales = []
    for g in range(groups):
        rows = slice(start + g * 16, start + g * 16 + 16)
        total = jnp.zeros((16, 128), F32)
        for cols in lanes:
            x = x_ref[rows, cols].astype(F32)
            total = total + x * x
        mean = jnp.sum(total, axis=-1, keepdims=True) * (1.0 / D)
        scales.append(jnp.broadcast_to(lax.rsqrt(mean + EPSILON), (16, 128)))
    for cols in lanes:
        gain = jnp.broadcast_to(gain_ref[cols].astype(F32).reshape(1, 128), (16, 128))
        for g in range(groups):
            rows = slice(start + g * 16, start + g * 16 + 16)
            n_ref[rows, cols] = (x_ref[rows, cols].astype(F32) * scales[g] * gain).astype(BF)


FIRST, SECOND, WHOLE = slice(0, 256), slice(256, 512), slice(0, 512)


def project(n_ref, w, out_ref, rows=WHOLE, between=()):
    for j in range(WIDTH // 256):
        cols = slice(j * 256, (j + 1) * 256)
        out_ref[rows, cols] = dot(n_ref[rows, :], w[:, cols]).astype(BF)
        for step in between[j::2]:
            step()


def gate_rows(wi_ref, wf_ref, n_ref, g_ref):
    wg = jnp.concatenate([wi_ref[...].astype(F32), wf_ref[...].astype(F32)], axis=0).astype(BF)
    g_ref[...] = dot_nt(wg, n_ref[...])


def norm_steps(x_ref, n_ref, gain, start, count):
    return [lambda g=g: norm_rows(x_ref, n_ref, gain, start + g * 64, 4) for g in range(count // 64)]


def k1_body(t_hbm, gain_hbm, wi_hbm, wf_hbm, wk_hbm, wv_hbm, win_hbm, wcv_hbm,
            n_ref, k_ref, v_ref, g_ref, gain_ref, wi_ref, wf_ref, wk_ref, wv_ref, win_ref, wcv_ref,
            t_buf, sem):
    half = [pl.ds(0, 256), pl.ds(256, 256)]
    pairs = [
        (gain_hbm, gain_ref), (t_hbm.at[half[0], :], t_buf.at[half[0], :]), (wk_hbm, wk_ref), (t_hbm.at[half[1], :], t_buf.at[half[1], :]),
        (wv_hbm, wv_ref), (wi_hbm, wi_ref), (wf_hbm, wf_ref), (win_hbm, win_ref), (wcv_hbm, wcv_ref),
    ]
    copies = [pltpu.make_async_copy(src, dst, sem.at[i]) for i, (src, dst) in enumerate(pairs)]
    for copy in copies[:3]:
        copy.start()
    copies[0].wait()
    copies[1].wait()
    copies[3].start()
    copies[4].start()
    for step in norm_steps(t_buf, n_ref, gain_ref, 0, 256):
        step()
    copies[2].wait()
    copies[3].wait()
    for copy in copies[5:]:
        copy.start()
    project(n_ref, wk_ref, k_ref, FIRST, norm_steps(t_buf, n_ref, gain_ref, 256, 256))
    project(n_ref, wk_ref, k_ref, SECOND)
    for copy in copies[4:7]:
        copy.wait()
    project(n_ref, wv_ref, v_ref)
    gate_rows(wi_ref, wf_ref, n_ref, g_ref)
    for copy in copies[7:]:
        copy.wait()


def log_sigmoid(v):
    x = jnp.exp(-jnp.abs(v))
    series = x * (1.0 - x * (0.5 - x * (1.0 / 3.0 - x * 0.25)))
    return jnp.minimum(v, 0.0) - jnp.where(x < 0.01, series, jnp.log(1.0 + x))


def lane_scan(x, op, fill):
    lane = lax.broadcasted_iota(jnp.int32, x.shape, 1)
    for sh in (1, 2, 4, 8, 16, 32, 64):
        x = op(x, jnp.where(lane >= sh, pltpu.roll(x, sh, 1), fill))
    return x


def split3(x):
    a = x.astype(BF).astype(F32)
    r = x - a
    b = r.astype(BF).astype(F32)
    return a, b, r - b


def write_scalars(pay_ref, ts, rim):
    a, b, c = split3(ts)
    pay_ref[512:PAY, :] = jnp.concatenate([a, b, c, rim], axis=0).astype(BF)


def read_scalars(pay_ref):
    s = pay_ref[512:PAY, :].astype(F32)
    ts = s[0:8] + s[8:16] + s[16:24]
    return ts[0:4], ts[4:8]


def k2_body(t_ref, gain_ref, wi_ref, wf_ref, wk_ref, wv_ref, g_own_ref, k_own_ref, v_own_ref,
            fx_ref, ib_ref, fb_ref, n_own_ref, win_ref, wcv_ref, wq_hbm,
            n_ref, v_ref, wq_ref, kt_ref, u_ref, cm_ref, tot_ref, bt_ref, term_ref, pay_ref, rm_ref, ts_s,
            k_ref, g_ref, i_s, f_s, ws_s, wb_s, q_sem):
    load_q = pltpu.make_async_copy(wq_hbm, wq_ref, q_sem)
    load_q.start()
    tp = lax.axis_index("tp")
    for step in norm_steps(t_ref, n_ref, gain_ref, 0, 256):
        step()
    project(n_ref, wk_ref, k_ref, FIRST, norm_steps(t_ref, n_ref, gain_ref, 256, 256))
    project(n_ref, wk_ref, k_ref, SECOND)
    gate_rows(wi_ref, wf_ref, n_ref, g_ref)
    first_core = jnp.full((HEADS, ROWS), tp, jnp.int32) == 0

    def column(ref):
        square = (8, 8)
        diagonal = lax.broadcasted_iota(jnp.int32, square, 0) == lax.broadcasted_iota(jnp.int32, square, 1)
        wide = jnp.broadcast_to(ref[...].reshape(1, 8), square)
        col = jnp.sum(jnp.where(diagonal, wide, 0.0), axis=1, keepdims=True)
        full = jnp.broadcast_to(col, (8, ROWS))
        return jnp.where(first_core, full[0:4], full[4:8])

    in_bias, forget_bias = column(ib_ref), column(fb_ref)
    for half in range(2):
        if half == 0:
            g = [jnp.where(first_core, g_own_ref[4 * a : 4 * a + 4, :], g_ref[4 * a : 4 * a + 4, :]) for a in range(4)]
        else:
            g = [jnp.where(first_core, g_ref[4 * a : 4 * a + 4, :], g_own_ref[4 * a : 4 * a + 4, :]) for a in range(4)]
        in_pre = jnp.where(first_core, g[0], g[1]) + in_bias
        forget_pre = jnp.where(first_core, g[2], g[3]) + forget_bias
        lf = log_sigmoid(forget_pre) + fx_ref[:, half * ROWS : (half + 1) * ROWS]
        for j in range(NB):
            b = half * NB + j
            i_s[b * 4 : b * 4 + 4, :] = in_pre[:, j * BLOCK : (j + 1) * BLOCK]
            f_s[b * 4 : b * 4 + 4, :] = lf[:, j * BLOCK : (j + 1) * BLOCK]
    cum = lane_scan(f_s[...], jnp.add, 0.0)
    u = i_s[...] - cum
    cmax = lane_scan(u, jnp.maximum, -jnp.inf)
    tot = jnp.broadcast_to(cum[:, BLOCK - 1 :], cum.shape)
    top = tot + jnp.broadcast_to(cmax[:, BLOCK - 1 :], cum.shape)
    u_ref[...] = u + LOG_KEY_FACTOR
    cm_ref[...] = cmax
    tot_ref[...] = tot
    bt_ref[...] = top
    ws_s[...] = jnp.exp(tot + u - top) * KEY_FACTOR
    suffix = jnp.zeros((HEADS, BLOCK), F32)
    scale = jnp.full((HEADS, BLOCK), LOWEST_LOG, F32)
    for b in reversed(range(2 * NB)):
        e = suffix + bt_ref[b * 4 : b * 4 + 4, :]
        wb_s[b * 4 : b * 4 + 4, :] = e
        scale = jnp.maximum(scale, e)
        suffix = suffix + tot_ref[b * 4 : b * 4 + 4, :]
    for b in range(2 * NB):
        wb_s[b * 4 : b * 4 + 4, :] = jnp.exp(wb_s[b * 4 : b * 4 + 4, :] - scale)
    ts_s[0:4, :] = suffix
    ts_s[4:8, :] = scale
    project(n_ref, wv_ref, v_ref)
    own_last = jnp.full((16, D), tp, jnp.int32) == 1
    last = jnp.where(own_last, n_own_ref[ROWS - 16 :, :].astype(F32), n_ref[ROWS - 16 :, :].astype(F32)).astype(BF)
    rim = dot(last, win_ref[...]).astype(BF).astype(F32) * dot(last, wcv_ref[...]).astype(BF).astype(F32)
    rim = jnp.concatenate([rim[14 + r : 15 + r, c * 128 : (c + 1) * 128] for r in range(2) for c in range(4)], axis=0)
    write_scalars(pay_ref, ts_s[...], rim)
    for h in range(HEADS):
        cols = slice(h * DH, (h + 1) * DH)
        total = jnp.zeros((DH, DH), F32)
        for slot, (kr, vr) in enumerate(((k_own_ref, v_own_ref), (k_ref, v_ref))):
            half = tp if slot == 0 else 1 - tp
            for j in range(NB):
                rows = slice(j * BLOCK, (j + 1) * BLOCK)
                r = half * 16 + (j * 4 + h)
                kt = kr[rows, cols].T
                kt_ref[r] = kt
                term = dot((kt.astype(F32) * ws_s[pl.ds(r, 1), :]).astype(BF), vr[rows, cols])
                term_ref[r] = term
                total = total + wb_s[pl.ds(r, 1), :] * term
        rm_ref[h * DH : (h + 1) * DH, :] = total
        pay_ref[h * DH : (h + 1) * DH, :] = total.astype(BF)
    load_q.wait()


def k3a_body(n_ref, wi_ref, wc_ref, wq_ref, cp_ref, q_ref):
    for j in range(2):
        cols = slice(j * 256, (j + 1) * 256)
        a = dot(n_ref[...], wi_ref[:, cols]).astype(BF).astype(F32)
        c = dot(n_ref[...], wc_ref[:, cols]).astype(BF).astype(F32)
        cp_ref[:, cols] = (a * c).astype(BF)
    project(n_ref, wq_ref, q_ref)


def k3c_body(n_own_ref, n_oth_ref, wg_ref, wo_ref, gain_ref, go_own_ref, go_oth_ref, sg_own_ref):
    project(n_own_ref, wg_ref, go_own_ref)
    project(n_oth_ref, wg_ref, go_oth_ref)
    gain = local_cols(gain_ref, lax.axis_index("tp")).reshape(1, WIDTH)
    gate_half(n_own_ref, wo_ref, gain, sg_own_ref, ())


def joined(lower, upper):
    total = lower[0] + upper[0]
    scale = jnp.maximum(lower[1] + upper[0], upper[1])
    return total, scale, jnp.exp(lower[1] + upper[0] - scale), jnp.exp(upper[1] - scale)


def prefix_merge(partner_lower, received, prefix):
    total, scale, w_new, w_old = joined(received, prefix)
    return (
        jnp.where(partner_lower, total, prefix[0]), jnp.where(partner_lower, scale, prefix[1]),
        jnp.where(partner_lower, w_new, 0.0), jnp.where(partner_lower, w_old, 1.0),
    )


def partner_is_lower(axis, round_index):
    place = lax.axis_index(axis)
    value = lax.rem(place, 2) if round_index == 0 else place - 1
    return jnp.full((HEADS, DH), value, jnp.int32) > 0


def merge_body(axis, round_index, first, rim_from_received, *refs):
    if first:
        rm_ref, rs_ref, own_pay_ref, recv_ref, pm_out, ps_out, rm_out, rs_out, pay_ref = refs
        prefix = (jnp.zeros((HEADS, DH), F32), jnp.full((HEADS, DH), LOWEST_LOG, F32))
    else:
        rm_ref, rs_ref, pm_ref, ps_ref, rim_ref, recv_ref, pm_out, ps_out, rm_out, rs_out, pay_ref = refs
        prefix = (ps_ref[0:4, :], ps_ref[4:8, :])
    lower = partner_is_lower(axis, round_index)
    received = read_scalars(recv_ref)
    total, scale, w_new, w_old = prefix_merge(lower, received, prefix)
    ps_out[0:4, :] = total
    ps_out[4:8, :] = scale
    mine = (rs_ref[0:4, :], rs_ref[4:8, :])
    low_first = joined(received, mine)
    low_second = joined(mine, received)
    rs_out[0:4, :] = low_first[0]
    rs_out[4:8, :] = jnp.where(lower, low_first[1], low_second[1])
    r_new = jnp.where(lower, low_first[2], low_second[3])
    r_old = jnp.where(lower, low_first[3], low_second[2])
    rim_source = recv_ref if rim_from_received else (own_pay_ref if first else rim_ref)
    write_scalars(pay_ref, rs_out[...], rim_source[536:PAY, :].astype(F32))
    for h in range(HEADS):
        rows, one = slice(h * DH, (h + 1) * DH), slice(h, h + 1)
        m = recv_ref[rows, :].astype(F32)
        pm_out[rows, :] = w_new[one] * m if first else w_new[one] * m + w_old[one] * pm_ref[rows, :]
        new = r_new[one] * m + r_old[one] * rm_ref[rows, :]
        rm_out[rows, :] = new
        pay_ref[rows, :] = new.astype(BF)


def slot_rows(ref, half):
    return ref[pl.ds(pl.multiple_of(half * 16, 16), 16), :]


def columns_of(rows16, pad_s, col_s):
    pad_s[0:16, :] = rows16
    col_s[...] = pad_s[...].T


def scores_half(q_ref, kt_ref, half, s_s):
    for c in range(16):
        rows, cols = slice(c // 4 * BLOCK, (c // 4 + 1) * BLOCK), slice(c % 4 * DH, (c % 4 + 1) * DH)
        s_s[c * BLOCK : (c + 1) * BLOCK, :] = dot(q_ref[rows, cols], kt_ref[half * 16 + c])


def weights_steps(u_ref, cm_ref, half, s_s, w_s, pad_s, col_s):
    columns_of(slot_rows(cm_ref, half), pad_s, col_s)
    causal = lax.broadcasted_iota(jnp.int32, (BLOCK, BLOCK), 1) <= lax.broadcasted_iota(jnp.int32, (BLOCK, BLOCK), 0)

    def step(c):
        rows = slice(c * BLOCK, (c + 1) * BLOCK)
        log = u_ref[pl.ds(half * 16 + c, 1), :] - col_s[:, c : c + 1]
        w_s[rows, :] = (jnp.exp(jnp.where(causal, log, -jnp.inf)) * s_s[rows, :]).astype(BF)

    return [lambda c=c: step(c) for c in range(16)]


def intra_half(w_s, v_ref, out_ref):
    for c in range(16):
        rows, cols = slice(c // 4 * BLOCK, (c // 4 + 1) * BLOCK), slice(c % 4 * DH, (c % 4 + 1) * DH)
        out_ref[rows, cols] = dot(w_s[c * BLOCK : (c + 1) * BLOCK, :], v_ref[rows, cols])


def local_cols(ref, tp):
    return ref[..., pl.ds(pl.multiple_of(tp * WIDTH, WIDTH), WIDTH)].astype(F32)


def gate_half(n_ref, wo_ref, gain, out_ref, between):
    share = len(between) // 4
    for i in range(2):
        rows = slice(i * 256, (i + 1) * 256)
        for j in range(WIDTH // 256):
            cols = slice(j * 256, (j + 1) * 256)
            raw = dot(n_ref[rows, :], wo_ref[:, cols]).astype(BF).astype(F32)
            out_ref[rows, cols] = jax.nn.sigmoid(raw) * gain[:, cols]
            for step in between[(i * 2 + j) * share : (i * 2 + j + 1) * share]:
                step()


def conv_steps(cp_ref, before_ref, go_ref, taps, out_ref, buf_s):
    buf_s[0:16, :] = before_ref[ROWS - 16 :, :].astype(F32)

    def step(r):
        for c in range(WIDTH // 128):
            cols = slice(c * 128, (c + 1) * 128)
            new = cp_ref[r : r + 32, cols].astype(F32)
            buf_s[16 + r : 48 + r, cols] = new
            mixed = buf_s[14 + r : 46 + r, cols] * taps[0:1, cols]
            mixed = mixed + buf_s[15 + r : 47 + r, cols] * taps[1:2, cols]
            mixed = mixed + new * taps[2:3, cols]
            out_ref[r : r + 32, cols] = (go_ref[r : r + 32, cols].astype(F32) * mixed).astype(BF)

    return [lambda r=r: step(r) for r in range(0, ROWS, 32)]


def k3b_body(n_oth_ref, wo_ref, go_own_ref, go_oth_ref, q_own_ref, q_oth_ref, kt_ref,
             v_own_ref, v_oth_ref, u_ref, cm_ref, cp_own_ref, cp_oth_ref, gain_ref, taps_ref,
             cv_own_ref, cv_oth_ref, sg_oth_ref, in_own_ref, in_oth_ref,
             pad_s, col_s, s_s, w_s, buf_s, buf2_s):
    tp = lax.axis_index("tp")
    pad_s[...] = jnp.zeros_like(pad_s)
    gain = local_cols(gain_ref, tp).reshape(1, WIDTH)
    taps = local_cols(taps_ref, tp)
    scores_half(q_own_ref, kt_ref, tp, s_s)
    weights = weights_steps(u_ref, cm_ref, tp, s_s, w_s, pad_s, col_s.at[0])
    conv = conv_steps(cp_own_ref, cp_oth_ref, go_own_ref, taps, cv_own_ref, buf_s)
    gate_half(n_oth_ref, wo_ref, gain, sg_oth_ref, [step for pair in zip(weights, conv) for step in pair])
    intra_half(w_s, v_own_ref, in_own_ref)
    scores_half(q_oth_ref, kt_ref, 1 - tp, s_s)
    for step in weights_steps(u_ref, cm_ref, 1 - tp, s_s, w_s, pad_s, col_s.at[1]):
        step()
    intra_half(w_s, v_oth_ref, in_oth_ref)
    for step in conv_steps(cp_oth_ref, cp_own_ref, go_oth_ref, taps, cv_oth_ref, buf2_s):
        step()


def readout_steps(q_ref, in_ref, sg_ref, st_ref, sc_ref, cm_ref, half, out_ref, pad_s, col_s, c_s):
    for c in range(16):
        rows, cols = slice(c // 4 * BLOCK, (c // 4 + 1) * BLOCK), slice(c % 4 * DH, (c % 4 + 1) * DH)
        c_s[c * BLOCK : (c + 1) * BLOCK, :] = dot(q_ref[rows, cols], st_ref[half * 16 + c])
    cm = slot_rows(cm_ref, half)
    sc = slot_rows(sc_ref, half)
    m = jnp.maximum(cm, sc)
    columns_of(jnp.exp(cm - m), pad_s, col_s.at[0])
    columns_of(jnp.exp(sc - m), pad_s, col_s.at[1])

    def step(c):
        cols = slice(c % 4 * DH, (c % 4 + 1) * DH)
        for g in range(2):
            rows = slice(c // 4 * BLOCK + g * 64, c // 4 * BLOCK + g * 64 + 64)
            t = slice(g * 64, g * 64 + 64)
            read = col_s[1, t, c : c + 1] * c_s[c * BLOCK + g * 64 : c * BLOCK + g * 64 + 64, :] + col_s[0, t, c : c + 1] * in_ref[rows, cols]
            scale = lax.rsqrt(jnp.mean(read * read, axis=-1, keepdims=True) + EPSILON)
            out_ref[rows, cols] = (read * scale * sg_ref[rows, cols]).astype(BF)

    return [lambda c=c: step(c) for c in range(16)]


def conv_fix(cv_ref, cp_ref, go_ref, recv_refs, taps_ref, half, out_ref):
    tp = lax.axis_index("tp")
    x = lax.axis_index("sp_1")
    z = lax.axis_index("sp_0")
    here = jnp.full((8, BLOCK), x, jnp.int32)
    row = jnp.full((8, BLOCK), z, jnp.int32)
    rx1, rx2, rz1, rz2 = [r[536:PAY, :].astype(F32) for r in recv_refs]
    above = jnp.where(row == 0, 0.0, jnp.where(row == 2, rz2, rz1))
    rim8 = jnp.where(here == 0, above, jnp.where(here == 2, rx2, rx1))
    rim = [jnp.concatenate([rim8[r * 4 + c : r * 4 + c + 1, :] for c in range(4)], axis=1) for r in range(2)]
    taps = local_cols(taps_ref, tp)
    p = jnp.concatenate([rim[0], rim[1], cp_ref[0:16, :].astype(F32)], axis=0)
    mixed = p[0:16] * taps[0:1] + p[1:17] * taps[1:2] + p[2:18] * taps[2:3]
    fixed = go_ref[0:16, :].astype(F32) * mixed
    first = jnp.full((16, WIDTH), half, jnp.int32) == 0
    out_ref[0:16, WIDTH:] = jnp.where(first, fixed, cv_ref[0:16, :].astype(F32)).astype(BF)
    out_ref[16:, WIDTH:] = cv_ref[16:, :]


def finish_half(first_steps, second_steps, a_ref, acc_s, wm_ref, wc_ref, out_ref):
    tiles = [slice(j * 256, (j + 1) * 256) for j in range(D // 256)]
    for j, cols in enumerate(tiles):
        acc_s[:, cols] = dot(a_ref[FIRST, WIDTH:], wc_ref[:, cols])
        for step in first_steps[j::8]:
            step()
    for j, cols in enumerate(tiles):
        out_ref[FIRST, cols] = (acc_s[:, cols] + dot(a_ref[FIRST, :WIDTH], wm_ref[:, cols])).astype(BF)
        for step in second_steps[j::8]:
            step()
    for cols in tiles:
        out_ref[SECOND, cols] = (dot(a_ref[SECOND, WIDTH:], wc_ref[:, cols]) + dot(a_ref[SECOND, :WIDTH], wm_ref[:, cols])).astype(BF)


def k4_body(pm_ref, ps_ref, rx1_ref, rx2_ref, rz1_ref, rz2_ref, init_ref, tot_ref, bt_ref, term_ref,
            q_ref, in_ref, sg_ref, cm_ref, cv_ref, cp_ref, go_ref, taps_ref, wm_ref, wc_ref,
            send_ref, st_ref, sc_ref, a_s, acc_s, pad_s, col_s, c_s, cs_s):
    tp = lax.axis_index("tp")
    half = 1 - tp
    pad_s[...] = jnp.zeros_like(pad_s)
    recv_refs = (rx1_ref, rx2_ref, rz1_ref, rz2_ref)
    total, scale, w_new, w_old = prefix_merge(
        partner_is_lower("sp_0", 1), read_scalars(rz2_ref), (ps_ref[0:4, :], ps_ref[4:8, :])
    )
    top = jnp.maximum(total, scale)
    w_init = jnp.exp(total - top)
    w_prefix = jnp.exp(scale - top)
    for b in range(2 * NB):
        cs_s[b * 4 : b * 4 + 4, :] = top
        tot = tot_ref[b * 4 : b * 4 + 4, :] + top
        bt = bt_ref[b * 4 : b * 4 + 4, :]
        top = jnp.maximum(tot, bt)
        cs_s[32 + b * 4 : 36 + b * 4, :] = jnp.exp(tot - top)
        cs_s[64 + b * 4 : 68 + b * 4, :] = jnp.exp(bt - top)
    sc_ref[...] = cs_s[0:32, :]
    for h in range(HEADS):
        rows = slice(h * DH, (h + 1) * DH)
        one = slice(h, h + 1)
        prefix = w_new[one] * rz2_ref[rows, :].astype(F32) + w_old[one] * pm_ref[rows, :]
        mem = w_init[one] * init_ref[h] + w_prefix[one] * prefix
        for b in range(2 * NB):
            r = b * 4 + h
            st_ref[r] = mem.astype(BF)
            if b < 2 * NB - 1:
                mem = cs_s[32 + r : 33 + r, :] * mem + cs_s[64 + r : 65 + r, :] * term_ref[r]
    conv_fix(cv_ref, cp_ref, go_ref, recv_refs, taps_ref, half, a_s)
    steps = readout_steps(q_ref, in_ref, sg_ref, st_ref, sc_ref, cm_ref, half, a_s, pad_s, col_s, c_s)
    finish_half(steps[:8], steps[8:], a_s, acc_s, wm_ref, wc_ref, send_ref)


def k5a_body(rx1_ref, rx2_ref, rz1_ref, rz2_ref, q_ref, in_ref, sg_ref, st_ref, sc_ref, cm_ref, cv_ref, cp_ref, go_ref, taps_ref, wm_ref, wc_ref,
             part_ref, a_s, acc_s, pad_s, col_s, c_s):
    tp = lax.axis_index("tp")
    pad_s[...] = jnp.zeros_like(pad_s)
    conv_fix(cv_ref, cp_ref, go_ref, (rx1_ref, rx2_ref, rz1_ref, rz2_ref), taps_ref, tp, a_s)
    steps = readout_steps(q_ref, in_ref, sg_ref, st_ref, sc_ref, cm_ref, tp, a_s, pad_s, col_s, c_s)
    finish_half(steps[:8], steps[8:], a_s, acc_s, wm_ref, wc_ref, part_ref)


def k5b_body(part_ref, recv_ref, out_hbm, buf, sem):
    copies = []
    for i in range(8):
        rows = pl.ds(i * 64, 64)
        buf[rows, :] = part_ref[rows, :] + recv_ref[rows, :]
        copies.append(pltpu.make_async_copy(buf.at[rows, :], out_hbm.at[rows, :], sem.at[i]))
        copies[-1].start()
    for copy in copies:
        copy.wait()


def swapped(value, axis, mask):
    return lax.ppermute(value, axis, [(i, i ^ mask) for i in range(lax.axis_size(axis))])


def in_hbm(value):
    return pltpu.with_memory_space_constraint(value, pltpu.HBM)


def rotated(value, axis, distance):
    size = lax.axis_size(axis)
    return lax.ppermute(value, axis, [(i, (i + distance) % size) for i in range(size)])


def local(
    tokens, norm_gain, w_query, w_key, w_value, w_outgate, w_gatein, w_gateout, w_convin,
    w_igate, w_fgate, input_bias, forget_bias, forget_extra, init_memory, head_gain, conv_taps,
    out_memory, out_conv,
):
    own = tokens[0]
    other = rotated(own, "tp", 1)
    fx = forget_extra[0].T
    half_act = sds((ROWS, WIDTH))
    half_f32 = sds((ROWS, WIDTH), F32)
    gflop = 2 * ROWS * D * WIDTH
    weight = sds((D, WIDTH))
    n_own, k_own, v_own, g_own, gain, wi, wf, wk, wv, win, wcv = call(
        k1_body, "k1", [HBM] * 8,
        [sds((ROWS, D)), half_act, half_act, sds((16, ROWS), F32), sds((D,)), sds((8, D)), sds((8, D))] + [weight] * 4,
        [pltpu.VMEM((ROWS, D), BF), pltpu.SemaphoreType.DMA((9,))],
        flops=3 * gflop,
    )(*[in_hbm(a) for a in (own, norm_gain, w_igate.T, w_fgate.T, w_key, w_value, w_gatein, w_convin)])
    rows32 = sds((32, BLOCK), F32)
    state, scal = sds((512, DH), F32), sds((8, DH), F32)
    n_oth, v_oth, wq, kt, u, cm, tot, bt, terms, pay, rm, rs = call(
        k2_body, "k2", [V] * 15 + [HBM],
        [sds((ROWS, D)), half_act, weight, sds((32, DH, DH)), rows32, rows32, rows32, rows32, sds((32, DH, DH), F32), sds((PAY, DH)), state, scal],
        [pltpu.VMEM((ROWS, WIDTH), BF), pltpu.VMEM((16, ROWS), F32)] + [pltpu.VMEM((32, BLOCK), F32)] * 4
        + [pltpu.SemaphoreType.DMA],
        flops=3 * gflop,
    )(other, gain, wi, wf, wk, wv, g_own, k_own, v_own, fx, input_bias, forget_bias, n_own, win, wcv, in_hbm(w_query))
    merged = [state, scal, state, scal, sds((PAY, DH))]

    def merge(name, axis, index, first, from_received, *args):
        body = functools.partial(merge_body, axis, index, first, from_received)
        return call(body, name, [V] * len(args), merged, flops=2**20, vmem=8)(*args)

    def cover(name, n, win, wcv, wq):
        return call(k3a_body, name, [V] * 4, [half_act] * 2, flops=5 * gflop)(n, win, wcv, wq)

    rx1 = swapped(pay, "sp_1", 1)
    cp_own, q_own = cover("k3a", n_own, win, wcv, wq)
    pm, ps, rm, rs, pay = merge("c1", "sp_1", 0, True, False, rm, rs, pay, rx1)
    rx2 = swapped(pay, "sp_1", 3)
    cp_oth, q_oth = cover("k3o", n_oth, win, wcv, wq)
    pm, ps, rm, rs, pay = merge("c2", "sp_1", 1, False, True, rm, rs, pm, ps, pay, rx2)
    rz1 = swapped(pay, "sp_0", 1)
    go_own, go_oth, sg_own = call(
        k3c_body, "k3c", [V] * 5, [half_act, half_act, half_f32], flops=5 * gflop,
    )(n_own, n_oth, w_gateout, w_outgate, head_gain)
    pm, ps, _, _, pay = merge("c3", "sp_0", 0, False, False, rm, rs, pm, ps, pay, rz1)
    rz2 = swapped(pay, "sp_0", 3)
    received = (rx1, rx2, rz1, rz2)
    square = pltpu.VMEM((BLOCK, BLOCK), F32)
    pair = pltpu.VMEM((2, BLOCK, BLOCK), F32)
    tall = pltpu.VMEM((16 * BLOCK, BLOCK), F32)
    pad_rows = pltpu.VMEM((ROWS + 16, WIDTH), F32)
    cv_own, cv_oth, sg_oth, in_own, in_oth = call(
        k3b_body, "k3b", [V] * 15, [half_act] * 2 + [half_f32] * 3,
        [square, pair, tall, pltpu.VMEM((16 * BLOCK, BLOCK), BF), pad_rows, pad_rows], flops=5 * gflop,
    )(n_oth, w_outgate, go_own, go_oth, q_own, q_oth, kt, v_own, v_oth, u, cm, cp_own, cp_oth, head_gain, conv_taps)
    wide = pltpu.VMEM((ROWS, 2 * WIDTH), BF)
    acc = pltpu.VMEM((256, D), F32)
    send, states, scales = call(
        k4_body, "k4", [V] * 20, [sds((ROWS, D)), sds((32, DH, DH)), rows32],
        [wide, acc, square, pair, tall, pltpu.VMEM((96, BLOCK), F32)], flops=3 * gflop,
    )(pm, ps, *received, init_memory[0], tot, bt, terms, q_oth, in_oth, sg_oth, cm, cv_oth, cp_oth, go_oth,
      conv_taps, out_memory, out_conv)
    recv = rotated(send, "tp", 1)
    (part,) = call(
        k5a_body, "k5a", [V] * 16, [sds((ROWS, D))], [wide, acc, square, pair, tall], flops=3 * gflop,
    )(*received, q_own, in_own, sg_own, states, scales, cm, cv_own, cp_own, go_own, conv_taps, out_memory, out_conv)
    out = pl.pallas_call(
        k5b_body, name="k5b", in_specs=[V, V], out_specs=HBM, out_shape=sds((ROWS, D)),
        scratch_shapes=[pltpu.VMEM((ROWS, D), BF), pltpu.SemaphoreType.DMA((8,))],
        compiler_params=pltpu.CompilerParams(vmem_limit_bytes=8 * MIB),
    )(part, recv)
    return out[None]


def solution(mesh):
    finer = Mesh(
        mesh.devices.reshape(4, 4, mesh.shape["fs"], mesh.shape["tp"]), ("sp_0", "sp_1", "fs", "tp")
    )
    sp_tp = ("sp_0", "sp_1", "tp")
    by_col = P(None, "tp")
    return jax.shard_map(
        local,
        mesh=finer,
        in_specs=(
            P("fs", sp_tp, None), P(), by_col, by_col, by_col, by_col, by_col, by_col, by_col,
            P(), P(), P(), P(), P("fs", SP, "tp"), P("fs", "tp", None, None), P(), P(),
            P("tp", None), P("tp", None),
        ),
        out_specs=P("fs", sp_tp, None),
        check_vma=False,
    )
```

```python
import functools
import math

import jax
import jax.numpy as jnp
from jax import lax
from jax.experimental import pallas as pl
from jax.experimental.pallas import tpu as pltpu
from jax.sharding import Mesh
from jax.sharding import PartitionSpec as P

BF = jnp.bfloat16
F32 = jnp.float32
BLOCK = 128
DH = 128
HEADS = 4
ROWS = 512
NB = 4
WIDTH = 512
D = 2048
EPSILON = 1e-06
LOWEST_LOG = -1e30
KEY_FACTOR = DH ** (-0.5)
LOG_KEY_FACTOR = math.log(KEY_FACTOR)
PAY = 544
SP = ("sp_0", "sp_1")
V = pl.BlockSpec(memory_space=pltpu.VMEM)
HBM = pl.BlockSpec(memory_space=pltpu.HBM)
SM = pl.BlockSpec(memory_space=pltpu.SMEM)
MIB = 2**20


def sds(shape, dtype=BF):
    return jax.ShapeDtypeStruct(shape, dtype)


def call(body, name, in_specs, outs, scratch=(), flops=0, vmem=16, nbytes=4 * MIB):
    return pl.pallas_call(
        body,
        name=name,
        in_specs=in_specs,
        out_specs=[V] * len(outs),
        out_shape=outs,
        scratch_shapes=list(scratch),
        compiler_params=pltpu.CompilerParams(vmem_limit_bytes=vmem * MIB),
        cost_estimate=pl.CostEstimate(flops=flops, bytes_accessed=nbytes, transcendentals=0),
    )


def dot(a, b):
    return jnp.dot(a, b, preferred_element_type=F32)


def dot_nt(a, b):
    return lax.dot_general(a, b, (((1,), (1,)), ((), ())), preferred_element_type=F32)


def norm_rows(x_ref, n_ref, gain_ref, start, groups):
    lanes = [slice(i * 128, (i + 1) * 128) for i in range(D // 128)]
    scales = []
    for g in range(groups):
        rows = slice(start + g * 16, start + g * 16 + 16)
        total = jnp.zeros((16, 128), F32)
        for cols in lanes:
            x = x_ref[rows, cols].astype(F32)
            total = total + x * x
        mean = jnp.sum(total, axis=-1, keepdims=True) * (1.0 / D)
        scales.append(jnp.broadcast_to(lax.rsqrt(mean + EPSILON), (16, 128)))
    for cols in lanes:
        gain = jnp.broadcast_to(gain_ref[cols].astype(F32).reshape(1, 128), (16, 128))
        for g in range(groups):
            rows = slice(start + g * 16, start + g * 16 + 16)
            n_ref[rows, cols] = (x_ref[rows, cols].astype(F32) * scales[g] * gain).astype(BF)


FIRST, SECOND, WHOLE = slice(0, 256), slice(256, 512), slice(0, 512)


def project(n_ref, w, out_ref, rows=WHOLE, between=()):
    for j in range(WIDTH // 256):
        cols = slice(j * 256, (j + 1) * 256)
        out_ref[rows, cols] = dot(n_ref[rows, :], w[:, cols]).astype(BF)
        for step in between[j::2]:
            step()


def gate_rows(wi_ref, wf_ref, n_ref, g_ref):
    wg = jnp.concatenate([wi_ref[...].astype(F32), wf_ref[...].astype(F32)], axis=0).astype(BF)
    g_ref[...] = dot_nt(wg, n_ref[...])


def norm_steps(x_ref, n_ref, gain, start, count):
    return [lambda g=g: norm_rows(x_ref, n_ref, gain, start + g * 64, 4) for g in range(count // 64)]


def k1_body(t_hbm, gain_hbm, wi_hbm, wf_hbm, wk_hbm, wv_hbm, win_hbm, wcv_hbm,
            n_ref, k_ref, v_ref, g_ref, gain_ref, wi_ref, wf_ref, wk_ref, wv_ref, win_ref, wcv_ref,
            t_buf, sem):
    quarter = [pl.ds(i * 64, 64) for i in range(4)]
    late = pl.ds(256, 256)
    pairs = [(gain_hbm, gain_ref)] + [(t_hbm.at[rows, :], t_buf.at[rows, :]) for rows in quarter]
    pairs += [(wk_hbm, wk_ref), (t_hbm.at[late, :], t_buf.at[late, :])]
    pairs += [(wi_hbm, wi_ref), (wf_hbm, wf_ref), (wv_hbm, wv_ref), (win_hbm, win_ref), (wcv_hbm, wcv_ref)]
    copies = [pltpu.make_async_copy(src, dst, sem.at[i]) for i, (src, dst) in enumerate(pairs)]
    for copy in copies[:7]:
        copy.start()
    for copy in copies[:5]:
        copy.wait()
    for copy in copies[7:]:
        copy.start()
    for step in norm_steps(t_buf, n_ref, gain_ref, 0, 256):
        step()
    copies[5].wait()
    copies[6].wait()
    project(n_ref, wk_ref, k_ref, FIRST, norm_steps(t_buf, n_ref, gain_ref, 256, 256))
    project(n_ref, wk_ref, k_ref, SECOND)
    for copy in copies[7:10]:
        copy.wait()
    project(n_ref, wv_ref, v_ref)
    gate_rows(wi_ref, wf_ref, n_ref, g_ref)
    for copy in copies[10:]:
        copy.wait()


def log_sigmoid(v):
    x = jnp.exp(-jnp.abs(v))
    series = x * (1.0 - x * (0.5 - x * (1.0 / 3.0 - x * 0.25)))
    return jnp.minimum(v, 0.0) - jnp.where(x < 0.01, series, jnp.log(1.0 + x))


def lane_scan(x, op, fill):
    lane = lax.broadcasted_iota(jnp.int32, x.shape, 1)
    for sh in (1, 2, 4, 8, 16, 32, 64):
        x = op(x, jnp.where(lane >= sh, pltpu.roll(x, sh, 1), fill))
    return x


def split3(x):
    a = x.astype(BF).astype(F32)
    r = x - a
    b = r.astype(BF).astype(F32)
    return a, b, r - b


def write_scalars(pay_ref, ts, rim):
    a, b, c = split3(ts)
    pay_ref[512:PAY, :] = jnp.concatenate([a, b, c, rim], axis=0).astype(BF)


def read_scalars(pay_ref):
    s = pay_ref[512:PAY, :].astype(F32)
    ts = s[0:8] + s[8:16] + s[16:24]
    return ts[0:4], ts[4:8]


def k2_body(t_ref, gain_ref, wi_ref, wf_ref, wk_ref, wv_ref, g_own_ref, k_own_ref, v_own_ref,
            fx_ref, ib_ref, fb_ref, n_own_ref, win_ref, wcv_ref, wq_hbm,
            n_ref, v_ref, wq_ref, kt_ref, u_ref, cm_ref, tot_ref, bt_ref, term_ref, pay_ref, rm_ref, ts_s,
            k_ref, g_ref, i_s, f_s, ws_s, wb_s, q_sem):
    load_q = pltpu.make_async_copy(wq_hbm, wq_ref, q_sem)
    load_q.start()
    tp = lax.axis_index("tp")
    for step in norm_steps(t_ref, n_ref, gain_ref, 0, 256):
        step()
    project(n_ref, wk_ref, k_ref, FIRST, norm_steps(t_ref, n_ref, gain_ref, 256, 256))
    project(n_ref, wk_ref, k_ref, SECOND)
    gate_rows(wi_ref, wf_ref, n_ref, g_ref)
    first_core = jnp.full((HEADS, ROWS), tp, jnp.int32) == 0

    def column(ref):
        square = (8, 8)
        diagonal = lax.broadcasted_iota(jnp.int32, square, 0) == lax.broadcasted_iota(jnp.int32, square, 1)
        wide = jnp.broadcast_to(ref[...].reshape(1, 8), square)
        col = jnp.sum(jnp.where(diagonal, wide, 0.0), axis=1, keepdims=True)
        full = jnp.broadcast_to(col, (8, ROWS))
        return jnp.where(first_core, full[0:4], full[4:8])

    in_bias, forget_bias = column(ib_ref), column(fb_ref)
    for half in range(2):
        if half == 0:
            g = [jnp.where(first_core, g_own_ref[4 * a : 4 * a + 4, :], g_ref[4 * a : 4 * a + 4, :]) for a in range(4)]
        else:
            g = [jnp.where(first_core, g_ref[4 * a : 4 * a + 4, :], g_own_ref[4 * a : 4 * a + 4, :]) for a in range(4)]
        in_pre = jnp.where(first_core, g[0], g[1]) + in_bias
        forget_pre = jnp.where(first_core, g[2], g[3]) + forget_bias
        lf = log_sigmoid(forget_pre) + fx_ref[:, half * ROWS : (half + 1) * ROWS]
        for j in range(NB):
            b = half * NB + j
            i_s[b * 4 : b * 4 + 4, :] = in_pre[:, j * BLOCK : (j + 1) * BLOCK]
            f_s[b * 4 : b * 4 + 4, :] = lf[:, j * BLOCK : (j + 1) * BLOCK]
    cum = lane_scan(f_s[...], jnp.add, 0.0)
    u = i_s[...] - cum
    cmax = lane_scan(u, jnp.maximum, -jnp.inf)
    tot = jnp.broadcast_to(cum[:, BLOCK - 1 :], cum.shape)
    top = tot + jnp.broadcast_to(cmax[:, BLOCK - 1 :], cum.shape)
    u_ref[...] = u + LOG_KEY_FACTOR
    cm_ref[...] = cmax
    tot_ref[...] = tot
    bt_ref[...] = top
    ws_s[...] = jnp.exp(tot + u - top) * KEY_FACTOR
    suffix = jnp.zeros((HEADS, BLOCK), F32)
    scale = jnp.full((HEADS, BLOCK), LOWEST_LOG, F32)
    for b in reversed(range(2 * NB)):
        e = suffix + bt_ref[b * 4 : b * 4 + 4, :]
        wb_s[b * 4 : b * 4 + 4, :] = e
        scale = jnp.maximum(scale, e)
        suffix = suffix + tot_ref[b * 4 : b * 4 + 4, :]
    for b in range(2 * NB):
        wb_s[b * 4 : b * 4 + 4, :] = jnp.exp(wb_s[b * 4 : b * 4 + 4, :] - scale)
    ts_s[0:4, :] = suffix
    ts_s[4:8, :] = scale
    project(n_ref, wv_ref, v_ref)
    own_last = jnp.full((16, D), tp, jnp.int32) == 1
    last = jnp.where(own_last, n_own_ref[ROWS - 16 :, :].astype(F32), n_ref[ROWS - 16 :, :].astype(F32)).astype(BF)
    rim = dot(last, win_ref[...]).astype(BF).astype(F32) * dot(last, wcv_ref[...]).astype(BF).astype(F32)
    rim = jnp.concatenate([rim[14 + r : 15 + r, c * 128 : (c + 1) * 128] for r in range(2) for c in range(4)], axis=0)
    write_scalars(pay_ref, ts_s[...], rim)
    for h in range(HEADS):
        cols = slice(h * DH, (h + 1) * DH)
        total = jnp.zeros((DH, DH), F32)
        for slot, (kr, vr) in enumerate(((k_own_ref, v_own_ref), (k_ref, v_ref))):
            half = tp if slot == 0 else 1 - tp
            for j in range(NB):
                rows = slice(j * BLOCK, (j + 1) * BLOCK)
                r = half * 16 + (j * 4 + h)
                kt = kr[rows, cols].T
                kt_ref[r] = kt
                term = dot((kt.astype(F32) * ws_s[pl.ds(r, 1), :]).astype(BF), vr[rows, cols])
                term_ref[r] = term
                total = total + wb_s[pl.ds(r, 1), :] * term
        rm_ref[h * DH : (h + 1) * DH, :] = total
        pay_ref[h * DH : (h + 1) * DH, :] = total.astype(BF)
    load_q.wait()


def k3a_body(n_ref, wi_ref, wc_ref, wq_ref, cp_ref, q_ref):
    for j in range(2):
        cols = slice(j * 256, (j + 1) * 256)
        a = dot(n_ref[...], wi_ref[:, cols]).astype(BF).astype(F32)
        c = dot(n_ref[...], wc_ref[:, cols]).astype(BF).astype(F32)
        cp_ref[:, cols] = (a * c).astype(BF)
    project(n_ref, wq_ref, q_ref)


def k3c_body(n_own_ref, n_oth_ref, wg_ref, wo_ref, gain_ref, go_own_ref, go_oth_ref, sg_own_ref):
    project(n_own_ref, wg_ref, go_own_ref)
    project(n_oth_ref, wg_ref, go_oth_ref)
    gain = local_cols(gain_ref, lax.axis_index("tp")).reshape(1, WIDTH)
    gate_half(n_own_ref, wo_ref, gain, sg_own_ref, ())


def joined(lower, upper):
    total = lower[0] + upper[0]
    scale = jnp.maximum(lower[1] + upper[0], upper[1])
    return total, scale, jnp.exp(lower[1] + upper[0] - scale), jnp.exp(upper[1] - scale)


def prefix_merge(partner_lower, received, prefix):
    total, scale, w_new, w_old = joined(received, prefix)
    return (
        jnp.where(partner_lower, total, prefix[0]), jnp.where(partner_lower, scale, prefix[1]),
        jnp.where(partner_lower, w_new, 0.0), jnp.where(partner_lower, w_old, 1.0),
    )


def partner_is_lower(axis, round_index):
    place = lax.axis_index(axis)
    value = lax.rem(place, 2) if round_index == 0 else place - 1
    return jnp.full((HEADS, DH), value, jnp.int32) > 0


def merge_body(axis, round_index, first, rim_from_received, last, *refs):
    if last:
        rm_ref, rs_ref, pm_ref, ps_ref, rim_ref, recv_ref, pm_out, ps_out, pay_ref, rm_out, rs_out = refs
        prefix = (ps_ref[0:4, :], ps_ref[4:8, :])
    elif first:
        rm_ref, rs_ref, own_pay_ref, recv_ref, pm_out, ps_out, rm_out, rs_out, pay_ref = refs
        prefix = (jnp.zeros((HEADS, DH), F32), jnp.full((HEADS, DH), LOWEST_LOG, F32))
    else:
        rm_ref, rs_ref, pm_ref, ps_ref, rim_ref, recv_ref, pm_out, ps_out, rm_out, rs_out, pay_ref = refs
        prefix = (ps_ref[0:4, :], ps_ref[4:8, :])
    lower = partner_is_lower(axis, round_index)
    received = read_scalars(recv_ref)
    total, scale, w_new, w_old = prefix_merge(lower, received, prefix)
    ps_out[0:4, :] = total
    ps_out[4:8, :] = scale
    mine = (rs_ref[0:4, :], rs_ref[4:8, :])
    low_first = joined(received, mine)
    low_second = joined(mine, received)
    rs_out[0:4, :] = low_first[0]
    rs_out[4:8, :] = jnp.where(lower, low_first[1], low_second[1])
    r_new = jnp.where(lower, low_first[2], low_second[3])
    r_old = jnp.where(lower, low_first[3], low_second[2])
    rim_source = recv_ref if rim_from_received else (own_pay_ref if first else rim_ref)
    write_scalars(pay_ref, rs_out[...], rim_source[536:PAY, :].astype(F32))
    for h in range(HEADS):
        rows, one = slice(h * DH, (h + 1) * DH), slice(h, h + 1)
        m = recv_ref[rows, :].astype(F32)
        pm_out[rows, :] = w_new[one] * m if first else w_new[one] * m + w_old[one] * pm_ref[rows, :]
        new = r_new[one] * m + r_old[one] * rm_ref[rows, :]
        rm_out[rows, :] = new
        pay_ref[rows, :] = new.astype(BF)


def slot_rows(ref, half):
    return ref[pl.ds(pl.multiple_of(half * 16, 16), 16), :]


def columns_of(rows16, pad_s, col_s):
    pad_s[0:16, :] = rows16
    col_s[...] = pad_s[...].T


def scores_half(q_ref, kt_ref, half, s_s):
    for c in range(16):
        rows, cols = slice(c // 4 * BLOCK, (c // 4 + 1) * BLOCK), slice(c % 4 * DH, (c % 4 + 1) * DH)
        s_s[c * BLOCK : (c + 1) * BLOCK, :] = dot(q_ref[rows, cols], kt_ref[half * 16 + c])


def weights_steps(u_ref, cm_ref, half, s_s, w_s, pad_s, col_s):
    columns_of(slot_rows(cm_ref, half), pad_s, col_s)
    causal = lax.broadcasted_iota(jnp.int32, (BLOCK, BLOCK), 1) <= lax.broadcasted_iota(jnp.int32, (BLOCK, BLOCK), 0)

    def step(c):
        rows = slice(c * BLOCK, (c + 1) * BLOCK)
        log = u_ref[pl.ds(half * 16 + c, 1), :] - col_s[:, c : c + 1]
        w_s[rows, :] = (jnp.exp(jnp.where(causal, log, -jnp.inf)) * s_s[rows, :]).astype(BF)

    return [lambda c=c: step(c) for c in range(16)]


def intra_half(w_s, v_ref, out_ref):
    for c in range(16):
        rows, cols = slice(c // 4 * BLOCK, (c // 4 + 1) * BLOCK), slice(c % 4 * DH, (c % 4 + 1) * DH)
        out_ref[rows, cols] = dot(w_s[c * BLOCK : (c + 1) * BLOCK, :], v_ref[rows, cols])


def local_cols(ref, tp):
    return ref[..., pl.ds(pl.multiple_of(tp * WIDTH, WIDTH), WIDTH)].astype(F32)


def gate_half(n_ref, wo_ref, gain, out_ref, between):
    share = len(between) // 4
    for i in range(2):
        rows = slice(i * 256, (i + 1) * 256)
        for j in range(WIDTH // 256):
            cols = slice(j * 256, (j + 1) * 256)
            raw = dot(n_ref[rows, :], wo_ref[:, cols]).astype(BF).astype(F32)
            out_ref[rows, cols] = jax.nn.sigmoid(raw) * gain[:, cols]
            for step in between[(i * 2 + j) * share : (i * 2 + j + 1) * share]:
                step()


def conv_steps(cp_ref, before_ref, go_ref, taps, out_ref, buf_s):
    buf_s[0:16, :] = before_ref[ROWS - 16 :, :].astype(F32)

    def step(r):
        for c in range(WIDTH // 128):
            cols = slice(c * 128, (c + 1) * 128)
            new = cp_ref[r : r + 32, cols].astype(F32)
            buf_s[16 + r : 48 + r, cols] = new
            mixed = buf_s[14 + r : 46 + r, cols] * taps[0:1, cols]
            mixed = mixed + buf_s[15 + r : 47 + r, cols] * taps[1:2, cols]
            mixed = mixed + new * taps[2:3, cols]
            out_ref[r : r + 32, cols] = (go_ref[r : r + 32, cols].astype(F32) * mixed).astype(BF)

    return [lambda r=r: step(r) for r in range(0, ROWS, 32)]


def k3b_body(n_oth_ref, wo_ref, go_own_ref, go_oth_ref, q_own_ref, q_oth_ref, kt_ref,
             v_own_ref, v_oth_ref, u_ref, cm_ref, cp_own_ref, cp_oth_ref, gain_ref, taps_ref,
             cv_own_ref, cv_oth_ref, sg_oth_ref, in_own_ref, in_oth_ref,
             pad_s, col_s, s_s, w_s, buf_s, buf2_s):
    tp = lax.axis_index("tp")
    pad_s[...] = jnp.zeros_like(pad_s)
    gain = local_cols(gain_ref, tp).reshape(1, WIDTH)
    taps = local_cols(taps_ref, tp)
    scores_half(q_own_ref, kt_ref, tp, s_s)
    weights = weights_steps(u_ref, cm_ref, tp, s_s, w_s, pad_s, col_s.at[0])
    conv = conv_steps(cp_own_ref, cp_oth_ref, go_own_ref, taps, cv_own_ref, buf_s)
    gate_half(n_oth_ref, wo_ref, gain, sg_oth_ref, [step for pair in zip(weights, conv) for step in pair])
    intra_half(w_s, v_own_ref, in_own_ref)
    scores_half(q_oth_ref, kt_ref, 1 - tp, s_s)
    for step in weights_steps(u_ref, cm_ref, 1 - tp, s_s, w_s, pad_s, col_s.at[1]):
        step()
    intra_half(w_s, v_oth_ref, in_oth_ref)
    for step in conv_steps(cp_oth_ref, cp_own_ref, go_oth_ref, taps, cv_oth_ref, buf2_s):
        step()


def readout_steps(q_ref, in_ref, sg_ref, st_ref, sc_ref, cm_ref, half, out_ref, pad_s, col_s, c_s):
    for c in range(16):
        rows, cols = slice(c // 4 * BLOCK, (c // 4 + 1) * BLOCK), slice(c % 4 * DH, (c % 4 + 1) * DH)
        c_s[c * BLOCK : (c + 1) * BLOCK, :] = dot(q_ref[rows, cols], st_ref[half * 16 + c])
    cm = slot_rows(cm_ref, half)
    sc = slot_rows(sc_ref, half)
    m = jnp.maximum(cm, sc)
    columns_of(jnp.exp(cm - m), pad_s, col_s.at[0])
    columns_of(jnp.exp(sc - m), pad_s, col_s.at[1])

    def step(c):
        cols = slice(c % 4 * DH, (c % 4 + 1) * DH)
        for g in range(2):
            rows = slice(c // 4 * BLOCK + g * 64, c // 4 * BLOCK + g * 64 + 64)
            t = slice(g * 64, g * 64 + 64)
            read = col_s[1, t, c : c + 1] * c_s[c * BLOCK + g * 64 : c * BLOCK + g * 64 + 64, :] + col_s[0, t, c : c + 1] * in_ref[rows, cols]
            scale = lax.rsqrt(jnp.mean(read * read, axis=-1, keepdims=True) + EPSILON)
            out_ref[rows, cols] = (read * scale * sg_ref[rows, cols]).astype(BF)

    return [lambda c=c: step(c) for c in range(16)]


def conv_fix(cv_ref, cp_ref, go_ref, recv_refs, taps_ref, half, out_ref):
    tp = lax.axis_index("tp")
    x = lax.axis_index("sp_1")
    z = lax.axis_index("sp_0")
    here = jnp.full((8, BLOCK), x, jnp.int32)
    row = jnp.full((8, BLOCK), z, jnp.int32)
    rx1, rx2, rz1, rz2 = [r[536:PAY, :].astype(F32) for r in recv_refs]
    above = jnp.where(row == 0, 0.0, jnp.where(row == 2, rz2, rz1))
    rim8 = jnp.where(here == 0, above, jnp.where(here == 2, rx2, rx1))
    rim = [jnp.concatenate([rim8[r * 4 + c : r * 4 + c + 1, :] for c in range(4)], axis=1) for r in range(2)]
    taps = local_cols(taps_ref, tp)
    p = jnp.concatenate([rim[0], rim[1], cp_ref[0:16, :].astype(F32)], axis=0)
    mixed = p[0:16] * taps[0:1] + p[1:17] * taps[1:2] + p[2:18] * taps[2:3]
    fixed = go_ref[0:16, :].astype(F32) * mixed
    first = jnp.full((16, WIDTH), half, jnp.int32) == 0
    out_ref[0:16, WIDTH:] = jnp.where(first, fixed, cv_ref[0:16, :].astype(F32)).astype(BF)
    out_ref[16:, WIDTH:] = cv_ref[16:, :]


def finish_half(first_steps, second_steps, a_ref, acc_s, wm_ref, wc_ref, out_ref):
    tiles = [slice(j * 256, (j + 1) * 256) for j in range(D // 256)]
    for j, cols in enumerate(tiles):
        acc_s[:, cols] = dot(a_ref[FIRST, WIDTH:], wc_ref[:, cols])
        for step in first_steps[j::8]:
            step()
    for j, cols in enumerate(tiles):
        out_ref[FIRST, cols] = (acc_s[:, cols] + dot(a_ref[FIRST, :WIDTH], wm_ref[:, cols])).astype(BF)
        for step in second_steps[j::8]:
            step()
    for cols in tiles:
        out_ref[SECOND, cols] = (dot(a_ref[SECOND, WIDTH:], wc_ref[:, cols]) + dot(a_ref[SECOND, :WIDTH], wm_ref[:, cols])).astype(BF)


def k4_body(pm_ref, ps_ref, rx1_ref, rx2_ref, rz1_ref, rz2_ref, init_ref, tot_ref, bt_ref, term_ref,
            q_ref, in_ref, sg_ref, cm_ref, cv_ref, cp_ref, go_ref, taps_ref, wm_ref, wc_ref,
            send_ref, st_ref, sc_ref, a_s, acc_s, pad_s, col_s, c_s, cs_s):
    tp = lax.axis_index("tp")
    half = 1 - tp
    pad_s[...] = jnp.zeros_like(pad_s)
    recv_refs = (rx1_ref, rx2_ref, rz1_ref, rz2_ref)
    total, scale, w_new, w_old = prefix_merge(
        partner_is_lower("sp_0", 1), read_scalars(rz2_ref), (ps_ref[0:4, :], ps_ref[4:8, :])
    )
    top = jnp.maximum(total, scale)
    w_init = jnp.exp(total - top)
    w_prefix = jnp.exp(scale - top)
    for b in range(2 * NB):
        cs_s[b * 4 : b * 4 + 4, :] = top
        tot = tot_ref[b * 4 : b * 4 + 4, :] + top
        bt = bt_ref[b * 4 : b * 4 + 4, :]
        top = jnp.maximum(tot, bt)
        cs_s[32 + b * 4 : 36 + b * 4, :] = jnp.exp(tot - top)
        cs_s[64 + b * 4 : 68 + b * 4, :] = jnp.exp(bt - top)
    sc_ref[...] = cs_s[0:32, :]
    for h in range(HEADS):
        rows = slice(h * DH, (h + 1) * DH)
        one = slice(h, h + 1)
        prefix = w_new[one] * rz2_ref[rows, :].astype(F32) + w_old[one] * pm_ref[rows, :]
        mem = w_init[one] * init_ref[h] + w_prefix[one] * prefix
        for b in range(2 * NB):
            r = b * 4 + h
            st_ref[r] = mem.astype(BF)
            if b < 2 * NB - 1:
                mem = cs_s[32 + r : 33 + r, :] * mem + cs_s[64 + r : 65 + r, :] * term_ref[r]
    conv_fix(cv_ref, cp_ref, go_ref, recv_refs, taps_ref, half, a_s)
    steps = readout_steps(q_ref, in_ref, sg_ref, st_ref, sc_ref, cm_ref, half, a_s, pad_s, col_s, c_s)
    finish_half(steps[:8], steps[8:], a_s, acc_s, wm_ref, wc_ref, send_ref)


def k5a_body(rx1_ref, rx2_ref, rz1_ref, rz2_ref, q_ref, in_ref, sg_ref, st_ref, sc_ref, cm_ref, cv_ref, cp_ref, go_ref, taps_ref, wm_ref, wc_ref,
             part_ref, a_s, acc_s, pad_s, col_s, c_s):
    tp = lax.axis_index("tp")
    pad_s[...] = jnp.zeros_like(pad_s)
    conv_fix(cv_ref, cp_ref, go_ref, (rx1_ref, rx2_ref, rz1_ref, rz2_ref), taps_ref, tp, a_s)
    steps = readout_steps(q_ref, in_ref, sg_ref, st_ref, sc_ref, cm_ref, tp, a_s, pad_s, col_s, c_s)
    finish_half(steps[:8], steps[8:], a_s, acc_s, wm_ref, wc_ref, part_ref)


def k5b_body(part_ref, recv_ref, out_hbm, buf, sem):
    copies = []
    for i in range(8):
        rows = pl.ds(i * 64, 64)
        buf[rows, :] = part_ref[rows, :] + recv_ref[rows, :]
        copies.append(pltpu.make_async_copy(buf.at[rows, :], out_hbm.at[rows, :], sem.at[i]))
        copies[-1].start()
    for copy in copies:
        copy.wait()


def swapped(value, axis, mask):
    return lax.ppermute(value, axis, [(i, i ^ mask) for i in range(lax.axis_size(axis))])


def in_hbm(value):
    return pltpu.with_memory_space_constraint(value, pltpu.HBM)


def rotated(value, axis, distance):
    size = lax.axis_size(axis)
    return lax.ppermute(value, axis, [(i, (i + distance) % size) for i in range(size)])


def local(
    tokens, norm_gain, w_query, w_key, w_value, w_outgate, w_gatein, w_gateout, w_convin,
    w_igate, w_fgate, input_bias, forget_bias, forget_extra, init_memory, head_gain, conv_taps,
    out_memory, out_conv,
):
    own = tokens[0]
    other = rotated(own, "tp", 1)
    fx = forget_extra[0].T
    half_act = sds((ROWS, WIDTH))
    half_f32 = sds((ROWS, WIDTH), F32)
    gflop = 2 * ROWS * D * WIDTH
    weight = sds((D, WIDTH))
    n_own, k_own, v_own, g_own, gain, wi, wf, wk, wv, win, wcv = call(
        k1_body, "k1", [HBM] * 8,
        [sds((ROWS, D)), half_act, half_act, sds((16, ROWS), F32), sds((D,)), sds((8, D)), sds((8, D))] + [weight] * 4,
        [pltpu.VMEM((ROWS, D), BF), pltpu.SemaphoreType.DMA((12,))],
        flops=3 * gflop,
    )(*[in_hbm(a) for a in (own, norm_gain, w_igate.T, w_fgate.T, w_key, w_value, w_gatein, w_convin)])
    rows32 = sds((32, BLOCK), F32)
    state, scal = sds((512, DH), F32), sds((8, DH), F32)
    n_oth, v_oth, wq, kt, u, cm, tot, bt, terms, pay, rm, rs = call(
        k2_body, "k2", [V] * 15 + [HBM],
        [sds((ROWS, D)), half_act, weight, sds((32, DH, DH)), rows32, rows32, rows32, rows32, sds((32, DH, DH), F32), sds((PAY, DH)), state, scal],
        [pltpu.VMEM((ROWS, WIDTH), BF), pltpu.VMEM((16, ROWS), F32)] + [pltpu.VMEM((32, BLOCK), F32)] * 4
        + [pltpu.SemaphoreType.DMA],
        flops=3 * gflop,
    )(other, gain, wi, wf, wk, wv, g_own, k_own, v_own, fx, input_bias, forget_bias, n_own, win, wcv, in_hbm(w_query))
    merged = [state, scal, state, scal, sds((PAY, DH))]

    def merge(name, axis, index, first, from_received, last, *args):
        body = functools.partial(merge_body, axis, index, first, from_received, last)
        outs = merged[:2] + merged[4:] if last else merged
        scratch = [pltpu.VMEM((512, DH), F32), pltpu.VMEM((8, DH), F32)] if last else []
        return call(body, name, [V] * len(args), outs, scratch, flops=2**20, vmem=8)(*args)

    def cover(name, n, win, wcv, wq):
        return call(k3a_body, name, [V] * 4, [half_act] * 2, flops=5 * gflop)(n, win, wcv, wq)

    rx1 = swapped(pay, "sp_1", 1)
    cp_own, q_own = cover("k3a", n_own, win, wcv, wq)
    pm, ps, rm, rs, pay = merge("c1", "sp_1", 0, True, False, False, rm, rs, pay, rx1)
    rx2 = swapped(pay, "sp_1", 3)
    cp_oth, q_oth = cover("k3o", n_oth, win, wcv, wq)
    pm, ps, rm, rs, pay = merge("c2", "sp_1", 1, False, True, False, rm, rs, pm, ps, pay, rx2)
    rz1 = swapped(pay, "sp_0", 1)
    go_own, go_oth, sg_own = call(
        k3c_body, "k3c", [V] * 5, [half_act, half_act, half_f32], flops=5 * gflop,
    )(n_own, n_oth, w_gateout, w_outgate, head_gain)
    pm, ps, pay = merge("c3", "sp_0", 0, False, False, True, rm, rs, pm, ps, pay, rz1)
    rz2 = swapped(pay, "sp_0", 3)
    received = (rx1, rx2, rz1, rz2)
    square = pltpu.VMEM((BLOCK, BLOCK), F32)
    pair = pltpu.VMEM((2, BLOCK, BLOCK), F32)
    tall = pltpu.VMEM((16 * BLOCK, BLOCK), F32)
    pad_rows = pltpu.VMEM((ROWS + 16, WIDTH), F32)
    cv_own, cv_oth, sg_oth, in_own, in_oth = call(
        k3b_body, "k3b", [V] * 15, [half_act] * 2 + [half_f32] * 3,
        [square, pair, tall, pltpu.VMEM((16 * BLOCK, BLOCK), BF), pad_rows, pad_rows], flops=5 * gflop,
    )(n_oth, w_outgate, go_own, go_oth, q_own, q_oth, kt, v_own, v_oth, u, cm, cp_own, cp_oth, head_gain, conv_taps)
    wide = pltpu.VMEM((ROWS, 2 * WIDTH), BF)
    acc = pltpu.VMEM((256, D), F32)
    send, states, scales = call(
        k4_body, "k4", [V] * 20, [sds((ROWS, D)), sds((32, DH, DH)), rows32],
        [wide, acc, square, pair, tall, pltpu.VMEM((96, BLOCK), F32)], flops=3 * gflop,
    )(pm, ps, *received, init_memory[0], tot, bt, terms, q_oth, in_oth, sg_oth, cm, cv_oth, cp_oth, go_oth,
      conv_taps, out_memory, out_conv)
    recv = rotated(send, "tp", 1)
    (part,) = call(
        k5a_body, "k5a", [V] * 16, [sds((ROWS, D))], [wide, acc, square, pair, tall], flops=3 * gflop,
    )(*received, q_own, in_own, sg_own, states, scales, cm, cv_own, cp_own, go_own, conv_taps, out_memory, out_conv)
    out = pl.pallas_call(
        k5b_body, name="k5b", in_specs=[V, V], out_specs=HBM, out_shape=sds((ROWS, D)),
        scratch_shapes=[pltpu.VMEM((ROWS, D), BF), pltpu.SemaphoreType.DMA((8,))],
        compiler_params=pltpu.CompilerParams(vmem_limit_bytes=8 * MIB),
    )(part, recv)
    return out[None]


def solution(mesh):
    finer = Mesh(
        mesh.devices.reshape(4, 4, mesh.shape["fs"], mesh.shape["tp"]), ("sp_0", "sp_1", "fs", "tp")
    )
    sp_tp = ("sp_0", "sp_1", "tp")
    by_col = P(None, "tp")
    return jax.shard_map(
        local,
        mesh=finer,
        in_specs=(
            P("fs", sp_tp, None), P(), by_col, by_col, by_col, by_col, by_col, by_col, by_col,
            P(), P(), P(), P(), P("fs", SP, "tp"), P("fs", "tp", None, None), P(), P(),
            P("tp", None), P("tp", None),
        ),
        out_specs=P("fs", sp_tp, None),
        check_vma=False,
    )
```

```python
import functools
import math

import jax
import jax.numpy as jnp
from jax import lax
from jax.experimental import pallas as pl
from jax.experimental.pallas import tpu as pltpu
from jax.sharding import Mesh
from jax.sharding import PartitionSpec as P


BF = jnp.bfloat16
F32 = jnp.float32
BLOCK = 128
DH = 128
HEADS = 4
ROWS = 512
NB = 4
WIDTH = 512
D = 2048
EPSILON = 1e-06
LOWEST_LOG = -1e30
KEY_FACTOR = DH ** (-0.5)
LOG_KEY_FACTOR = math.log(KEY_FACTOR)
PAY = 544
SP = ("sp_0", "sp_1")
V = pl.BlockSpec(memory_space=pltpu.VMEM)
HBM = pl.BlockSpec(memory_space=pltpu.HBM)
SM = pl.BlockSpec(memory_space=pltpu.SMEM)
MIB = 2**20


def sds(shape, dtype=BF):
    return jax.ShapeDtypeStruct(shape, dtype)


def call(body, in_specs, outs, scratch=(), flops=0, vmem=16, nbytes=4 * MIB):
    return pl.pallas_call(
        body,
        in_specs=in_specs,
        out_specs=[V] * len(outs),
        out_shape=outs,
        scratch_shapes=list(scratch),
        compiler_params=pltpu.CompilerParams(vmem_limit_bytes=vmem * MIB),
        cost_estimate=pl.CostEstimate(flops=flops, bytes_accessed=nbytes, transcendentals=0),
    )


def dot(a, b):
    return jnp.dot(a, b, preferred_element_type=F32)


def dot_nt(a, b):
    return lax.dot_general(a, b, (((1,), (1,)), ((), ())), preferred_element_type=F32)


def norm_rows(x_ref, n_ref, gain_ref, start, groups):
    lanes = [slice(i * 128, (i + 1) * 128) for i in range(D // 128)]
    scales = []
    for g in range(groups):
        rows = slice(start + g * 16, start + g * 16 + 16)
        total = jnp.zeros((16, 128), F32)
        for cols in lanes:
            x = x_ref[rows, cols].astype(F32)
            total = total + x * x
        mean = jnp.sum(total, axis=-1, keepdims=True) * (1.0 / D)
        scales.append(jnp.broadcast_to(lax.rsqrt(mean + EPSILON), (16, 128)))
    for cols in lanes:
        gain = jnp.broadcast_to(gain_ref[cols].astype(F32).reshape(1, 128), (16, 128))
        for g in range(groups):
            rows = slice(start + g * 16, start + g * 16 + 16)
            n_ref[rows, cols] = (x_ref[rows, cols].astype(F32) * scales[g] * gain).astype(BF)


FIRST, SECOND, WHOLE = slice(0, 256), slice(256, 512), slice(0, 512)


def project(n_ref, w, out_ref, rows=WHOLE, between=()):
    for j in range(WIDTH // 256):
        cols = slice(j * 256, (j + 1) * 256)
        out_ref[rows, cols] = dot(n_ref[rows, :], w[:, cols]).astype(BF)
        for step in between[j::2]:
            step()


def gate_rows(wi_ref, wf_ref, n_ref, g_ref):
    wg = jnp.concatenate([wi_ref[...].astype(F32), wf_ref[...].astype(F32)], axis=0).astype(BF)
    g_ref[...] = dot_nt(wg, n_ref[...])


def norm_steps(x_ref, n_ref, gain, start, count):
    return [lambda g=g: norm_rows(x_ref, n_ref, gain, start + g * 64, 4) for g in range(count // 64)]


def k1_body(t_hbm, gain_hbm, wi_hbm, wf_hbm, wk_hbm, wv_hbm, win_hbm, wcv_hbm,
            n_ref, k_ref, v_ref, g_ref, gain_ref, wi_ref, wf_ref, wk_ref, wv_ref, win_ref, wcv_ref,
            t_buf, sem):
    quarter = [pl.ds(i * 64, 64) for i in range(4)]
    late = pl.ds(256, 256)
    pairs = [(gain_hbm, gain_ref)] + [(t_hbm.at[rows, :], t_buf.at[rows, :]) for rows in quarter]
    pairs += [(wk_hbm, wk_ref), (t_hbm.at[late, :], t_buf.at[late, :])]
    pairs += [(wi_hbm, wi_ref), (wf_hbm, wf_ref), (wv_hbm, wv_ref), (win_hbm, win_ref), (wcv_hbm, wcv_ref)]
    copies = [pltpu.make_async_copy(src, dst, sem.at[i]) for i, (src, dst) in enumerate(pairs)]
    for copy in copies[:7]:
        copy.start()
    for copy in copies[:5]:
        copy.wait()
    for copy in copies[7:]:
        copy.start()
    for step in norm_steps(t_buf, n_ref, gain_ref, 0, 256):
        step()
    copies[5].wait()
    copies[6].wait()
    project(n_ref, wk_ref, k_ref, FIRST, norm_steps(t_buf, n_ref, gain_ref, 256, 256))
    project(n_ref, wk_ref, k_ref, SECOND)
    for copy in copies[7:10]:
        copy.wait()
    project(n_ref, wv_ref, v_ref)
    gate_rows(wi_ref, wf_ref, n_ref, g_ref)
    for copy in copies[10:]:
        copy.wait()


def log_sigmoid(v):
    x = jnp.exp(-jnp.abs(v))
    series = x * (1.0 - x * (0.5 - x * (1.0 / 3.0 - x * 0.25)))
    return jnp.minimum(v, 0.0) - jnp.where(x < 0.01, series, jnp.log(1.0 + x))


def lane_scan(x, op, fill):
    lane = lax.broadcasted_iota(jnp.int32, x.shape, 1)
    for sh in (1, 2, 4, 8, 16, 32, 64):
        x = op(x, jnp.where(lane >= sh, pltpu.roll(x, sh, 1), fill))
    return x


def split3(x):
    a = x.astype(BF).astype(F32)
    r = x - a
    b = r.astype(BF).astype(F32)
    return a, b, r - b


def write_scalars(pay_ref, ts, rim):
    a, b, c = split3(ts)
    pay_ref[512:PAY, :] = jnp.concatenate([a, b, c, rim], axis=0).astype(BF)


def read_scalars(pay_ref):
    s = pay_ref[512:PAY, :].astype(F32)
    ts = s[0:8] + s[8:16] + s[16:24]
    return ts[0:4], ts[4:8]


def k2_body(t_ref, gain_ref, wi_ref, wf_ref, wk_ref, wv_ref, g_own_ref, k_own_ref, v_own_ref,
            fx_ref, ib_ref, fb_ref, n_own_ref, win_ref, wcv_ref, wq_hbm,
            n_ref, v_ref, wq_ref, kt_ref, u_ref, cm_ref, tot_ref, bt_ref, term_ref, pay_ref, rm_ref, ts_s,
            k_ref, g_ref, i_s, f_s, ws_s, wb_s, q_sem):
    load_q = pltpu.make_async_copy(wq_hbm, wq_ref, q_sem)
    load_q.start()
    tp = lax.axis_index("tp")
    for step in norm_steps(t_ref, n_ref, gain_ref, 0, 256):
        step()
    project(n_ref, wk_ref, k_ref, FIRST, norm_steps(t_ref, n_ref, gain_ref, 256, 256))
    project(n_ref, wk_ref, k_ref, SECOND)
    gate_rows(wi_ref, wf_ref, n_ref, g_ref)
    first_core = jnp.full((HEADS, ROWS), tp, jnp.int32) == 0

    def column(ref):
        square = (8, 8)
        diagonal = lax.broadcasted_iota(jnp.int32, square, 0) == lax.broadcasted_iota(jnp.int32, square, 1)
        wide = jnp.broadcast_to(ref[...].reshape(1, 8), square)
        col = jnp.sum(jnp.where(diagonal, wide, 0.0), axis=1, keepdims=True)
        full = jnp.broadcast_to(col, (8, ROWS))
        return jnp.where(first_core, full[0:4], full[4:8])

    in_bias, forget_bias = column(ib_ref), column(fb_ref)
    for half in range(2):
        if half == 0:
            g = [jnp.where(first_core, g_own_ref[4 * a : 4 * a + 4, :], g_ref[4 * a : 4 * a + 4, :]) for a in range(4)]
        else:
            g = [jnp.where(first_core, g_ref[4 * a : 4 * a + 4, :], g_own_ref[4 * a : 4 * a + 4, :]) for a in range(4)]
        in_pre = jnp.where(first_core, g[0], g[1]) + in_bias
        forget_pre = jnp.where(first_core, g[2], g[3]) + forget_bias
        lf = log_sigmoid(forget_pre) + fx_ref[:, half * ROWS : (half + 1) * ROWS]
        for j in range(NB):
            b = half * NB + j
            i_s[b * 4 : b * 4 + 4, :] = in_pre[:, j * BLOCK : (j + 1) * BLOCK]
            f_s[b * 4 : b * 4 + 4, :] = lf[:, j * BLOCK : (j + 1) * BLOCK]
    cum = lane_scan(f_s[...], jnp.add, 0.0)
    u = i_s[...] - cum
    cmax = lane_scan(u, jnp.maximum, -jnp.inf)
    tot = jnp.broadcast_to(cum[:, BLOCK - 1 :], cum.shape)
    top = tot + jnp.broadcast_to(cmax[:, BLOCK - 1 :], cum.shape)
    u_ref[...] = u + LOG_KEY_FACTOR
    cm_ref[...] = cmax
    tot_ref[...] = tot
    bt_ref[...] = top
    ws_s[...] = jnp.exp(tot + u - top) * KEY_FACTOR
    suffix = jnp.zeros((HEADS, BLOCK), F32)
    scale = jnp.full((HEADS, BLOCK), LOWEST_LOG, F32)
    for b in reversed(range(2 * NB)):
        e = suffix + bt_ref[b * 4 : b * 4 + 4, :]
        wb_s[b * 4 : b * 4 + 4, :] = e
        scale = jnp.maximum(scale, e)
        suffix = suffix + tot_ref[b * 4 : b * 4 + 4, :]
    for b in range(2 * NB):
        wb_s[b * 4 : b * 4 + 4, :] = jnp.exp(wb_s[b * 4 : b * 4 + 4, :] - scale)
    ts_s[0:4, :] = suffix
    ts_s[4:8, :] = scale
    project(n_ref, wv_ref, v_ref)
    own_last = jnp.full((16, D), tp, jnp.int32) == 1
    last = jnp.where(own_last, n_own_ref[ROWS - 16 :, :].astype(F32), n_ref[ROWS - 16 :, :].astype(F32)).astype(BF)
    rim = dot(last, win_ref[...]).astype(BF).astype(F32) * dot(last, wcv_ref[...]).astype(BF).astype(F32)
    rim = jnp.concatenate([rim[14 + r : 15 + r, c * 128 : (c + 1) * 128] for r in range(2) for c in range(4)], axis=0)
    write_scalars(pay_ref, ts_s[...], rim)
    for h in range(HEADS):
        cols = slice(h * DH, (h + 1) * DH)
        total = jnp.zeros((DH, DH), F32)
        for slot, (kr, vr) in enumerate(((k_own_ref, v_own_ref), (k_ref, v_ref))):
            half = tp if slot == 0 else 1 - tp
            for j in range(NB):
                rows = slice(j * BLOCK, (j + 1) * BLOCK)
                r = half * 16 + (j * 4 + h)
                kt = kr[rows, cols].T
                kt_ref[r] = kt
                term = dot((kt.astype(F32) * ws_s[pl.ds(r, 1), :]).astype(BF), vr[rows, cols])
                term_ref[r] = term
                total = total + wb_s[pl.ds(r, 1), :] * term
        rm_ref[h * DH : (h + 1) * DH, :] = total
        pay_ref[h * DH : (h + 1) * DH, :] = total.astype(BF)
    load_q.wait()


def k3a_body(n_ref, wi_ref, wc_ref, wq_ref, cp_ref, q_ref):
    for j in range(2):
        cols = slice(j * 256, (j + 1) * 256)
        a = dot(n_ref[...], wi_ref[:, cols]).astype(BF).astype(F32)
        c = dot(n_ref[...], wc_ref[:, cols]).astype(BF).astype(F32)
        cp_ref[:, cols] = (a * c).astype(BF)
    project(n_ref, wq_ref, q_ref)


def k3c_body(n_own_ref, n_oth_ref, wg_ref, wo_ref, gain_ref, go_own_ref, go_oth_ref, sg_own_ref):
    project(n_own_ref, wg_ref, go_own_ref)
    project(n_oth_ref, wg_ref, go_oth_ref)
    gain = local_cols(gain_ref, lax.axis_index("tp")).reshape(1, WIDTH)
    gate_half(n_own_ref, wo_ref, gain, sg_own_ref, ())


def joined(lower, upper):
    total = lower[0] + upper[0]
    scale = jnp.maximum(lower[1] + upper[0], upper[1])
    return total, scale, jnp.exp(lower[1] + upper[0] - scale), jnp.exp(upper[1] - scale)


def prefix_merge(partner_lower, received, prefix):
    total, scale, w_new, w_old = joined(received, prefix)
    return (
        jnp.where(partner_lower, total, prefix[0]), jnp.where(partner_lower, scale, prefix[1]),
        jnp.where(partner_lower, w_new, 0.0), jnp.where(partner_lower, w_old, 1.0),
    )


def partner_is_lower(axis, round_index):
    place = lax.axis_index(axis)
    value = lax.rem(place, 2) if round_index == 0 else place - 1
    return jnp.full((HEADS, DH), value, jnp.int32) > 0


def merge_body(axis, round_index, first, rim_from_received, last, *refs):
    if last:
        rm_ref, rs_ref, pm_ref, ps_ref, rim_ref, recv_ref, pm_out, ps_out, pay_ref, rm_out, rs_out = refs
        prefix = (ps_ref[0:4, :], ps_ref[4:8, :])
    elif first:
        rm_ref, rs_ref, own_pay_ref, recv_ref, pm_out, ps_out, rm_out, rs_out, pay_ref = refs
        prefix = (jnp.zeros((HEADS, DH), F32), jnp.full((HEADS, DH), LOWEST_LOG, F32))
    else:
        rm_ref, rs_ref, pm_ref, ps_ref, rim_ref, recv_ref, pm_out, ps_out, rm_out, rs_out, pay_ref = refs
        prefix = (ps_ref[0:4, :], ps_ref[4:8, :])
    lower = partner_is_lower(axis, round_index)
    received = read_scalars(recv_ref)
    total, scale, w_new, w_old = prefix_merge(lower, received, prefix)
    ps_out[0:4, :] = total
    ps_out[4:8, :] = scale
    mine = (rs_ref[0:4, :], rs_ref[4:8, :])
    low_first = joined(received, mine)
    low_second = joined(mine, received)
    rs_out[0:4, :] = low_first[0]
    rs_out[4:8, :] = jnp.where(lower, low_first[1], low_second[1])
    r_new = jnp.where(lower, low_first[2], low_second[3])
    r_old = jnp.where(lower, low_first[3], low_second[2])
    rim_source = recv_ref if rim_from_received else (own_pay_ref if first else rim_ref)
    write_scalars(pay_ref, rs_out[...], rim_source[536:PAY, :].astype(F32))
    for h in range(HEADS):
        rows, one = slice(h * DH, (h + 1) * DH), slice(h, h + 1)
        m = recv_ref[rows, :].astype(F32)
        pm_out[rows, :] = w_new[one] * m if first else w_new[one] * m + w_old[one] * pm_ref[rows, :]
        new = r_new[one] * m + r_old[one] * rm_ref[rows, :]
        rm_out[rows, :] = new
        pay_ref[rows, :] = new.astype(BF)


def slot_rows(ref, half):
    return ref[pl.ds(pl.multiple_of(half * 16, 16), 16), :]


def columns_of(rows16, pad_s, col_s):
    pad_s[0:16, :] = rows16
    col_s[...] = pad_s[...].T


def scores_half(q_ref, kt_ref, half, s_s):
    for c in range(16):
        rows, cols = slice(c // 4 * BLOCK, (c // 4 + 1) * BLOCK), slice(c % 4 * DH, (c % 4 + 1) * DH)
        s_s[c * BLOCK : (c + 1) * BLOCK, :] = dot(q_ref[rows, cols], kt_ref[half * 16 + c])


def weights_steps(u_ref, cm_ref, half, s_s, w_s, pad_s, col_s):
    columns_of(slot_rows(cm_ref, half), pad_s, col_s)
    causal = lax.broadcasted_iota(jnp.int32, (BLOCK, BLOCK), 1) <= lax.broadcasted_iota(jnp.int32, (BLOCK, BLOCK), 0)

    def step(c):
        rows = slice(c * BLOCK, (c + 1) * BLOCK)
        log = u_ref[pl.ds(half * 16 + c, 1), :] - col_s[:, c : c + 1]
        w_s[rows, :] = (jnp.exp(jnp.where(causal, log, -jnp.inf)) * s_s[rows, :]).astype(BF)

    return [lambda c=c: step(c) for c in range(16)]


def intra_half(w_s, v_ref, out_ref):
    for c in range(16):
        rows, cols = slice(c // 4 * BLOCK, (c // 4 + 1) * BLOCK), slice(c % 4 * DH, (c % 4 + 1) * DH)
        out_ref[rows, cols] = dot(w_s[c * BLOCK : (c + 1) * BLOCK, :], v_ref[rows, cols])


def local_cols(ref, tp):
    return ref[..., pl.ds(pl.multiple_of(tp * WIDTH, WIDTH), WIDTH)].astype(F32)


def gate_half(n_ref, wo_ref, gain, out_ref, between):
    share = len(between) // 4
    for i in range(2):
        rows = slice(i * 256, (i + 1) * 256)
        for j in range(WIDTH // 256):
            cols = slice(j * 256, (j + 1) * 256)
            raw = dot(n_ref[rows, :], wo_ref[:, cols]).astype(BF).astype(F32)
            out_ref[rows, cols] = jax.nn.sigmoid(raw) * gain[:, cols]
            for step in between[(i * 2 + j) * share : (i * 2 + j + 1) * share]:
                step()


def conv_steps(cp_ref, before_ref, go_ref, taps, out_ref, buf_s):
    buf_s[0:16, :] = before_ref[ROWS - 16 :, :].astype(F32)

    def step(r):
        for c in range(WIDTH // 128):
            cols = slice(c * 128, (c + 1) * 128)
            new = cp_ref[r : r + 32, cols].astype(F32)
            buf_s[16 + r : 48 + r, cols] = new
            mixed = buf_s[14 + r : 46 + r, cols] * taps[0:1, cols]
            mixed = mixed + buf_s[15 + r : 47 + r, cols] * taps[1:2, cols]
            mixed = mixed + new * taps[2:3, cols]
            out_ref[r : r + 32, cols] = (go_ref[r : r + 32, cols].astype(F32) * mixed).astype(BF)

    return [lambda r=r: step(r) for r in range(0, ROWS, 32)]


def k3b_body(n_oth_ref, wo_ref, go_own_ref, go_oth_ref, q_own_ref, q_oth_ref, kt_ref,
             v_own_ref, v_oth_ref, u_ref, cm_ref, cp_own_ref, cp_oth_ref, gain_ref, taps_ref,
             cv_own_ref, cv_oth_ref, sg_oth_ref, in_own_ref, in_oth_ref,
             pad_s, col_s, s_s, w_s, buf_s, buf2_s):
    tp = lax.axis_index("tp")
    pad_s[...] = jnp.zeros_like(pad_s)
    gain = local_cols(gain_ref, tp).reshape(1, WIDTH)
    taps = local_cols(taps_ref, tp)
    scores_half(q_own_ref, kt_ref, tp, s_s)
    weights = weights_steps(u_ref, cm_ref, tp, s_s, w_s, pad_s, col_s.at[0])
    conv = conv_steps(cp_own_ref, cp_oth_ref, go_own_ref, taps, cv_own_ref, buf_s)
    gate_half(n_oth_ref, wo_ref, gain, sg_oth_ref, [step for pair in zip(weights, conv) for step in pair])
    intra_half(w_s, v_own_ref, in_own_ref)
    scores_half(q_oth_ref, kt_ref, 1 - tp, s_s)
    for step in weights_steps(u_ref, cm_ref, 1 - tp, s_s, w_s, pad_s, col_s.at[1]):
        step()
    intra_half(w_s, v_oth_ref, in_oth_ref)
    for step in conv_steps(cp_oth_ref, cp_own_ref, go_oth_ref, taps, cv_oth_ref, buf2_s):
        step()


def readout_steps(q_ref, in_ref, sg_ref, st_ref, sc_ref, cm_ref, half, out_ref, pad_s, col_s, c_s, blocks=range(16)):
    for c in blocks:
        rows, cols = slice(c // 4 * BLOCK, (c // 4 + 1) * BLOCK), slice(c % 4 * DH, (c % 4 + 1) * DH)
        c_s[c * BLOCK : (c + 1) * BLOCK, :] = dot(q_ref[rows, cols], st_ref[half * 16 + c])
    cm = slot_rows(cm_ref, half)
    sc = slot_rows(sc_ref, half)
    m = jnp.maximum(cm, sc)
    columns_of(jnp.exp(cm - m), pad_s, col_s.at[0])
    columns_of(jnp.exp(sc - m), pad_s, col_s.at[1])

    def step(c):
        cols = slice(c % 4 * DH, (c % 4 + 1) * DH)
        for g in range(2):
            rows = slice(c // 4 * BLOCK + g * 64, c // 4 * BLOCK + g * 64 + 64)
            t = slice(g * 64, g * 64 + 64)
            read = col_s[1, t, c : c + 1] * c_s[c * BLOCK + g * 64 : c * BLOCK + g * 64 + 64, :] + col_s[0, t, c : c + 1] * in_ref[rows, cols]
            scale = lax.rsqrt(jnp.mean(read * read, axis=-1, keepdims=True) + EPSILON)
            out_ref[rows, cols] = (read * scale * sg_ref[rows, cols]).astype(BF)

    return [lambda c=c: step(c) for c in blocks]


def conv_fix(cv_ref, cp_ref, go_ref, recv_refs, taps_ref, half, out_ref):
    tp = lax.axis_index("tp")
    x = lax.axis_index("sp_1")
    z = lax.axis_index("sp_0")
    here = jnp.full((8, BLOCK), x, jnp.int32)
    row = jnp.full((8, BLOCK), z, jnp.int32)
    rx1, rx2, rz1, rz2 = [r[536:PAY, :].astype(F32) for r in recv_refs]
    above = jnp.where(row == 0, 0.0, jnp.where(row == 2, rz2, rz1))
    rim8 = jnp.where(here == 0, above, jnp.where(here == 2, rx2, rx1))
    rim = [jnp.concatenate([rim8[r * 4 + c : r * 4 + c + 1, :] for c in range(4)], axis=1) for r in range(2)]
    taps = local_cols(taps_ref, tp)
    p = jnp.concatenate([rim[0], rim[1], cp_ref[0:16, :].astype(F32)], axis=0)
    mixed = p[0:16] * taps[0:1] + p[1:17] * taps[1:2] + p[2:18] * taps[2:3]
    fixed = go_ref[0:16, :].astype(F32) * mixed
    first = jnp.full((16, WIDTH), half, jnp.int32) == 0
    out_ref[0:16, WIDTH:] = jnp.where(first, fixed, cv_ref[0:16, :].astype(F32)).astype(BF)
    out_ref[16:, WIDTH:] = cv_ref[16:, :]


def finish_half(first_steps, second_steps, a_ref, acc_s, wm_ref, wc_ref, out_ref):
    tiles = [slice(j * 256, (j + 1) * 256) for j in range(D // 256)]
    for j, cols in enumerate(tiles):
        acc_s[:, cols] = dot(a_ref[FIRST, WIDTH:], wc_ref[:, cols])
        for step in first_steps[j::8]:
            step()
    for j, cols in enumerate(tiles):
        out_ref[FIRST, cols] = (acc_s[:, cols] + dot(a_ref[FIRST, :WIDTH], wm_ref[:, cols])).astype(BF)
        for step in second_steps[j::8]:
            step()
    for cols in tiles:
        out_ref[SECOND, cols] = (dot(a_ref[SECOND, WIDTH:], wc_ref[:, cols]) + dot(a_ref[SECOND, :WIDTH], wm_ref[:, cols])).astype(BF)


def finish_rows(steps, conv_rows, memory_rows, acc_s, wm_ref, wc_ref, out_ref):
    tiles = [slice(j * 256, (j + 1) * 256) for j in range(D // 256)]
    for j, cols in enumerate(tiles):
        acc_s[:, cols] = dot(conv_rows[...], wc_ref[:, cols])
        steps[j]()
    for cols in tiles:
        out_ref[:, cols] = (acc_s[:, cols] + dot(memory_rows[...], wm_ref[:, cols])).astype(BF)


def k4b_body(q_ref, in_ref, sg_ref, st_ref, sc_ref, cm_ref, cv_ref, wm_ref, wc_ref, send_ref, a_s, acc_s, pad_s, col_s, c_s):
    half = 1 - lax.axis_index("tp")
    pad_s[...] = jnp.zeros_like(pad_s)
    steps = readout_steps(q_ref, in_ref, sg_ref, st_ref, sc_ref, cm_ref, half, a_s, pad_s, col_s, c_s, range(8, 16))
    finish_rows(steps, cv_ref.at[SECOND, :], a_s.at[SECOND, :WIDTH], acc_s, wm_ref, wc_ref, send_ref)


def k4_body(pm_ref, ps_ref, rx1_ref, rx2_ref, rz1_ref, rz2_ref, init_ref, tot_ref, bt_ref, term_ref,
            q_ref, in_ref, sg_ref, cm_ref, cv_ref, cp_ref, go_ref, taps_ref, wm_ref, wc_ref,
            send_ref, st_ref, sc_ref, a_s, acc_s, pad_s, col_s, c_s, cs_s):
    tp = lax.axis_index("tp")
    half = 1 - tp
    pad_s[...] = jnp.zeros_like(pad_s)
    recv_refs = (rx1_ref, rx2_ref, rz1_ref, rz2_ref)
    total, scale, w_new, w_old = prefix_merge(
        partner_is_lower("sp_0", 1), read_scalars(rz2_ref), (ps_ref[0:4, :], ps_ref[4:8, :])
    )
    top = jnp.maximum(total, scale)
    w_init = jnp.exp(total - top)
    w_prefix = jnp.exp(scale - top)
    for b in range(2 * NB):
        cs_s[b * 4 : b * 4 + 4, :] = top
        tot = tot_ref[b * 4 : b * 4 + 4, :] + top
        bt = bt_ref[b * 4 : b * 4 + 4, :]
        top = jnp.maximum(tot, bt)
        cs_s[32 + b * 4 : 36 + b * 4, :] = jnp.exp(tot - top)
        cs_s[64 + b * 4 : 68 + b * 4, :] = jnp.exp(bt - top)
    sc_ref[...] = cs_s[0:32, :]
    for h in range(HEADS):
        rows = slice(h * DH, (h + 1) * DH)
        one = slice(h, h + 1)
        prefix = w_new[one] * rz2_ref[rows, :].astype(F32) + w_old[one] * pm_ref[rows, :]
        mem = w_init[one] * init_ref[h] + w_prefix[one] * prefix
        for b in range(2 * NB):
            r = b * 4 + h
            st_ref[r] = mem.astype(BF)
            if b < 2 * NB - 1:
                mem = cs_s[32 + r : 33 + r, :] * mem + cs_s[64 + r : 65 + r, :] * term_ref[r]
    conv_fix(cv_ref, cp_ref, go_ref, recv_refs, taps_ref, half, a_s)
    steps = readout_steps(q_ref, in_ref, sg_ref, st_ref, sc_ref, cm_ref, half, a_s, pad_s, col_s, c_s, range(8))
    finish_rows(steps, a_s.at[FIRST, WIDTH:], a_s.at[FIRST, :WIDTH], acc_s, wm_ref, wc_ref, send_ref)


def k5a_body(rx1_ref, rx2_ref, rz1_ref, rz2_ref, q_ref, in_ref, sg_ref, st_ref, sc_ref, cm_ref, cv_ref, cp_ref, go_ref, taps_ref, wm_ref, wc_ref,
             part_ref, a_s, acc_s, pad_s, col_s, c_s):
    tp = lax.axis_index("tp")
    pad_s[...] = jnp.zeros_like(pad_s)
    conv_fix(cv_ref, cp_ref, go_ref, (rx1_ref, rx2_ref, rz1_ref, rz2_ref), taps_ref, tp, a_s)
    steps = readout_steps(q_ref, in_ref, sg_ref, st_ref, sc_ref, cm_ref, tp, a_s, pad_s, col_s, c_s)
    finish_half(steps[:8], steps[8:], a_s, acc_s, wm_ref, wc_ref, part_ref)


def k5b_body(part_ref, recv1_ref, recv2_ref, out_hbm, buf, sem):
    copies = []
    for i in range(8):
        rows = pl.ds(i * 64, 64)
        recv_ref = recv1_ref if i < 4 else recv2_ref
        buf[rows, :] = part_ref[rows, :] + recv_ref[i % 4 * 64 : i % 4 * 64 + 64, :]
        copies.append(pltpu.make_async_copy(buf.at[rows, :], out_hbm.at[rows, :], sem.at[i]))
        copies[-1].start()
    for copy in copies:
        copy.wait()


def swapped(value, axis, mask):
    return lax.ppermute(value, axis, [(i, i ^ mask) for i in range(lax.axis_size(axis))])


def in_hbm(value):
    return pltpu.with_memory_space_constraint(value, pltpu.HBM)


def rotated(value, axis, distance):
    size = lax.axis_size(axis)
    return lax.ppermute(value, axis, [(i, (i + distance) % size) for i in range(size)])


def local(
    tokens, norm_gain, w_query, w_key, w_value, w_outgate, w_gatein, w_gateout, w_convin,
    w_igate, w_fgate, input_bias, forget_bias, forget_extra, init_memory, head_gain, conv_taps,
    out_memory, out_conv,
):
    own = tokens[0]
    other = rotated(own, "tp", 1)
    fx = forget_extra[0].T
    half_act = sds((ROWS, WIDTH))
    half_f32 = sds((ROWS, WIDTH), F32)
    gflop = 2 * ROWS * D * WIDTH
    weight = sds((D, WIDTH))
    n_own, k_own, v_own, g_own, gain, wi, wf, wk, wv, win, wcv = call(
        k1_body, [HBM] * 8,
        [sds((ROWS, D)), half_act, half_act, sds((16, ROWS), F32), sds((D,)), sds((8, D)), sds((8, D))] + [weight] * 4,
        [pltpu.VMEM((ROWS, D), BF), pltpu.SemaphoreType.DMA((12,))],
        flops=3 * gflop,
    )(*[in_hbm(a) for a in (own, norm_gain, w_igate.T, w_fgate.T, w_key, w_value, w_gatein, w_convin)])
    rows32 = sds((32, BLOCK), F32)
    state, scal = sds((512, DH), F32), sds((8, DH), F32)
    n_oth, v_oth, wq, kt, u, cm, tot, bt, terms, pay, rm, rs = call(
        k2_body, [V] * 15 + [HBM],
        [sds((ROWS, D)), half_act, weight, sds((32, DH, DH)), rows32, rows32, rows32, rows32, sds((32, DH, DH), F32), sds((PAY, DH)), state, scal],
        [pltpu.VMEM((ROWS, WIDTH), BF), pltpu.VMEM((16, ROWS), F32)] + [pltpu.VMEM((32, BLOCK), F32)] * 4
        + [pltpu.SemaphoreType.DMA],
        flops=3 * gflop,
    )(other, gain, wi, wf, wk, wv, g_own, k_own, v_own, fx, input_bias, forget_bias, n_own, win, wcv, in_hbm(w_query))
    merged = [state, scal, state, scal, sds((PAY, DH))]

    def merge(axis, index, first, from_received, last, *args):
        body = functools.partial(merge_body, axis, index, first, from_received, last)
        outs = merged[:2] + merged[4:] if last else merged
        scratch = [pltpu.VMEM((512, DH), F32), pltpu.VMEM((8, DH), F32)] if last else []
        return call(body, [V] * len(args), outs, scratch, flops=2**20, vmem=8)(*args)

    def cover(n, win, wcv, wq):
        return call(k3a_body, [V] * 4, [half_act] * 2, flops=5 * gflop)(n, win, wcv, wq)

    rx1 = swapped(pay, "sp_1", 1)
    cp_own, q_own = cover(n_own, win, wcv, wq)
    pm, ps, rm, rs, pay = merge("sp_1", 0, True, False, False, rm, rs, pay, rx1)
    rx2 = swapped(pay, "sp_1", 3)
    cp_oth, q_oth = cover(n_oth, win, wcv, wq)
    pm, ps, rm, rs, pay = merge("sp_1", 1, False, True, False, rm, rs, pm, ps, pay, rx2)
    rz1 = swapped(pay, "sp_0", 1)
    go_own, go_oth, sg_own = call(
        k3c_body, [V] * 5, [half_act, half_act, half_f32], flops=5 * gflop,
    )(n_own, n_oth, w_gateout, w_outgate, head_gain)
    pm, ps, pay = merge("sp_0", 0, False, False, True, rm, rs, pm, ps, pay, rz1)
    rz2 = swapped(pay, "sp_0", 3)
    received = (rx1, rx2, rz1, rz2)
    square = pltpu.VMEM((BLOCK, BLOCK), F32)
    pair = pltpu.VMEM((2, BLOCK, BLOCK), F32)
    tall = pltpu.VMEM((16 * BLOCK, BLOCK), F32)
    pad_rows = pltpu.VMEM((ROWS + 16, WIDTH), F32)
    cv_own, cv_oth, sg_oth, in_own, in_oth = call(
        k3b_body, [V] * 15, [half_act] * 2 + [half_f32] * 3,
        [square, pair, tall, pltpu.VMEM((16 * BLOCK, BLOCK), BF), pad_rows, pad_rows], flops=5 * gflop,
    )(n_oth, w_outgate, go_own, go_oth, q_own, q_oth, kt, v_own, v_oth, u, cm, cp_own, cp_oth, head_gain, conv_taps)
    wide = pltpu.VMEM((ROWS, 2 * WIDTH), BF)
    acc = pltpu.VMEM((256, D), F32)
    half_send = sds((ROWS // 2, D))
    send1, states, scales = call(
        k4_body, [V] * 20, [half_send, sds((32, DH, DH)), rows32],
        [wide, acc, square, pair, tall, pltpu.VMEM((96, BLOCK), F32)], flops=3 * gflop,
    )(pm, ps, *received, init_memory[0], tot, bt, terms, q_oth, in_oth, sg_oth, cm, cv_oth, cp_oth, go_oth,
      conv_taps, out_memory, out_conv)
    recv1 = rotated(send1, "tp", 1)
    (send2,) = call(
        k4b_body, [V] * 9, [half_send], [wide, acc, square, pair, tall], flops=gflop,
    )(q_oth, in_oth, sg_oth, states, scales, cm, cv_oth, out_memory, out_conv)
    recv2 = rotated(send2, "tp", 1)
    (part,) = call(
        k5a_body, [V] * 16, [sds((ROWS, D))], [wide, acc, square, pair, tall], flops=3 * gflop,
    )(*received, q_own, in_own, sg_own, states, scales, cm, cv_own, cp_own, go_own, conv_taps, out_memory, out_conv)
    out = pl.pallas_call(
        k5b_body, name="k5b", in_specs=[V, V, V], out_specs=HBM, out_shape=sds((ROWS, D)),
        scratch_shapes=[pltpu.VMEM((ROWS, D), BF), pltpu.SemaphoreType.DMA((8,))],
        compiler_params=pltpu.CompilerParams(vmem_limit_bytes=8 * MIB),
    )(part, recv1, recv2)
    return out[None]


def solution(mesh):
    finer = Mesh(
        mesh.devices.reshape(4, 4, mesh.shape["fs"], mesh.shape["tp"]), ("sp_0", "sp_1", "fs", "tp")
    )
    sp_tp = ("sp_0", "sp_1", "tp")
    by_col = P(None, "tp")
    return jax.shard_map(
        local,
        mesh=finer,
        in_specs=(
            P("fs", sp_tp, None), P(), by_col, by_col, by_col, by_col, by_col, by_col, by_col,
            P(), P(), P(), P(), P("fs", SP, "tp"), P("fs", "tp", None, None), P(), P(),
            P("tp", None), P("tp", None),
        ),
        out_specs=P("fs", sp_tp, None),
        check_vma=False,
    )
```
